256 devices in a mesh: ep: 64 (over z, x, core), tp: 4 (over y).
Axes of the slice: x: 4, y: 4, z: 8, core: 2. Of those that a mesh axis runs over, the one named last changes fastest.
Arguments:
- mix_in: bfloat16 [8192, 2048], P('ep'), may hold values from -6 to 6
- mix_gain: float32 [2048], replicated, may hold values from 0.1 to 1.9
- query_weight: bfloat16 [2048, 3072], P(None, 'tp'), may hold values from -0.125 to 0.125
- latent_weight: bfloat16 [2048, 512], replicated, may hold values from -0.125 to 0.125
- rotary_weight: bfloat16 [2048, 64], replicated, may hold values from -0.125 to 0.125
- latent_gain: float32 [512], replicated, may hold values from 0.1 to 1.9
- key_weight: bfloat16 [512, 2048], P(None, 'tp'), may hold values from -0.25 to 0.25
- value_weight: bfloat16 [512, 2048], P(None, 'tp'), may hold values from -0.25 to 0.25
- output_weight: bfloat16 [2048, 2048], P('tp'), may hold values from -0.125 to 0.125
- out_gain: float32 [2048], replicated, may hold values from 0.1 to 1.9
- ffn_in: bfloat16 [8192, 2048], P('ep'), may hold values from -6 to 6
- ffn_gain: float32 [2048], replicated, may hold values from 0.1 to 1.9
- gate_weight: bfloat16 [64, 2048, 1024], P('ep', None, 'tp'), may hold values from -0.375 to 0.375
- up_weight: bfloat16 [64, 2048, 1024], P('ep', None, 'tp'), may hold values from -0.375 to 0.375
- down_weight: bfloat16 [64, 1024, 2048], P('ep', 'tp'), may hold values from -0.046875 to 0.046875
- routes: int32 [8192, 4], P('ep'), may hold values from 0 to 63, all different within a row; in each aligned block of 32 rows (0 to 31, 32 to 63, ...) at most 4 rows name the same one
- route_scores: float32 [8192, 4], P('ep'), may hold values from -6 to 6
Outputs:
- mixed: bfloat16 [8192, 2048], P(('ep', 'tp'))
- moe_out: bfloat16 [8192, 2048], P(('ep', 'tp'))
The draws below stay inside these ranges and needn't reach their ends.
Inputs may be any that keep to these rules, and one draw needn't show every extreme that they name: `routes`: each row names 4 different experts; in each aligned block of 32 rows no expert is named by more than 4 rows, a bound that some blocks reach.
All inputs are finite; a program needn't handle non-finite values.
Results may differ from the reference program's by a relative error of at most 0.014.
Values may be sent and summed in bfloat16 or wider, within the bound.
A program may use at most 192 MiB of HBM per device.

```python
import math
import jax
import jax.numpy as jnp
import numpy as np
from jax import lax

D = 2048
HEADS = 16
NOPE = 128
ROPE = 64
VD = 128
KVR = 512
FF = 1024
TOP = 4
EXPERTS = 64
TOKENS_A = 8192
TOKENS_B = 8192
QB = 32
MOST = 4
N_TP = 4


def steps_of(own_key, shape, pieces, least, high):
    factor_of = 1.0
    for position, blocks in pieces:
        heights = jax.random.uniform(jax.random.fold_in(jax.random.fold_in(own_key, 6), position), (blocks,), jnp.float32, least / len(pieces), high / len(pieces))
        factor_of = factor_of * jnp.repeat(jnp.exp(heights), shape[position] // blocks).reshape((-1,) + (1,) * (len(shape) - 1 - position))
    return factor_of


def assign_block(key, own, number, rows, count, top, bound, slope):
    ranking = jax.random.permutation(key, count)
    crowded, usual = portions_of(count, rows * top, bound, slope, True), portions_of(count, rows * top, bound, slope, False)
    places = jnp.arange(count)

    def named(lengths, turn):
        used = int((lengths > 0).sum())
        fixed = max(1, used // 4)
        moved = fixed + (places - fixed + turn * (used - fixed)) % max(1, count - fixed)
        return jnp.zeros((count,), jnp.int32).at[ranking[jnp.where(places < fixed, places, moved)]].set(jnp.asarray(lengths, jnp.int32))

    lengths = jnp.where(number % 4 == 0, named(crowded, number // 4), named(usual, number - number // 4 - 1))
    mixed = jax.random.permutation(jax.random.fold_in(own, 3), count)
    source_of, taker = mixed[0:count // 2 * 2:2], mixed[1:count // 2 * 2:2]
    room = jnp.minimum(lengths[source_of] - 1, bound - lengths[taker]) // 2
    room = jnp.where((source_of == ranking[0]) | (taker == ranking[0]) | (lengths[taker] == 0), 0, jnp.maximum(room, 0))
    moved = jax.random.randint(jax.random.fold_in(own, 4), (count // 2,), 0, 1 << 20) % (room + 1)
    lengths = lengths.at[source_of].add(-moved).at[taker].add(moved)
    items = jnp.searchsorted(jnp.cumsum(lengths), jnp.arange(rows * top), side="right").astype(jnp.int32)
    table = items.reshape(top, rows).T
    table = table[jax.random.permutation(jax.random.fold_in(own, 1), rows)]
    turn = jax.random.randint(jax.random.fold_in(own, 2), (rows, 1), 0, top)
    return jnp.take_along_axis(table, (jnp.arange(top)[None, :] + turn) % top, axis=1)


def portions_of(count, total, most, lean, full):
    portions = [(1 << 20) // math.isqrt(grade ** lean) + 1 for grade in range(1, count + 1)]
    largest = most if full else min(most, max(-(-total // count), total * portions[0] // sum(portions)))
    least = 1 if total - largest >= count - 1 else 0
    holding, rest = [largest] + [least] * (count - 1), total - largest - least * (count - 1)
    while rest > 0:
        movable = [i for i in range(1, count) if holding[i] < largest] or [i for i in range(1, count) if holding[i] < most]
        mass, budget = sum([portions[i] for i in movable]), rest
        for i in movable:
            more = min(most - holding[i], max(1, budget * portions[i] // mass), rest)
            holding[i] = holding[i] + more
            rest = rest - more
    return np.array(holding)


def noise(own_key, dims, deviation, limit, split=(), kind=jnp.bfloat16):
    gain = steps_of(own_key, dims, split, -0.22, 0.18) if split else 1.0
    drawn = jax.random.normal(own_key, dims, jnp.float32) * deviation * gain
    return jnp.minimum(jnp.maximum(drawn, -limit), limit).astype(kind)


def setup_inputs(seed: int = 0) -> dict:
    key_list = jax.random.split(jax.random.key(seed), 18)
    mix_in = noise(key_list[0], (TOKENS_A, D), 1.0, 6.0, ((0, 64),))
    mix_gain = jnp.clip(1.0 + 0.18 * jax.random.normal(key_list[1], (D,), jnp.float32), 0.1, 1.9)
    query_weight = noise(key_list[2], (D, HEADS * (NOPE + ROPE)), D ** -0.5, 0.125, ((1, 4),))
    latent_weight = noise(key_list[3], (D, KVR), D ** -0.5, 0.125)
    rotary_weight = noise(key_list[4], (D, ROPE), D ** -0.5, 0.125)
    latent_gain = jnp.clip(1.0 + 0.18 * jax.random.normal(key_list[5], (KVR,), jnp.float32), 0.1, 1.9)
    key_weight = noise(key_list[6], (KVR, HEADS * NOPE), KVR ** -0.5, 0.25, ((1, 4),))
    value_weight = noise(key_list[7], (KVR, HEADS * VD), KVR ** -0.5, 0.25, ((1, 4),))
    output_weight = noise(key_list[8], (HEADS * VD, D), (HEADS * VD) ** -0.5, 0.125, ((0, 4),))
    out_gain = jnp.clip(1.0 + 0.18 * jax.random.normal(key_list[9], (D,), jnp.float32), 0.1, 1.9)
    ffn_in = noise(key_list[10], (TOKENS_B, D), 1.0, 6.0, ((0, 64),))
    ffn_gain = jnp.clip(1.0 + 0.18 * jax.random.normal(key_list[11], (D,), jnp.float32), 0.1, 1.9)
    gate_weight = noise(key_list[12], (EXPERTS, D, FF), (D // 8) ** -0.5, 0.375, ((0, 64), (2, 4)))
    up_weight = noise(key_list[13], (EXPERTS, D, FF), (D // 8) ** -0.5, 0.375, ((0, 64), (2, 4)))
    down_weight = noise(key_list[14], (EXPERTS, FF, D), (FF * 16) ** -0.5, 0.046875, ((0, 64), (1, 4)))
    routes_keys = jax.random.split(jax.random.fold_in(key_list[15], 1), TOKENS_B // QB)
    routes_turns = jax.random.permutation(jax.random.fold_in(key_list[15], 3), TOKENS_B // QB)
    routes = jax.vmap(lambda own, number: assign_block(jax.random.fold_in(key_list[15], 2), own, number, QB, EXPERTS, TOP, MOST, 2))(routes_keys, routes_turns).reshape((TOKENS_B, TOP))
    route_scores = noise(key_list[16], (TOKENS_B, TOP), 1.0, 6.0, ((0, 64),), jnp.float32)
    return dict(mix_in=mix_in, mix_gain=mix_gain, query_weight=query_weight, latent_weight=latent_weight, rotary_weight=rotary_weight, latent_gain=latent_gain, key_weight=key_weight, value_weight=value_weight, output_weight=output_weight, out_gain=out_gain, ffn_in=ffn_in, ffn_gain=ffn_gain, gate_weight=gate_weight, up_weight=up_weight, down_weight=down_weight, routes=routes, route_scores=route_scores)


norm_eps = 1e-06
clamp_limit = 7.0
gate_slope = 1.702
rope_base = 10000.0

def rms_rows(rows_in, scales):
    mean_square = lax.optimization_barrier(jnp.mean(rows_in * rows_in, axis=-1, keepdims=True))
    return rows_in * lax.rsqrt(mean_square + norm_eps) * scales.astype(jnp.float32)

def angle_tables(positions):
    inverse = rope_base ** (-jnp.arange(0, ROPE, 2).astype(jnp.float32) / ROPE)
    angle_rows = positions.astype(jnp.float32)[:, None] * inverse[None, :]
    return (jnp.cos(angle_rows), jnp.sin(angle_rows))

def rotate_last(vectors, cosine, sine_rows):
    half_rope = vectors.shape[-1] // 2
    upper_half = vectors[..., :half_rope]
    lower_half = vectors[..., half_rope:]
    return jnp.concatenate([upper_half * cosine - lower_half * sine_rows, lower_half * cosine + upper_half * sine_rows], axis=-1)

def clamped_unit(gate_part, linear):
    gate_part = jnp.minimum(gate_part, clamp_limit)
    linear = jnp.clip(linear, -clamp_limit, clamp_limit)
    return gate_part * jax.nn.sigmoid(gate_slope * gate_part) * (linear + 1.0)

def rounded(vectors):
    return lax.optimization_barrier(vectors.astype(jnp.bfloat16)).astype(jnp.float32)

def mixer_half(mix_in, mix_gain, query_weight, latent_weight, rotary_weight, latent_gain, key_weight, value_weight, output_weight, out_gain):
    length = mix_in.shape[0]
    normed = rms_rows(mix_in.astype(jnp.float32), mix_gain).astype(jnp.bfloat16)
    positions = jnp.arange(length, dtype=jnp.int32)
    cosine, sine_rows = angle_tables(positions)
    queries = jnp.dot(normed, query_weight, preferred_element_type=jnp.float32).reshape(length, HEADS, NOPE + ROPE)
    query_plain = queries[..., :NOPE].astype(jnp.bfloat16)
    query_turn = rotate_last(queries[..., NOPE:], cosine[:, None, :], sine_rows[:, None, :]).astype(jnp.bfloat16)
    latent = rms_rows(jnp.dot(normed, latent_weight, preferred_element_type=jnp.float32), latent_gain).astype(jnp.bfloat16)
    rotary_key = rotate_last(jnp.dot(normed, rotary_weight, preferred_element_type=jnp.float32), cosine, sine_rows).astype(jnp.bfloat16)
    key_rows = jnp.dot(latent, key_weight, preferred_element_type=jnp.float32).astype(jnp.bfloat16)
    key_rows = key_rows.reshape(length, HEADS, NOPE).astype(jnp.float32)
    value_rows = jnp.dot(latent, value_weight, preferred_element_type=jnp.float32).astype(jnp.bfloat16)
    value_rows = value_rows.reshape(length, HEADS, VD).astype(jnp.float32)
    rotary_wide = rotary_key.astype(jnp.float32)
    score_scale = (NOPE + ROPE) ** (-0.5)
    block_rows = math.gcd(length, 256)
    block_count = length // block_rows

    def attend(block_index):
        start_row = block_index * block_rows
        plain_block = lax.dynamic_slice_in_dim(query_plain, start_row, block_rows, 0).astype(jnp.float32)
        turn_block = lax.dynamic_slice_in_dim(query_turn, start_row, block_rows, 0).astype(jnp.float32)
        scores = jnp.einsum('ihd,jhd->hij', plain_block, key_rows)
        scores = scores + jnp.einsum('ihd,jd->hij', turn_block, rotary_wide)
        query_places = start_row + jnp.arange(block_rows, dtype=jnp.int32)
        allowed = positions[None, :] <= query_places[:, None]
        weights = jnp.where(allowed[None], jnp.exp(scores * score_scale), 0.0)
        totals = lax.optimization_barrier(jnp.sum(weights, axis=-1))
        weighted = jnp.einsum('hij,jhd->hid', rounded(weights), value_rows)
        return (weighted / totals[..., None]).astype(jnp.bfloat16)
    attended = lax.map(attend, jnp.arange(block_count))
    attended = attended.transpose(0, 2, 1, 3).reshape(length, HEADS, VD)
    group_heads = HEADS // N_TP
    projected = jnp.zeros((length, D), jnp.float32)
    for group in range(N_TP):
        head_block = attended[:, group * group_heads:(group + 1) * group_heads, :].reshape(length, group_heads * VD)
        weight_rows = output_weight[group * group_heads * VD:(group + 1) * group_heads * VD]
        projected = projected + rounded(jnp.dot(head_block, weight_rows, preferred_element_type=jnp.float32))
    return rms_rows(projected, out_gain).astype(jnp.bfloat16)

def expert_half(ffn_in, ffn_gain, gate_weight, up_weight, down_weight, routes, route_scores):
    row_count = ffn_in.shape[0]
    normed = rms_rows(ffn_in.astype(jnp.float32), ffn_gain).astype(jnp.bfloat16)
    padded = jnp.concatenate([normed, jnp.zeros((1, D), jnp.bfloat16)], axis=0)
    gate_share = jax.nn.softmax(route_scores.astype(jnp.float32), axis=-1).reshape(-1)
    gate_share = jnp.concatenate([gate_share, jnp.zeros((1,), jnp.float32)], axis=0)
    flat_routes = routes.reshape(-1)
    assignment_count = flat_routes.shape[0]
    capacity_all = MOST * (row_count // QB)
    unit_group = FF // N_TP

    def one_expert(totals, expert):
        matches = flat_routes == expert
        slot_rank = jnp.cumsum(matches.astype(jnp.int32)) - 1
        destination = jnp.where(matches, slot_rank, capacity_all).astype(jnp.int32)
        slot_of = jnp.full((capacity_all + 1,), assignment_count, jnp.int32)
        slot_of = slot_of.at[destination].set(jnp.arange(assignment_count, dtype=jnp.int32))[:capacity_all]
        token_of = slot_of // TOP
        gathered = padded[token_of]
        gate_part = jnp.dot(gathered, gate_weight[expert], preferred_element_type=jnp.float32)
        up_part = jnp.dot(gathered, up_weight[expert], preferred_element_type=jnp.float32)
        hidden = clamped_unit(gate_part, up_part).astype(jnp.bfloat16)
        expert_sum = jnp.zeros((capacity_all, D), jnp.float32)
        for group in range(N_TP):
            expert_sum = expert_sum + rounded(jnp.dot(hidden[:, group * unit_group:(group + 1) * unit_group], down_weight[expert][group * unit_group:(group + 1) * unit_group], preferred_element_type=jnp.float32))
        weighted = rounded(expert_sum) * gate_share[slot_of][:, None]
        totals = totals.at[token_of].add(weighted, mode='drop')
        return (totals, None)
    totals, _ = lax.scan(one_expert, jnp.zeros((row_count, D), jnp.float32), jnp.arange(EXPERTS, dtype=jnp.int32))
    return totals.astype(jnp.bfloat16)

def reference(mix_in, mix_gain, query_weight, latent_weight, rotary_weight, latent_gain, key_weight, value_weight, output_weight, out_gain, ffn_in, ffn_gain, gate_weight, up_weight, down_weight, routes, route_scores):
    mixed = mixer_half(mix_in, mix_gain, query_weight, latent_weight, rotary_weight, latent_gain, key_weight, value_weight, output_weight, out_gain)
    moe_out = expert_half(ffn_in, ffn_gain, gate_weight, up_weight, down_weight, routes, route_scores)
    return (mixed, moe_out)
```

```python
import jax
import jax.numpy as jnp
import numpy as np
from jax import lax
from jax.experimental import pallas as pl
from jax.experimental.pallas import tpu as pltpu
from jax.sharding import PartitionSpec as P

NOPE = 128
ROPE = 64
VD = 128
QB = 32
MOST = 4

norm_eps = 1e-06
clamp_limit = 7.0
gate_slope = 1.702
rope_base = 10000.0

MESH = pl.DeviceIdType.MESH
bf16 = jnp.bfloat16
f32 = jnp.float32

ORDER = (0, 1, 7, 2, 6, 3, 5, 4)


def iota(shape, dim):
    return lax.broadcasted_iota(jnp.int32, shape, dim)


def rms(rows, gain):
    mean_square = jnp.mean(rows * rows, axis=-1, keepdims=True)
    return rows * lax.rsqrt(mean_square + norm_eps) * gain


def drain(view, sem):
    pltpu.make_async_copy(view, view, sem).wait()


def kernel(
    NZ,
    J,
    TP,
    mix_in,
    mix_gain,
    query_weight,
    latent_weight,
    rotary_weight,
    latent_gain,
    key_weight,
    value_weight,
    output_weight,
    out_gain,
    ffn_in,
    ffn_gain,
    gate_weight,
    up_weight,
    down_weight,
    routes,
    route_scores,
    base_turn,
    row_turn,
    mixed_out,
    moe_out,
    mix_v,
    ffn_v,
    qw,
    lw,
    rw,
    kw,
    vw,
    ow,
    gw,
    uw,
    wd,
    outg,
    X,
    H,
    Dn,
    R,
    sel,
    w_hi,
    w_lo,
    m_send,
    m_recv,
    Q,
    KV,
    q_out,
    kv_out,
    Kc,
    Vc,
    o_out,
    t_out,
    o_in,
    t_in,
    p_out,
    p_in,
    load_sem,
    disp_recv,
    x_recv,
    h_recv,
    one_recv,
    send_sem,
):
    E = NZ * J
    e = lax.axis_index("ep")
    t = lax.axis_index("tp")
    z = e // J
    j = e % J
    rows = ffn_v.shape[0]
    width = outg.shape[1]
    cell = outg.shape[0] // E
    right = lax.rem(t + 1, TP)
    left = lax.rem(t + TP - 1, TP)
    unit = J * cell

    def load(src, dst, number):
        copy = pltpu.make_async_copy(src, dst, load_sem.at[number])
        copy.start()
        return copy

    def send(src, dst, s_sem, r_sem, ep, tp):
        pltpu.make_async_remote_copy(
            src_ref=src,
            dst_ref=dst,
            send_sem=s_sem,
            recv_sem=r_sem,
            device_id=(ep, tp),
            device_id_type=MESH,
        ).start()

    load_ffn = load(ffn_in, ffn_v, 0)
    load_mix = load(mix_in, mix_v, 1)
    load_q = load(query_weight, qw, 2)
    load_l = load(latent_weight, lw, 3)
    load_r = load(rotary_weight, rw, 4)
    load_k = load(key_weight, kw, 5)
    load_v = load(value_weight, vw, 6)
    load_g = load(gate_weight.at[0], gw, 7)
    load_u = load(up_weight.at[0], uw, 8)
    load_d = load(
        down_weight.at[0, :, pl.ds(pl.multiple_of(t * width, 128), width)], wd.at[t], 9
    )
    load_o = load(output_weight, ow, 10)

    barrier = pltpu.get_barrier_semaphore()

    @pl.loop(1, E)
    def _(step):
        pl.semaphore_signal(
            barrier, inc=1, device_id=(lax.rem(e + step, E), t), device_id_type=MESH
        )

    for step in range(1, TP):
        pl.semaphore_signal(
            barrier, inc=1, device_id=(e, lax.rem(t + step, TP)), device_id_type=MESH
        )

    slots = outg.shape[0]
    blocks = rows // QB
    slot = iota((1, slots), 1)
    slot_expert = slot // cell
    slot_block = (slot // MOST) % blocks
    slot_rank = (slot % MOST).astype(f32)
    row_block = iota((rows, 1), 0) // QB
    route = routes[...]
    choose = route.shape[1]
    named = jnp.zeros((rows, slots), f32)
    for k in range(choose):
        named = named + jnp.where(route[:, k : k + 1] == slot_expert, 1.0, 0.0)
    low_r = iota((rows, rows), 0)
    low_c = iota((rows, rows), 1)
    lower = jnp.where((low_c < low_r) & (low_c // QB == low_r // QB), 1.0, 0.0).astype(bf16)
    rank = jnp.dot(lower, named.astype(bf16), preferred_element_type=f32)
    picked = jnp.where((rank == slot_rank) & (row_block == slot_block), named, 0.0)
    sel[...] = picked.astype(bf16)

    load_ffn.wait()
    x = ffn_v[...].astype(f32)
    inverse = lax.rsqrt(jnp.mean(x * x, axis=-1, keepdims=True) + norm_eps)
    columns = pl.ds(pl.multiple_of(t * width, 128), width)
    normed_part = (ffn_v[:, columns].astype(f32) * inverse * ffn_gain[:, columns]).astype(bf16)
    outg[...] = lax.dot_general(
        sel[...], normed_part, (((0,), (0,)), ((), ())), preferred_element_type=f32
    ).astype(bf16)

    pl.semaphore_wait(barrier, E - 1 + TP - 1)

    my_rows = pl.ds(pl.multiple_of(e * cell, cell), cell)
    for number, dz in enumerate(ORDER):
        target_z = lax.rem(z + NZ - dz, NZ)

        @pl.loop(1 if dz == 0 else 0, J)
        def _(step, number=number, target_z=target_z):
            target = target_z * J + lax.rem(j + step, J)
            send(
                outg.at[pl.ds(pl.multiple_of(target * cell, cell), cell)],
                X.at[t, my_rows],
                send_sem.at[0],
                disp_recv.at[number],
                target,
                t,
            )

    X[t, my_rows] = outg[my_rows, :]

    for step in range(1, TP):
        peer = lax.rem(t + step, TP)
        send(
            down_weight.at[0, :, pl.ds(pl.multiple_of(peer * width, 128), width)],
            wd.at[t],
            send_sem.at[1],
            one_recv.at[0],
            e,
            peer,
        )

    load_mix.wait()
    normed = rms(mix_v[...].astype(f32), mix_gain[...]).astype(bf16)
    load_q.wait()
    queries = jnp.dot(normed, qw[...], preferred_element_type=f32)
    base = base_turn[pl.ds(e, 1), :]
    base_cos, base_sin = base[:, :128], base[:, 128:]
    row_cos, row_sin = row_turn[:, :128], row_turn[:, 128:]
    cosine = base_cos * row_cos - base_sin * row_sin
    sine = base_sin * row_cos + base_cos * row_sin
    lane = iota((rows, 128), 1)
    first_half = lane % ROPE < ROPE // 2
    sine = jnp.where(first_half, -sine, sine)

    def turned(v):
        partner = jnp.where(first_half, pltpu.roll(v, 96, 1), pltpu.roll(v, 32, 1))
        return v * cosine + partner * sine

    low_lanes = lane < 64
    A = [queries[:, 128 * i : 128 * (i + 1)] for i in range(6)]
    q_out[:, 0:128] = A[0].astype(bf16)
    q_out[:, 128:256] = pltpu.roll(jnp.where(low_lanes, A[2], A[1]), 64, 1).astype(bf16)
    q_out[:, 256:384] = A[3].astype(bf16)
    q_out[:, 384:512] = pltpu.roll(jnp.where(low_lanes, A[5], A[4]), 64, 1).astype(bf16)
    q_out[:, 512:640] = turned(jnp.where(low_lanes, A[1], A[2])).astype(bf16)
    q_out[:, 640:768] = turned(jnp.where(low_lanes, A[4], A[5])).astype(bf16)

    load_l.wait()
    latent = jnp.dot(normed, lw[...], preferred_element_type=f32)
    kv_out[:, 0:512] = rms(latent, latent_gain[...]).astype(bf16)
    load_r.wait()
    rotary = jnp.dot(normed, rw[...], preferred_element_type=f32)
    kv_out[:, 512:640] = turned(jnp.concatenate([rotary, rotary], axis=1)).astype(bf16)

    for step in range(1, J):
        send(
            q_out,
            Q.at[j],
            send_sem.at[2],
            one_recv.at[1],
            z * J + lax.rem(j + step, J),
            t,
        )
    for step in (1, 7, 2, 6, 3, 5, 4):
        send(
            kv_out,
            KV.at[z],
            send_sem.at[3],
            one_recv.at[2],
            lax.rem(z + step, NZ) * J + j,
            t,
        )
    Q[j] = q_out[...]
    KV[z] = kv_out[...]

    score = route_scores[...]
    grown = jnp.exp(score - jnp.max(score, axis=-1, keepdims=True))
    share = grown / jnp.sum(grown, axis=-1, keepdims=True)
    gates = jnp.zeros((rows, slots), f32)
    for k in range(choose):
        gates = gates + jnp.where(route[:, k : k + 1] == slot_expert, share[:, k : k + 1], 0.0)
    gates = gates * sel[...].astype(f32)
    gates_hi = gates.astype(bf16)
    w_hi[...] = gates_hi
    w_lo[...] = (gates - gates_hi.astype(f32)).astype(bf16)

    def unit_rows(number):
        source_z = lax.rem(z + ORDER[number], NZ)
        return pl.ds(pl.multiple_of(source_z * unit, unit), unit)

    def spread(buf, number, sems, base_send):
        place = unit_rows(number)
        send(buf.at[t, place], buf.at[t, place], send_sem.at[base_send], sems.at[0, number], e, right)
        send(buf.at[t, place], buf.at[t, place], send_sem.at[base_send], sems.at[1, number], e, left)

    def relay(buf, number, sems, base_send):
        place = unit_rows(number)
        drain(buf.at[left, place], sems.at[0, number])
        drain(buf.at[right, place], sems.at[1, number])
        if number % 2 == 0:
            send(
                buf.at[left, place],
                buf.at[left, place],
                send_sem.at[base_send + 1],
                sems.at[2, number],
                e,
                right,
            )
        else:
            send(
                buf.at[right, place],
                buf.at[right, place],
                send_sem.at[base_send + 1],
                sems.at[2, number],
                e,
                left,
            )

    def relayed(buf, number, sems):
        across = lax.rem(t + 2, TP)
        drain(buf.at[across, unit_rows(number)], sems.at[2, number])

    def take(number):
        if ORDER[number] == 0:
            drain(X.at[t, pl.ds(0, unit - cell)], disp_recv.at[number])
        else:
            drain(X.at[t, pl.ds(0, unit)], disp_recv.at[number])
        spread(X, number, x_recv, 4)

    def hidden(batch):
        pair = (2 * batch, 2 * batch + 1)
        for number in pair:
            relayed(X, number, x_recv)
        gate_part = jnp.zeros((2 * unit, gw.shape[1]), f32)
        up_part = jnp.zeros((2 * unit, gw.shape[1]), f32)
        for part in range(TP):
            block = jnp.concatenate([X[part, unit_rows(number)] for number in pair], axis=0)
            depth = pl.ds(part * width, width)
            gate_part = gate_part + jnp.dot(block, gw[depth, :], preferred_element_type=f32)
            up_part = up_part + jnp.dot(block, uw[depth, :], preferred_element_type=f32)
        gate_part = jnp.minimum(gate_part, clamp_limit)
        up_part = jnp.clip(up_part, -clamp_limit, clamp_limit)
        result = (gate_part * jax.nn.sigmoid(gate_slope * gate_part) * (up_part + 1.0)).astype(bf16)
        for i, number in enumerate(pair):
            H[t, unit_rows(number)] = result[i * unit : (i + 1) * unit]
        for number in pair:
            spread(H, number, h_recv, 6)

    def hidden_relay(batch):
        for number in (2 * batch, 2 * batch + 1):
            relay(H, number, h_recv, 6)

    def down(batch):
        pair = (2 * batch, 2 * batch + 1)
        for number in pair:
            relayed(H, number, h_recv)
        total = jnp.zeros((2 * unit, width), f32)
        for part in range(TP):
            block = jnp.concatenate([H[part, unit_rows(number)] for number in pair], axis=0)
            total = total + jnp.dot(block, wd[part], preferred_element_type=f32)
        total = total.astype(bf16)
        for i, number in enumerate(pair):
            Dn[unit_rows(number), :] = total[i * unit : (i + 1) * unit]
        for number in pair:
            source_z = lax.rem(z + ORDER[number], NZ)

            @pl.loop(1 if ORDER[number] == 0 else 0, J)
            def _(step, source_z=source_z):
                source = source_z * J + lax.rem(j + step, J)
                send(
                    Dn.at[pl.ds(pl.multiple_of(source * cell, cell), cell)],
                    R.at[my_rows],
                    send_sem.at[8],
                    one_recv.at[3],
                    source,
                    t,
                )

            if ORDER[number] == 0:
                R[my_rows, :] = Dn[my_rows, :]

    def expand():
        drain(Q.at[pl.ds(0, J - 1)], one_recv.at[1])
        drain(KV.at[pl.ds(0, NZ - 1)], one_recv.at[2])
        load_k.wait()
        load_v.wait()
        lat = KV[...].reshape(NZ * rows, 640)
        turn = lat[:, 512:640]
        keys = jnp.dot(lat[:, :512], kw[...], preferred_element_type=f32).astype(bf16)
        values = jnp.dot(lat[:, :512], vw[...], preferred_element_type=f32).astype(bf16)
        low = iota((NZ * rows, 128), 1) < 64
        zero = jnp.zeros_like(turn)
        even, odd = jnp.where(low, turn, zero), jnp.where(low, zero, turn)
        ones = jnp.ones_like(turn)
        for h in range(4):
            Kc[h, :, 0:128] = keys[:, 128 * h : 128 * (h + 1)]
            Kc[h, :, 128:256] = even if h % 2 == 0 else odd
            Vc[h, :, 0:128] = values[:, 128 * h : 128 * (h + 1)]
            Vc[h, :, 128:256] = ones

    scale = (NOPE + ROPE) ** (-0.5)

    def head(h):
        span = 2 * rows

        @pl.loop(0, J // 2)
        def _(chunk):
            plain = Q[pl.ds(2 * chunk, 2), :, 128 * h : 128 * (h + 1)].reshape(span, 128)
            pair = 512 + 128 * (h // 2)
            turn = Q[pl.ds(2 * chunk, 2), :, pair : pair + 128].reshape(span, 128)
            both = jnp.concatenate([plain, turn], axis=1)
            scores = lax.dot_general(
                both, Kc[h], (((1,), (1,)), ((), ())), preferred_element_type=f32
            )
            place = iota((1, NZ * rows), 1)
            key_place = (place // rows) * (J * rows) + j * rows + place % rows
            query_place = z * (J * rows) + chunk * span + iota((span, 1), 0)
            weights = jnp.where(key_place <= query_place, jnp.exp(scores * scale), 0.0).astype(bf16)
            both_out = jnp.dot(weights, Vc[h], preferred_element_type=f32)
            here = pl.ds(pl.multiple_of(chunk * span, span), span)
            o_out[here, 128 * h : 128 * (h + 1)] = both_out[:, :128].astype(bf16)
            sums = both_out[:, 128:]
            if h == 0:
                t_out[here, :] = sums
            else:
                lanes = iota((span, 128), 1)
                t_out[here, :] = jnp.where(lanes // 32 == h, sums, t_out[here, :])

    def give_back():
        for step in range(1, J):
            target = lax.rem(j + step, J)
            place = pl.ds(pl.multiple_of(target * rows, rows), rows)
            send(o_out.at[place], o_in.at[j], send_sem.at[9], one_recv.at[4], z * J + target, t)
            send(t_out.at[place], t_in.at[j], send_sem.at[10], one_recv.at[5], z * J + target, t)
        place = pl.ds(pl.multiple_of(j * rows, rows), rows)
        o_in[j] = o_out[place, :]
        t_in[j] = t_out[place, :]

    quarter = rows // TP

    def project():
        drain(o_in.at[pl.ds(0, J - 1)], one_recv.at[4])
        drain(t_in.at[pl.ds(0, J - 1)], one_recv.at[5])
        load_o.wait()
        osum = jnp.zeros((rows, 4 * VD), f32)
        tsum = jnp.zeros((rows, 128), f32)
        for i in range(J):
            osum = osum + o_in[i].astype(f32)
            tsum = tsum + t_in[i]
        heads = [
            (osum[:, VD * h : VD * (h + 1)] / tsum[:, 32 * h : 32 * h + 1]).astype(bf16)
            for h in range(4)
        ]
        attended = jnp.concatenate(heads, axis=1)
        p_out[...] = jnp.dot(attended, ow[...], preferred_element_type=f32).astype(bf16)
        for step in range(1, TP):
            peer = lax.rem(t + step, TP)
            place = pl.ds(pl.multiple_of(peer * quarter, quarter), quarter)
            send(p_out.at[place], p_in.at[t], send_sem.at[11], one_recv.at[6], e, peer)
        p_in[t] = p_out[pl.ds(pl.multiple_of(t * quarter, quarter), quarter), :]

    def finish_mixed():
        drain(p_in.at[pl.ds(0, TP - 1)], one_recv.at[6])
        projected = jnp.zeros((quarter, p_in.shape[2]), f32)
        for i in range(TP):
            projected = projected + p_in[i].astype(f32)
        mixed_out[...] = rms(projected, out_gain[...]).astype(bf16)

    take(0)
    take(1)
    relay(X, 0, x_recv, 4)
    take(2)
    relay(X, 1, x_recv, 4)
    take(3)
    relay(X, 2, x_recv, 4)
    load_g.wait()
    load_u.wait()
    hidden(0)
    take(4)
    relay(X, 3, x_recv, 4)
    take(5)
    relay(X, 4, x_recv, 4)
    hidden(1)
    hidden_relay(0)
    take(6)
    relay(X, 5, x_recv, 4)
    take(7)
    relay(X, 6, x_recv, 4)
    expand()
    hidden(2)
    relay(X, 7, x_recv, 4)
    hidden_relay(1)
    load_d.wait()
    drain(wd.at[pl.ds(0, TP - 1)], one_recv.at[0])
    down(0)
    head(0)
    hidden(3)
    hidden_relay(2)
    down(1)
    head(1)
    hidden_relay(3)
    down(2)
    head(2)
    down(3)
    head(3)
    give_back()
    project()
    finish_mixed()

    drain(R.at[pl.ds(0, slots - cell)], one_recv.at[3])
    total = jnp.dot(w_hi[...], R[...], preferred_element_type=f32)
    total = total + jnp.dot(w_lo[...], R[...], preferred_element_type=f32)
    m_send[...] = total.astype(bf16)
    for step in range(1, TP):
        peer = lax.rem(t + step, TP)
        place = pl.ds(pl.multiple_of(peer * quarter, quarter), quarter)
        send(m_send.at[place], m_recv.at[t], send_sem.at[12], one_recv.at[7], e, peer)
    m_recv[t] = m_send[pl.ds(pl.multiple_of(t * quarter, quarter), quarter), :]
    drain(m_recv.at[pl.ds(0, TP - 1)], one_recv.at[7])
    for i in range(TP):
        moe_out[:, i * width : (i + 1) * width] = m_recv[i]

    drain(outg.at[pl.ds(0, slots - cell)], send_sem.at[0])
    drain(wd.at[pl.ds(0, TP - 1)], send_sem.at[1])
    drain(Q.at[pl.ds(0, J - 1)], send_sem.at[2])
    drain(KV.at[pl.ds(0, NZ - 1)], send_sem.at[3])
    drain(X.at[pl.ds(0, 2)], send_sem.at[4])
    drain(X.at[0], send_sem.at[5])
    drain(H.at[pl.ds(0, 2)], send_sem.at[6])
    drain(H.at[0], send_sem.at[7])
    drain(Dn.at[pl.ds(0, slots - cell)], send_sem.at[8])
    drain(o_in.at[pl.ds(0, J - 1)], send_sem.at[9])
    drain(t_in.at[pl.ds(0, J - 1)], send_sem.at[10])
    drain(p_in.at[pl.ds(0, TP - 1)], send_sem.at[11])
    drain(m_recv.at[pl.ds(0, TP - 1)], send_sem.at[12])


def turn_tables(devices, rows):
    inverse = rope_base ** (-np.arange(0, ROPE, 2) / ROPE)
    inverse = np.tile(inverse, 4)[None, :]
    base = np.arange(devices)[:, None] * rows * inverse
    row = np.arange(rows)[:, None] * inverse
    return (
        np.concatenate([np.cos(base), np.sin(base)], axis=1).astype(np.float32),
        np.concatenate([np.cos(row), np.sin(row)], axis=1).astype(np.float32),
    )


def solution(mesh):
    EP, TP = mesh.shape["ep"], mesh.shape["tp"]
    J = 8
    NZ = EP // J
    placed = (
        P("ep", None),
        P(),
        P(None, "tp"),
        P(),
        P(),
        P(),
        P(None, "tp"),
        P(None, "tp"),
        P("tp", None),
        P(),
        P("ep", None),
        P(),
        P("ep", None, "tp"),
        P("ep", None, "tp"),
        P("ep", "tp", None),
        P("ep", None),
        P("ep", None),
    )

    def local(
        mix_in,
        mix_gain,
        query_weight,
        latent_weight,
        rotary_weight,
        latent_gain,
        key_weight,
        value_weight,
        output_weight,
        out_gain,
        ffn_in,
        ffn_gain,
        gate_weight,
        up_weight,
        down_weight,
        routes,
        route_scores,
    ):
        rows, D = mix_in.shape
        width = D // TP
        cell = MOST * (rows // QB)
        slots = EP * cell
        unit = gate_weight.shape[2]
        quarter = rows // TP
        base_turn, row_turn = turn_tables(EP, rows)
        hbm = pl.BlockSpec(memory_space=pl.ANY)
        vmem = pl.BlockSpec(memory_space=pltpu.VMEM)
        V = lambda *shape: pltpu.VMEM(shape, bf16)
        F = lambda *shape: pltpu.VMEM(shape, f32)
        S = pltpu.SemaphoreType.DMA

        def body(*refs):
            kernel(NZ, J, TP, *refs)

        out = jax.ShapeDtypeStruct((quarter, D), bf16)
        return pl.pallas_call(
            body,
            name="layer",
            out_shape=(out, out),
            in_specs=[
                hbm, vmem, hbm, hbm, hbm, vmem, hbm, hbm, hbm, vmem,
                hbm, vmem, hbm, hbm, hbm, vmem, vmem, vmem, vmem,
            ],
            out_specs=(vmem, vmem),
            scratch_shapes=[
                V(rows, D),
                V(rows, D),
                V(D, query_weight.shape[1]),
                V(D, latent_weight.shape[1]),
                V(D, ROPE),
                V(*key_weight.shape),
                V(*value_weight.shape),
                V(*output_weight.shape),
                V(D, unit),
                V(D, unit),
                V(TP, unit, width),
                V(slots, width),
                V(TP, slots, width),
                V(TP, slots, unit),
                V(slots, width),
                V(slots, width),
                V(rows, slots),
                V(rows, slots),
                V(rows, slots),
                V(rows, width),
                V(TP, quarter, width),
                V(J, rows, 768),
                V(NZ, rows, 640),
                V(rows, 768),
                V(rows, 640),
                V(4, NZ * rows, 256),
                V(4, NZ * rows, 256),
                V(J * rows, 512),
                F(J * rows, 128),
                V(J, rows, 512),
                F(J, rows, 128),
                V(rows, D),
                V(TP, quarter, D),
                S((11,)),
                S((8,)),
                S((3, 8)),
                S((3, 8)),
                S((8,)),
                S((13,)),
            ],
            compiler_params=pltpu.CompilerParams(
                collective_id=0, has_side_effects=True, vmem_limit_bytes=62 * 1024 * 1024
            ),
        )(
            mix_in,
            mix_gain[None, :],
            query_weight,
            latent_weight,
            rotary_weight,
            latent_gain[None, :],
            key_weight,
            value_weight,
            output_weight,
            out_gain[None, :],
            ffn_in,
            ffn_gain[None, :],
            gate_weight,
            up_weight,
            down_weight,
            routes,
            route_scores,
            base_turn,
            row_turn,
        )

    return jax.shard_map(
        local,
        mesh=mesh,
        in_specs=placed,
        out_specs=(P(("ep", "tp"), None), P(("ep", "tp"), None)),
        check_vma=False,
    )
```

```python
import jax
import jax.numpy as jnp
import numpy as np
from jax import lax
from jax.experimental import pallas as pl
from jax.experimental.pallas import tpu as pltpu
from jax.sharding import PartitionSpec as P

NOPE = 128
ROPE = 64
VD = 128
QB = 32
MOST = 4

norm_eps = 1e-06
clamp_limit = 7.0
gate_slope = 1.702
rope_base = 10000.0

MESH = pl.DeviceIdType.MESH
bf16 = jnp.bfloat16
f32 = jnp.float32

ORDER = (0, 1, 4, 3, 5, 6, 2, 7)


def iota(shape, dim):
    return lax.broadcasted_iota(jnp.int32, shape, dim)


def rms(rows, gain):
    mean_square = jnp.mean(rows * rows, axis=-1, keepdims=True)
    return rows * lax.rsqrt(mean_square + norm_eps) * gain


def drain(view, sem):
    with jax.named_scope("wait"):
        pltpu.make_async_copy(view, view, sem).wait()


def kernel(
    NZ,
    J,
    TP,
    mix_in,
    mix_gain,
    query_weight,
    latent_weight,
    rotary_weight,
    latent_gain,
    key_weight,
    value_weight,
    output_weight,
    out_gain,
    ffn_in,
    ffn_gain,
    gate_weight,
    up_weight,
    down_weight,
    routes,
    route_scores,
    base_turn,
    row_turn,
    mixed_out,
    moe_out,
    mix_v,
    ffn_v,
    qw,
    lw,
    rw,
    kw,
    vw,
    ow,
    gw,
    uw,
    wd,
    outg,
    near,
    X,
    H,
    Dn,
    R,
    sel,
    w_hi,
    w_lo,
    m_send,
    m_recv,
    Q,
    KV,
    q_out,
    Kc,
    Vc,
    o_out,
    t_out,
    t_row,
    o_in,
    t_in,
    p_out,
    p_in,
    load_sem,
    disp_recv,
    x_recv,
    h_recv,
    kv_recv,
    one_recv,
    send_sem,
):
    E = NZ * J
    e = lax.axis_index("ep")
    t = lax.axis_index("tp")
    z = e // J
    j = e % J
    rows = ffn_v.shape[0]
    width = outg.shape[1]
    cell = outg.shape[0] // E
    right = lax.rem(t + 1, TP)
    left = lax.rem(t + TP - 1, TP)
    unit = J * cell

    def load(src, dst, number):
        copy = pltpu.make_async_copy(src, dst, load_sem.at[number])
        copy.start()
        return copy

    def send(src, dst, s_sem, r_sem, ep, tp):
        pltpu.make_async_remote_copy(
            src_ref=src,
            dst_ref=dst,
            send_sem=s_sem,
            recv_sem=r_sem,
            device_id=(ep, tp),
            device_id_type=MESH,
        ).start()

    load_ffn = load(ffn_in, ffn_v, 0)
    load_mix = load(mix_in, mix_v, 1)
    load_q = load(query_weight, qw, 2)
    load_l = load(latent_weight, lw, 3)
    load_r = load(rotary_weight, rw, 4)
    load_k = load(key_weight, kw, 5)
    load_v = load(value_weight, vw, 6)
    load_g = load(gate_weight.at[0], gw, 7)
    load_u = load(up_weight.at[0], uw, 8)
    load_d = load(
        down_weight.at[0, :, pl.ds(pl.multiple_of(t * width, 128), width)], wd.at[t], 9
    )
    load_o = load(output_weight, ow, 10)

    barrier = pltpu.get_barrier_semaphore()

    for dz in (4, 3, 5, 2, 6, 1, 7, 0):

        @pl.loop(1 if dz == 0 else 0, J)
        def _(step, dz=dz):
            peer = lax.rem(z + dz, NZ) * J + lax.rem(j + step, J)
            pl.semaphore_signal(barrier, inc=1, device_id=(peer, t), device_id_type=MESH)

    for step in range(1, TP):
        pl.semaphore_signal(
            barrier, inc=1, device_id=(e, lax.rem(t + step, TP)), device_id_type=MESH
        )

    slots = outg.shape[0]
    blocks = rows // QB
    slot = iota((slots, 1), 0)
    slot_expert = slot // cell
    slot_block = (slot // MOST) % blocks
    slot_rank = (slot % MOST).astype(f32)
    row_block = iota((1, rows), 1) // QB
    route = routes[...]
    choose = route.shape[0]
    named = jnp.zeros((slots, rows), f32)
    for k in range(choose):
        named = named + jnp.where(route[k : k + 1, :] == slot_expert, 1.0, 0.0)
    up_r = iota((rows, rows), 0)
    up_c = iota((rows, rows), 1)
    upper = jnp.where((up_r < up_c) & (up_c // QB == up_r // QB), 1.0, 0.0).astype(bf16)
    rank = jnp.dot(named.astype(bf16), upper, preferred_element_type=f32)
    picked = jnp.where((rank == slot_rank) & (row_block == slot_block), named, 0.0)
    sel[...] = picked.astype(bf16)

    load_ffn.wait()
    ffn_v[...] = rms(ffn_v[...].astype(f32), ffn_gain[...]).astype(bf16)
    columns = pl.ds(pl.multiple_of(t * width, 128), width)
    outg[...] = jnp.dot(sel[...], ffn_v[:, columns], preferred_element_type=f32).astype(bf16)
    own_z = pl.ds(pl.multiple_of(z * unit, unit), unit)
    for part in range(TP):
        near[part] = jnp.dot(
            sel[own_z, :], ffn_v[:, part * width : (part + 1) * width], preferred_element_type=f32
        ).astype(bf16)

    base = base_turn[pl.ds(e, 1), :]
    base_cos, base_sin = base[:, :128], base[:, 128:]
    row_cos, row_sin = row_turn[:, :128], row_turn[:, 128:]
    cosine = base_cos * row_cos - base_sin * row_sin
    sine = base_sin * row_cos + base_cos * row_sin
    lane = iota((rows, 128), 1)
    first_half = lane % ROPE < ROPE // 2
    sine = jnp.where(first_half, -sine, sine)

    def turned(v):
        partner = jnp.where(first_half, pltpu.roll(v, 96, 1), pltpu.roll(v, 32, 1))
        return v * cosine + partner * sine

    load_mix.wait()
    mix_v[...] = rms(mix_v[...].astype(f32), mix_gain[...]).astype(bf16)
    load_l.wait()
    latent = jnp.dot(mix_v[...], lw[...], preferred_element_type=f32)
    KV[z, :, 0:512] = rms(latent, latent_gain[...]).astype(bf16)
    load_r.wait()
    rotary = lax.dot_general(
        mix_v[...], rw[...], (((1,), (1,)), ((), ())), preferred_element_type=f32
    )
    KV[z, :, 512:640] = turned(jnp.concatenate([rotary, rotary], axis=1)).astype(bf16)

    with jax.named_scope("barrier"):
        pl.semaphore_wait(barrier, E - 1 + TP - 1)

    for step in range(1, TP):
        peer = lax.rem(t + step, TP)
        send(
            down_weight.at[0, :, pl.ds(pl.multiple_of(peer * width, 128), width)],
            wd.at[t],
            send_sem.at[1],
            one_recv.at[0],
            e,
            peer,
        )

    my_rows = pl.ds(pl.multiple_of(e * cell, cell), cell)

    @pl.loop(1, J)
    def _(step):
        to = lax.rem(j + step, J)
        send(
            near.at[:, pl.ds(pl.multiple_of(to * cell, cell), cell)],
            X.at[:, my_rows],
            send_sem.at[0],
            disp_recv.at[0],
            z * J + to,
            t,
        )

    for part in range(TP):
        X[part, my_rows] = near[part, pl.ds(pl.multiple_of(j * cell, cell), cell)]

    def dispatch(number):
        target_z = lax.rem(z + NZ - ORDER[number], NZ)

        @pl.loop(0, J)
        def _(step):
            target = target_z * J + lax.rem(j + step, J)
            send(
                outg.at[pl.ds(pl.multiple_of(target * cell, cell), cell)],
                X.at[t, my_rows],
                send_sem.at[13],
                disp_recv.at[number],
                target,
                t,
            )

    up_z, down_z = lax.rem(z + 1, NZ), lax.rem(z + NZ - 1, NZ)
    half = rows // 2

    def pass_on(hop):
        if hop > 0:
            at_up, at_down = lax.rem(z + NZ - hop, NZ), lax.rem(z + hop, NZ)
            drain(KV.at[at_up], kv_recv.at[0, hop - 1])
            drain(KV.at[at_down], kv_recv.at[1, hop - 1])
        else:
            at_up = at_down = z
        upward, downward = KV.at[at_up], KV.at[at_down]
        if 2 * (hop + 1) == NZ:
            upward, downward = KV.at[at_up, pl.ds(0, half)], KV.at[at_down, pl.ds(half, half)]
        send(upward, upward, send_sem.at[3], kv_recv.at[0, hop], up_z * J + j, t)
        send(downward, downward, send_sem.at[3], kv_recv.at[1, hop], down_z * J + j, t)

    def latents_here():
        across = lax.rem(z + NZ // 2, NZ)
        drain(KV.at[across, pl.ds(0, half)], kv_recv.at[0, NZ // 2 - 1])
        drain(KV.at[across, pl.ds(half, half)], kv_recv.at[1, NZ // 2 - 1])

    pass_on(0)
    dispatch(1)

    load_q.wait()
    queries = jnp.dot(mix_v[...], qw[...], preferred_element_type=f32)
    low_lanes = lane < 64
    A = [queries[:, 128 * i : 128 * (i + 1)] for i in range(6)]
    q_out[:, 0:128] = A[0].astype(bf16)
    q_out[:, 128:256] = pltpu.roll(jnp.where(low_lanes, A[2], A[1]), 64, 1).astype(bf16)
    q_out[:, 256:384] = A[3].astype(bf16)
    q_out[:, 384:512] = pltpu.roll(jnp.where(low_lanes, A[5], A[4]), 64, 1).astype(bf16)
    q_out[:, 512:640] = turned(jnp.where(low_lanes, A[1], A[2])).astype(bf16)
    q_out[:, 640:768] = turned(jnp.where(low_lanes, A[4], A[5])).astype(bf16)
    Q[j] = q_out[...]
    mate = j + 1 - 2 * lax.rem(j, 2)
    for step in range(2, J, 2):
        send(Q.at[j], Q.at[j], send_sem.at[2], one_recv.at[1], z * J + lax.rem(j + step, J), t)
    send(Q.at[j], Q.at[j], send_sem.at[14], one_recv.at[8], z * J + mate, t)

    def share_queries():
        drain(Q.at[pl.ds(0, J // 2 - 1)], one_recv.at[1])
        for step in range(2, J, 2):
            from_j = lax.rem(j + step, J)
            send(Q.at[from_j], Q.at[from_j], send_sem.at[14], one_recv.at[8], z * J + mate, t)

    score = route_scores[...]
    grown = jnp.exp(score - jnp.max(score, axis=0, keepdims=True))
    share = grown / jnp.sum(grown, axis=0, keepdims=True)
    gates = jnp.zeros((slots, rows), f32)
    for k in range(choose):
        gates = gates + jnp.where(route[k : k + 1, :] == slot_expert, share[k : k + 1, :], 0.0)
    gates = jnp.transpose(gates * sel[...].astype(f32))
    gates_hi = gates.astype(bf16)
    w_hi[...] = gates_hi
    w_lo[...] = (gates - gates_hi.astype(f32)).astype(bf16)

    def unit_rows(number):
        source_z = lax.rem(z + ORDER[number], NZ)
        return pl.ds(pl.multiple_of(source_z * unit, unit), unit)

    def spread(buf, number, sems, base_send):
        place = unit_rows(number)
        send(buf.at[t, place], buf.at[t, place], send_sem.at[base_send], sems.at[0, number], e, right)
        send(buf.at[t, place], buf.at[t, place], send_sem.at[base_send], sems.at[1, number], e, left)

    def relay(buf, number, sems, base_send):
        place = unit_rows(number)
        drain(buf.at[left, place], sems.at[0, number])
        drain(buf.at[right, place], sems.at[1, number])
        if number % 2 == 0:
            send(
                buf.at[left, place],
                buf.at[left, place],
                send_sem.at[base_send + 1],
                sems.at[2, number],
                e,
                right,
            )
        else:
            send(
                buf.at[right, place],
                buf.at[right, place],
                send_sem.at[base_send + 1],
                sems.at[2, number],
                e,
                left,
            )

    def relayed(buf, number, sems):
        across = lax.rem(t + 2, TP)
        drain(buf.at[across, unit_rows(number)], sems.at[2, number])

    def take(number):
        if number == 0:
            drain(X.at[:, pl.ds(0, unit - cell)], disp_recv.at[0])
        else:
            drain(X.at[t, pl.ds(0, unit)], disp_recv.at[number])
            spread(X, number, x_recv, 4)

    def hidden(batch):
        pair = (2 * batch, 2 * batch + 1)
        for number in pair:
            if number > 0:
                relayed(X, number, x_recv)
        gate_part = jnp.zeros((2 * unit, gw.shape[1]), f32)
        up_part = jnp.zeros((2 * unit, gw.shape[1]), f32)
        for part in range(TP):
            block = jnp.concatenate([X[part, unit_rows(number)] for number in pair], axis=0)
            depth = pl.ds(part * width, width)
            gate_part = gate_part + jnp.dot(block, gw[depth, :], preferred_element_type=f32)
            up_part = up_part + jnp.dot(block, uw[depth, :], preferred_element_type=f32)
        gate_part = jnp.minimum(gate_part, clamp_limit)
        up_part = jnp.clip(up_part, -clamp_limit, clamp_limit)
        result = (gate_part * jax.nn.sigmoid(gate_slope * gate_part) * (up_part + 1.0)).astype(bf16)
        for i, number in enumerate(pair):
            H[t, unit_rows(number)] = result[i * unit : (i + 1) * unit]
        for number in pair:
            spread(H, number, h_recv, 6)

    def hidden_relay(batch):
        for number in (2 * batch, 2 * batch + 1):
            relay(H, number, h_recv, 6)

    def down(batch):
        pair = (2 * batch, 2 * batch + 1)
        for number in pair:
            relayed(H, number, h_recv)
        total = jnp.zeros((2 * unit, width), f32)
        for part in range(TP):
            block = jnp.concatenate([H[part, unit_rows(number)] for number in pair], axis=0)
            total = total + jnp.dot(block, wd[part], preferred_element_type=f32)
        total = total.astype(bf16)
        for i, number in enumerate(pair):
            Dn[unit_rows(number), :] = total[i * unit : (i + 1) * unit]
        for number in pair:
            source_z = lax.rem(z + ORDER[number], NZ)

            @pl.loop(1 if ORDER[number] == 0 else 0, J)
            def _(step, source_z=source_z):
                source = source_z * J + lax.rem(j + step, J)
                send(
                    Dn.at[pl.ds(pl.multiple_of(source * cell, cell), cell)],
                    R.at[my_rows],
                    send_sem.at[8],
                    one_recv.at[3],
                    source,
                    t,
                )

            if ORDER[number] == 0:
                R[my_rows, :] = Dn[my_rows, :]

    def expand():
        drain(Q.at[pl.ds(0, J // 2)], one_recv.at[8])
        latents_here()
        load_k.wait()
        load_v.wait()
        lat = KV[...].reshape(NZ * rows, 640)
        turn = lat[:, 512:640]
        keys = jnp.dot(lat[:, :512], kw[...], preferred_element_type=f32).astype(bf16)
        values = jnp.dot(lat[:, :512], vw[...], preferred_element_type=f32).astype(bf16)
        low = iota((NZ * rows, 128), 1) < 64
        zero = jnp.zeros_like(turn)
        even, odd = jnp.where(low, turn, zero), jnp.where(low, zero, turn)
        ones = jnp.ones_like(turn)
        for h in range(4):
            Kc[h, :, 0:128] = keys[:, 128 * h : 128 * (h + 1)]
            Kc[h, :, 128:256] = even if h % 2 == 0 else odd
            Vc[h, :, 0:128] = values[:, 128 * h : 128 * (h + 1)]
            Vc[h, :, 128:256] = ones

    scale = (NOPE + ROPE) ** (-0.5)

    def head(h):
        span = 2 * rows

        @pl.loop(0, J // 2)
        def _(chunk):
            plain = Q[pl.ds(2 * chunk, 2), :, 128 * h : 128 * (h + 1)].reshape(span, 128)
            pair = 512 + 128 * (h // 2)
            turn = Q[pl.ds(2 * chunk, 2), :, pair : pair + 128].reshape(span, 128)
            both = jnp.concatenate([plain, turn], axis=1)
            scores = lax.dot_general(
                both, Kc[h], (((1,), (1,)), ((), ())), preferred_element_type=f32
            )
            place = iota((1, NZ * rows), 1)
            key_place = (place // rows) * (J * rows) + j * rows + place % rows
            query_place = z * (J * rows) + chunk * span + iota((span, 1), 0)
            weights = jnp.where(key_place <= query_place, jnp.exp(scores * scale), 0.0).astype(bf16)
            both_out = jnp.dot(weights, Vc[h], preferred_element_type=f32)
            here = pl.ds(pl.multiple_of(chunk * span, span), span)
            o_out[here, 128 * h : 128 * (h + 1)] = both_out[:, :128].astype(bf16)
            sums = both_out[:, 128:]
            if h == 0:
                t_out[here, :] = sums
            else:
                lanes = iota((span, 128), 1)
                t_out[here, :] = jnp.where(lanes // 32 == h, sums, t_out[here, :])

    def give_back():
        for i in range(J):
            across = jnp.transpose(t_out[i * rows : (i + 1) * rows, :])
            picks = [across[32 * h : 32 * h + 1, :] for h in range(4)]
            t_row[i] = jnp.concatenate(picks + picks, axis=0)
        for step in (4, 2, 6, 3, 5, 1, 7):
            target = lax.rem(j + step, J)
            place = pl.ds(pl.multiple_of(target * rows, rows), rows)
            send(o_out.at[place], o_in.at[j], send_sem.at[9], one_recv.at[4], z * J + target, t)
            send(t_row.at[target], t_in.at[j], send_sem.at[10], one_recv.at[5], z * J + target, t)
        o_in[j] = o_out[pl.ds(pl.multiple_of(j * rows, rows), rows), :]
        t_in[j] = t_row[j]

    quarter = rows // TP

    def project():
        drain(o_in.at[pl.ds(0, J - 1)], one_recv.at[4])
        drain(t_in.at[pl.ds(0, J - 1)], one_recv.at[5])
        load_o.wait()
        osum = jnp.zeros((rows, 4 * VD), f32)
        tsum = jnp.zeros(t_in.shape[1:], f32)
        for i in range(J):
            osum = osum + o_in[i].astype(f32)
            tsum = tsum + t_in[i]
        tsum = jnp.transpose(jnp.concatenate([tsum] * (128 // tsum.shape[0]), axis=0))
        heads = [
            (osum[:, VD * h : VD * (h + 1)] / tsum[:, h : h + 1]).astype(bf16)
            for h in range(4)
        ]
        attended = jnp.concatenate(heads, axis=1)
        p_out[...] = jnp.dot(attended, ow[...], preferred_element_type=f32).astype(bf16)
        for step in range(1, TP):
            peer = lax.rem(t + step, TP)
            place = pl.ds(pl.multiple_of(peer * quarter, quarter), quarter)
            send(p_out.at[place], p_in.at[t], send_sem.at[11], one_recv.at[6], e, peer)
        p_in[t] = p_out[pl.ds(pl.multiple_of(t * quarter, quarter), quarter), :]

    def finish_mixed():
        drain(p_in.at[pl.ds(0, TP - 1)], one_recv.at[6])
        projected = jnp.zeros((quarter, p_in.shape[2]), f32)
        for i in range(TP):
            projected = projected + p_in[i].astype(f32)
        mixed_out[...] = rms(projected, out_gain[...]).astype(bf16)

    with jax.named_scope("s00_pass_on_1"):
        pass_on(1)
    with jax.named_scope("s01_dispatch_2"):
        dispatch(2)
    with jax.named_scope("s02_take_0"):
        take(0)
    with jax.named_scope("s03_take_1"):
        take(1)
    with jax.named_scope("s04_pass_on_2"):
        pass_on(2)
    with jax.named_scope("s05_dispatch_3"):
        dispatch(3)
    with jax.named_scope("s06_dispatch_4"):
        dispatch(4)
    with jax.named_scope("s07_share_queries_"):
        share_queries()
    with jax.named_scope("s08_relay_X_1"):
        relay(X, 1, x_recv, 4)
    with jax.named_scope("s09_take_2"):
        take(2)
    with jax.named_scope("s10_load_gu_"):
        load_g.wait()
        load_u.wait()
    with jax.named_scope("s11_hidden_0"):
        hidden(0)
    with jax.named_scope("s12_pass_on_3"):
        pass_on(3)
    with jax.named_scope("s13_dispatch_5"):
        dispatch(5)
    with jax.named_scope("s14_dispatch_6"):
        dispatch(6)
    with jax.named_scope("s15_dispatch_7"):
        dispatch(7)
    with jax.named_scope("s16_relay_X_2"):
        relay(X, 2, x_recv, 4)
    with jax.named_scope("s17_hidden_relay_0"):
        hidden_relay(0)
    with jax.named_scope("s18_take_3"):
        take(3)
    with jax.named_scope("s19_take_4"):
        take(4)
    with jax.named_scope("s20_relay_X_3"):
        relay(X, 3, x_recv, 4)
    with jax.named_scope("s21_expand_"):
        expand()
    with jax.named_scope("s22_relay_X_4"):
        relay(X, 4, x_recv, 4)
    with jax.named_scope("s23_hidden_1"):
        hidden(1)
    with jax.named_scope("s24_head_0"):
        head(0)
    with jax.named_scope("s25_take_5"):
        take(5)
    with jax.named_scope("s26_load_dd_"):
        load_d.wait()
        drain(wd.at[pl.ds(0, TP - 1)], one_recv.at[0])
    with jax.named_scope("s27_down_0"):
        down(0)
    with jax.named_scope("s28_head_1"):
        head(1)
    with jax.named_scope("s29_take_6"):
        take(6)
    with jax.named_scope("s30_relay_X_5"):
        relay(X, 5, x_recv, 4)
    with jax.named_scope("s31_hidden_relay_1"):
        hidden_relay(1)
    with jax.named_scope("s32_head_2"):
        head(2)
    with jax.named_scope("s33_take_7"):
        take(7)
    with jax.named_scope("s34_relay_X_6"):
        relay(X, 6, x_recv, 4)
    with jax.named_scope("s35_hidden_2"):
        hidden(2)
    with jax.named_scope("s36_down_1"):
        down(1)
    with jax.named_scope("s37_head_3"):
        head(3)
    with jax.named_scope("s38_relay_X_7"):
        relay(X, 7, x_recv, 4)
    with jax.named_scope("s39_hidden_relay_2"):
        hidden_relay(2)
    with jax.named_scope("s40_give_back_"):
        give_back()
    with jax.named_scope("s41_hidden_3"):
        hidden(3)
    with jax.named_scope("s42_down_2"):
        down(2)
    with jax.named_scope("s43_hidden_relay_3"):
        hidden_relay(3)
    with jax.named_scope("s44_project_"):
        project()
    with jax.named_scope("s45_down_3"):
        down(3)
    with jax.named_scope("s46_finish_mixed_"):
        finish_mixed()

    with jax.named_scope("returns"):
        drain(R.at[pl.ds(0, slots - cell)], one_recv.at[3])
    total = jnp.dot(w_hi[...], R[...], preferred_element_type=f32)
    total = total + jnp.dot(w_lo[...], R[...], preferred_element_type=f32)
    m_send[...] = total.astype(bf16)
    for step in range(1, TP):
        peer = lax.rem(t + step, TP)
        place = pl.ds(pl.multiple_of(peer * quarter, quarter), quarter)
        send(m_send.at[place], m_recv.at[t], send_sem.at[12], one_recv.at[7], e, peer)
    m_recv[t] = m_send[pl.ds(pl.multiple_of(t * quarter, quarter), quarter), :]
    with jax.named_scope("last"):
        drain(m_recv.at[pl.ds(0, TP - 1)], one_recv.at[7])
    for i in range(TP):
        moe_out[:, i * width : (i + 1) * width] = m_recv[i]

    most = slots - unit
    drain(X.at[:, pl.ds(0, unit - cell)], send_sem.at[0])
    drain(outg.at[pl.ds(0, most)], send_sem.at[13])
    drain(wd.at[pl.ds(0, TP - 1)], send_sem.at[1])
    drain(Q.at[pl.ds(0, J // 2 - 1)], send_sem.at[2])
    drain(Q.at[pl.ds(0, J // 2)], send_sem.at[14])
    drain(KV.at[pl.ds(0, NZ - 1)], send_sem.at[3])
    drain(X.at[pl.ds(0, 2), pl.ds(0, most)], send_sem.at[4])
    drain(X.at[0, pl.ds(0, most)], send_sem.at[5])
    drain(H.at[pl.ds(0, 2)], send_sem.at[6])
    drain(H.at[0], send_sem.at[7])
    drain(Dn.at[pl.ds(0, slots - cell)], send_sem.at[8])
    drain(o_in.at[pl.ds(0, J - 1)], send_sem.at[9])
    drain(t_in.at[pl.ds(0, J - 1)], send_sem.at[10])
    drain(p_in.at[pl.ds(0, TP - 1)], send_sem.at[11])
    drain(m_recv.at[pl.ds(0, TP - 1)], send_sem.at[12])


def turn_tables(devices, rows):
    inverse = rope_base ** (-np.arange(0, ROPE, 2) / ROPE)
    inverse = np.tile(inverse, 4)[None, :]
    base = np.arange(devices)[:, None] * rows * inverse
    row = np.arange(rows)[:, None] * inverse
    return (
        np.concatenate([np.cos(base), np.sin(base)], axis=1).astype(np.float32),
        np.concatenate([np.cos(row), np.sin(row)], axis=1).astype(np.float32),
    )


def solution(mesh):
    EP, TP = mesh.shape["ep"], mesh.shape["tp"]
    J = 8
    NZ = EP // J
    placed = (
        P("ep", None),
        P(),
        P(None, "tp"),
        P(),
        P(),
        P(),
        P(None, "tp"),
        P(None, "tp"),
        P("tp", None),
        P(),
        P("ep", None),
        P(),
        P("ep", None, "tp"),
        P("ep", None, "tp"),
        P("ep", "tp", None),
        P("ep", None),
        P("ep", None),
    )

    def local(
        mix_in,
        mix_gain,
        query_weight,
        latent_weight,
        rotary_weight,
        latent_gain,
        key_weight,
        value_weight,
        output_weight,
        out_gain,
        ffn_in,
        ffn_gain,
        gate_weight,
        up_weight,
        down_weight,
        routes,
        route_scores,
    ):
        rows, D = mix_in.shape
        width = D // TP
        cell = MOST * (rows // QB)
        slots = EP * cell
        unit = gate_weight.shape[2]
        quarter = rows // TP
        base_turn, row_turn = turn_tables(EP, rows)
        hbm = pl.BlockSpec(memory_space=pl.ANY)
        vmem = pl.BlockSpec(memory_space=pltpu.VMEM)
        V = lambda *shape: pltpu.VMEM(shape, bf16)
        F = lambda *shape: pltpu.VMEM(shape, f32)
        S = pltpu.SemaphoreType.DMA

        def body(*refs):
            kernel(NZ, J, TP, *refs)

        out = jax.ShapeDtypeStruct((quarter, D), bf16)
        return pl.pallas_call(
            body,
            name="layer",
            out_shape=(out, out),
            in_specs=[
                hbm, vmem, hbm, hbm, hbm, vmem, hbm, hbm, hbm, vmem,
                hbm, vmem, hbm, hbm, hbm, vmem, vmem, vmem, vmem,
            ],
            out_specs=(vmem, vmem),
            scratch_shapes=[
                V(rows, D),
                V(rows, D),
                V(D, query_weight.shape[1]),
                V(D, latent_weight.shape[1]),
                V(ROPE, D),
                V(*key_weight.shape),
                V(*value_weight.shape),
                V(*output_weight.shape),
                V(D, unit),
                V(D, unit),
                V(TP, unit, width),
                V(slots, width),
                V(TP, J * cell, width),
                V(TP, slots, width),
                V(TP, slots, unit),
                V(slots, width),
                V(slots, width),
                V(slots, rows),
                V(rows, slots),
                V(rows, slots),
                V(rows, width),
                V(TP, quarter, width),
                V(J, rows, 768),
                V(NZ, rows, 640),
                V(rows, 768),
                V(4, NZ * rows, 256),
                V(4, NZ * rows, 256),
                V(J * rows, 512),
                F(J * rows, 128),
                F(J, 8, rows),
                V(J, rows, 512),
                F(J, 8, rows),
                V(rows, D),
                V(TP, quarter, D),
                S((11,)),
                S((8,)),
                S((3, 8)),
                S((3, 8)),
                S((2, NZ // 2)),
                S((9,)),
                S((15,)),
            ],
            compiler_params=pltpu.CompilerParams(
                collective_id=0, has_side_effects=True, vmem_limit_bytes=62 * 1024 * 1024
            ),
        )(
            mix_in,
            mix_gain[None, :],
            query_weight,
            latent_weight,
            rotary_weight.T,
            latent_gain[None, :],
            key_weight,
            value_weight,
            output_weight,
            out_gain[None, :],
            ffn_in,
            ffn_gain[None, :],
            gate_weight,
            up_weight,
            down_weight,
            routes.T,
            route_scores.T,
            base_turn,
            row_turn,
        )

    return jax.shard_map(
        local,
        mesh=mesh,
        in_specs=placed,
        out_specs=(P(("ep", "tp"), None), P(("ep", "tp"), None)),
        check_vma=False,
    )
```

```python
import jax
import jax.numpy as jnp
import numpy as np
from jax import lax
from jax.experimental import pallas as pl
from jax.experimental.pallas import tpu as pltpu
from jax.sharding import PartitionSpec as P

NOPE = 128
ROPE = 64
VD = 128
QB = 32
MOST = 4

norm_eps = 1e-06
clamp_limit = 7.0
gate_slope = 1.702
rope_base = 10000.0

MESH = pl.DeviceIdType.MESH
bf16 = jnp.bfloat16
f32 = jnp.float32

ORDER = (0, 4, 3, 5, 2, 6, 1, 7)


def iota(shape, dim):
    return lax.broadcasted_iota(jnp.int32, shape, dim)


def rms(rows, gain):
    mean_square = jnp.mean(rows * rows, axis=-1, keepdims=True)
    return rows * lax.rsqrt(mean_square + norm_eps) * gain


def drain(view, sem):
    with jax.named_scope("wait"):
        pltpu.make_async_copy(view, view, sem).wait()


def kernel(
    NZ,
    J,
    TP,
    mix_in,
    mix_gain,
    query_weight,
    latent_weight,
    rotary_weight,
    latent_gain,
    key_weight,
    value_weight,
    output_weight,
    out_gain,
    ffn_in,
    ffn_gain,
    gate_weight,
    up_weight,
    down_weight,
    routes,
    route_scores,
    base_turn,
    row_turn,
    mixed_out,
    moe_out,
    mix_v,
    ffn_v,
    qw,
    lw,
    rw,
    kw,
    vw,
    ow,
    gw,
    uw,
    wd,
    outg,
    near,
    X,
    H,
    Dn,
    R,
    sel,
    w_hi,
    w_lo,
    m_send,
    m_recv,
    Q,
    KV,
    q_out,
    Kc,
    Vc,
    o_out,
    t_out,
    t_row,
    o_in,
    t_in,
    p_out,
    p_in,
    load_sem,
    disp_recv,
    x_recv,
    h_recv,
    kv_recv,
    one_recv,
    send_sem,
):
    E = NZ * J
    e = lax.axis_index("ep")
    t = lax.axis_index("tp")
    z = e // J
    j = e % J
    rows = ffn_v.shape[0]
    width = outg.shape[1]
    cell = outg.shape[0] // E
    right = lax.rem(t + 1, TP)
    left = lax.rem(t + TP - 1, TP)
    unit = J * cell

    def load(src, dst, number):
        copy = pltpu.make_async_copy(src, dst, load_sem.at[number])
        copy.start()
        return copy

    def send(src, dst, s_sem, r_sem, ep, tp):
        pltpu.make_async_remote_copy(
            src_ref=src,
            dst_ref=dst,
            send_sem=s_sem,
            recv_sem=r_sem,
            device_id=(ep, tp),
            device_id_type=MESH,
        ).start()

    load_ffn = load(ffn_in, ffn_v, 0)
    load_mix = load(mix_in, mix_v, 1)
    load_q = load(query_weight, qw, 2)
    load_l = load(latent_weight, lw, 3)
    load_r = load(rotary_weight, rw, 4)
    load_k = load(key_weight, kw, 5)
    load_v = load(value_weight, vw, 6)
    load_g = load(gate_weight.at[0], gw, 7)
    load_u = load(up_weight.at[0], uw, 8)
    load_d = load(
        down_weight.at[0, :, pl.ds(pl.multiple_of(t * width, 128), width)], wd.at[t], 9
    )
    load_o = load(output_weight, ow, 10)

    barrier = pltpu.get_barrier_semaphore()

    for dz in (4, 3, 5, 2, 6, 1, 7, 0):

        @pl.loop(1 if dz == 0 else 0, J)
        def _(step, dz=dz):
            peer = lax.rem(z + dz, NZ) * J + lax.rem(j + step, J)
            pl.semaphore_signal(barrier, inc=1, device_id=(peer, t), device_id_type=MESH)

    for step in range(1, TP):
        pl.semaphore_signal(
            barrier, inc=1, device_id=(e, lax.rem(t + step, TP)), device_id_type=MESH
        )

    slots = outg.shape[0]
    blocks = rows // QB
    slot = iota((slots, 1), 0)
    slot_expert = slot // cell
    slot_block = (slot // MOST) % blocks
    slot_rank = (slot % MOST).astype(f32)
    row_block = iota((1, rows), 1) // QB
    route = routes[...]
    choose = route.shape[0]
    named = jnp.zeros((slots, rows), f32)
    for k in range(choose):
        named = named + jnp.where(route[k : k + 1, :] == slot_expert, 1.0, 0.0)
    up_r = iota((rows, rows), 0)
    up_c = iota((rows, rows), 1)
    upper = jnp.where((up_r < up_c) & (up_c // QB == up_r // QB), 1.0, 0.0).astype(bf16)
    rank = jnp.dot(named.astype(bf16), upper, preferred_element_type=f32)
    picked = jnp.where((rank == slot_rank) & (row_block == slot_block), named, 0.0)
    sel[...] = picked.astype(bf16)

    load_ffn.wait()
    ffn_v[...] = rms(ffn_v[...].astype(f32), ffn_gain[...]).astype(bf16)
    columns = pl.ds(pl.multiple_of(t * width, 128), width)
    outg[...] = jnp.dot(sel[...], ffn_v[:, columns], preferred_element_type=f32).astype(bf16)
    own_z = pl.ds(pl.multiple_of(z * unit, unit), unit)
    for part in range(TP):
        near[part] = jnp.dot(
            sel[own_z, :], ffn_v[:, part * width : (part + 1) * width], preferred_element_type=f32
        ).astype(bf16)

    base = base_turn[pl.ds(e, 1), :]
    base_cos, base_sin = base[:, :128], base[:, 128:]
    row_cos, row_sin = row_turn[:, :128], row_turn[:, 128:]
    cosine = base_cos * row_cos - base_sin * row_sin
    sine = base_sin * row_cos + base_cos * row_sin
    lane = iota((rows, 128), 1)
    first_half = lane % ROPE < ROPE // 2
    sine = jnp.where(first_half, -sine, sine)

    def turned(v):
        partner = jnp.where(first_half, pltpu.roll(v, 96, 1), pltpu.roll(v, 32, 1))
        return v * cosine + partner * sine

    with jax.named_scope("barrier"):
        pl.semaphore_wait(barrier, E - 1 + TP - 1)

    for step in range(1, TP):
        peer = lax.rem(t + step, TP)
        send(
            down_weight.at[0, :, pl.ds(pl.multiple_of(peer * width, 128), width)],
            wd.at[t],
            send_sem.at[1],
            one_recv.at[0],
            e,
            peer,
        )

    my_rows = pl.ds(pl.multiple_of(e * cell, cell), cell)

    @pl.loop(1, J)
    def _(step):
        to = lax.rem(j + step, J)
        send(
            near.at[:, pl.ds(pl.multiple_of(to * cell, cell), cell)],
            X.at[:, my_rows],
            send_sem.at[0],
            disp_recv.at[0],
            z * J + to,
            t,
        )

    for part in range(TP):
        X[part, my_rows] = near[part, pl.ds(pl.multiple_of(j * cell, cell), cell)]

    def dispatch(number):
        target_z = lax.rem(z + NZ - ORDER[number], NZ)

        @pl.loop(0, J)
        def _(step):
            target = target_z * J + lax.rem(j + step, J)
            send(
                outg.at[pl.ds(pl.multiple_of(target * cell, cell), cell)],
                X.at[t, my_rows],
                send_sem.at[13],
                disp_recv.at[number],
                target,
                t,
            )

    up_z, down_z = lax.rem(z + 1, NZ), lax.rem(z + NZ - 1, NZ)
    half = rows // 2

    def pass_on(hop):
        if hop > 0:
            at_up, at_down = lax.rem(z + NZ - hop, NZ), lax.rem(z + hop, NZ)
            drain(KV.at[at_up], kv_recv.at[0, hop - 1])
            drain(KV.at[at_down], kv_recv.at[1, hop - 1])
        else:
            at_up = at_down = z
        upward, downward = KV.at[at_up], KV.at[at_down]
        if 2 * (hop + 1) == NZ:
            upward, downward = KV.at[at_up, pl.ds(0, half)], KV.at[at_down, pl.ds(half, half)]
        send(upward, upward, send_sem.at[3], kv_recv.at[0, hop], up_z * J + j, t)
        send(downward, downward, send_sem.at[3], kv_recv.at[1, hop], down_z * J + j, t)

    def latents_here():
        across = lax.rem(z + NZ // 2, NZ)
        drain(KV.at[across, pl.ds(0, half)], kv_recv.at[0, NZ // 2 - 1])
        drain(KV.at[across, pl.ds(half, half)], kv_recv.at[1, NZ // 2 - 1])

    dispatch(1)
    load_mix.wait()
    mix_v[...] = rms(mix_v[...].astype(f32), mix_gain[...]).astype(bf16)
    load_l.wait()
    latent = jnp.dot(mix_v[...], lw[...], preferred_element_type=f32)
    KV[z, :, 0:512] = rms(latent, latent_gain[...]).astype(bf16)
    load_r.wait()
    rotary = lax.dot_general(
        mix_v[...], rw[...], (((1,), (1,)), ((), ())), preferred_element_type=f32
    )
    KV[z, :, 512:640] = turned(jnp.concatenate([rotary, rotary], axis=1)).astype(bf16)

    pass_on(0)
    dispatch(2)

    load_q.wait()
    queries = jnp.dot(mix_v[...], qw[...], preferred_element_type=f32)
    low_lanes = lane < 64
    A = [queries[:, 128 * i : 128 * (i + 1)] for i in range(6)]
    q_out[:, 0:128] = A[0].astype(bf16)
    q_out[:, 128:256] = pltpu.roll(jnp.where(low_lanes, A[2], A[1]), 64, 1).astype(bf16)
    q_out[:, 256:384] = A[3].astype(bf16)
    q_out[:, 384:512] = pltpu.roll(jnp.where(low_lanes, A[5], A[4]), 64, 1).astype(bf16)
    q_out[:, 512:640] = turned(jnp.where(low_lanes, A[1], A[2])).astype(bf16)
    q_out[:, 640:768] = turned(jnp.where(low_lanes, A[4], A[5])).astype(bf16)
    Q[j] = q_out[...]
    mate = j + 1 - 2 * lax.rem(j, 2)
    for step in range(2, J, 2):
        send(Q.at[j], Q.at[j], send_sem.at[2], one_recv.at[1], z * J + lax.rem(j + step, J), t)
    send(Q.at[j], Q.at[j], send_sem.at[14], one_recv.at[8], z * J + mate, t)

    def share_queries():
        drain(Q.at[pl.ds(0, J // 2 - 1)], one_recv.at[1])
        for step in range(2, J, 2):
            from_j = lax.rem(j + step, J)
            send(Q.at[from_j], Q.at[from_j], send_sem.at[14], one_recv.at[8], z * J + mate, t)

    score = route_scores[...]
    grown = jnp.exp(score - jnp.max(score, axis=0, keepdims=True))
    share = grown / jnp.sum(grown, axis=0, keepdims=True)
    gates = jnp.zeros((slots, rows), f32)
    for k in range(choose):
        gates = gates + jnp.where(route[k : k + 1, :] == slot_expert, share[k : k + 1, :], 0.0)
    gates = jnp.transpose(gates * sel[...].astype(f32))
    gates_hi = gates.astype(bf16)
    w_hi[...] = gates_hi
    w_lo[...] = (gates - gates_hi.astype(f32)).astype(bf16)

    def unit_rows(number):
        source_z = lax.rem(z + ORDER[number], NZ)
        return pl.ds(pl.multiple_of(source_z * unit, unit), unit)

    def spread(buf, number, sems, base_send):
        place = unit_rows(number)
        send(buf.at[t, place], buf.at[t, place], send_sem.at[base_send], sems.at[0, number], e, right)
        send(buf.at[t, place], buf.at[t, place], send_sem.at[base_send], sems.at[1, number], e, left)

    def relay(buf, number, sems, base_send):
        place = unit_rows(number)
        drain(buf.at[left, place], sems.at[0, number])
        drain(buf.at[right, place], sems.at[1, number])
        if number % 2 == 0:
            send(
                buf.at[left, place],
                buf.at[left, place],
                send_sem.at[base_send + 1],
                sems.at[2, number],
                e,
                right,
            )
        else:
            send(
                buf.at[right, place],
                buf.at[right, place],
                send_sem.at[base_send + 1],
                sems.at[2, number],
                e,
                left,
            )

    def relayed(buf, number, sems):
        across = lax.rem(t + 2, TP)
        drain(buf.at[across, unit_rows(number)], sems.at[2, number])

    def take(number):
        if number == 0:
            drain(X.at[:, pl.ds(0, unit - cell)], disp_recv.at[0])
        else:
            drain(X.at[t, pl.ds(0, unit)], disp_recv.at[number])
            spread(X, number, x_recv, 4)

    def hidden(batch):
        pair = (2 * batch, 2 * batch + 1)
        for number in pair:
            if number > 0:
                relayed(X, number, x_recv)
        gate_part = jnp.zeros((2 * unit, gw.shape[1]), f32)
        up_part = jnp.zeros((2 * unit, gw.shape[1]), f32)
        for part in range(TP):
            block = jnp.concatenate([X[part, unit_rows(number)] for number in pair], axis=0)
            depth = pl.ds(part * width, width)
            gate_part = gate_part + jnp.dot(block, gw[depth, :], preferred_element_type=f32)
            up_part = up_part + jnp.dot(block, uw[depth, :], preferred_element_type=f32)
        gate_part = jnp.minimum(gate_part, clamp_limit)
        up_part = jnp.clip(up_part, -clamp_limit, clamp_limit)
        result = (gate_part * jax.nn.sigmoid(gate_slope * gate_part) * (up_part + 1.0)).astype(bf16)
        for i, number in enumerate(pair):
            H[t, unit_rows(number)] = result[i * unit : (i + 1) * unit]
        for number in pair:
            spread(H, number, h_recv, 6)

    def hidden_relay(batch):
        for number in (2 * batch, 2 * batch + 1):
            relay(H, number, h_recv, 6)

    def down(batch):
        pair = (2 * batch, 2 * batch + 1)
        for number in pair:
            relayed(H, number, h_recv)
        total = jnp.zeros((2 * unit, width), f32)
        for part in range(TP):
            block = jnp.concatenate([H[part, unit_rows(number)] for number in pair], axis=0)
            total = total + jnp.dot(block, wd[part], preferred_element_type=f32)
        total = total.astype(bf16)
        for i, number in enumerate(pair):
            Dn[unit_rows(number), :] = total[i * unit : (i + 1) * unit]
        for number in pair:
            source_z = lax.rem(z + ORDER[number], NZ)

            @pl.loop(1 if ORDER[number] == 0 else 0, J)
            def _(step, source_z=source_z):
                source = source_z * J + lax.rem(j + step, J)
                send(
                    Dn.at[pl.ds(pl.multiple_of(source * cell, cell), cell)],
                    R.at[my_rows],
                    send_sem.at[8],
                    one_recv.at[3],
                    source,
                    t,
                )

            if ORDER[number] == 0:
                R[my_rows, :] = Dn[my_rows, :]

    def expand():
        drain(Q.at[pl.ds(0, J // 2)], one_recv.at[8])
        latents_here()
        load_k.wait()
        load_v.wait()
        lat = KV[...].reshape(NZ * rows, 640)
        turn = lat[:, 512:640]
        keys = jnp.dot(lat[:, :512], kw[...], preferred_element_type=f32).astype(bf16)
        values = jnp.dot(lat[:, :512], vw[...], preferred_element_type=f32).astype(bf16)
        low = iota((NZ * rows, 128), 1) < 64
        zero = jnp.zeros_like(turn)
        even, odd = jnp.where(low, turn, zero), jnp.where(low, zero, turn)
        ones = jnp.ones_like(turn)
        for h in range(4):
            Kc[h, :, 0:128] = keys[:, 128 * h : 128 * (h + 1)]
            Kc[h, :, 128:256] = even if h % 2 == 0 else odd
            Vc[h, :, 0:128] = values[:, 128 * h : 128 * (h + 1)]
            Vc[h, :, 128:256] = ones

    scale = (NOPE + ROPE) ** (-0.5)

    def head(h):
        span = 2 * rows

        @pl.loop(0, J // 2)
        def _(chunk):
            plain = Q[pl.ds(2 * chunk, 2), :, 128 * h : 128 * (h + 1)].reshape(span, 128)
            pair = 512 + 128 * (h // 2)
            turn = Q[pl.ds(2 * chunk, 2), :, pair : pair + 128].reshape(span, 128)
            both = jnp.concatenate([plain, turn], axis=1)
            scores = lax.dot_general(
                both, Kc[h], (((1,), (1,)), ((), ())), preferred_element_type=f32
            )
            place = iota((1, NZ * rows), 1)
            key_place = (place // rows) * (J * rows) + j * rows + place % rows
            query_place = z * (J * rows) + chunk * span + iota((span, 1), 0)
            weights = jnp.where(key_place <= query_place, jnp.exp(scores * scale), 0.0).astype(bf16)
            both_out = jnp.dot(weights, Vc[h], preferred_element_type=f32)
            here = pl.ds(pl.multiple_of(chunk * span, span), span)
            o_out[h, here, :] = both_out[:, :128].astype(bf16)
            sums = both_out[:, 128:]
            if h == 0:
                t_out[here, :] = sums
            else:
                lanes = iota((span, 128), 1)
                t_out[here, :] = jnp.where(lanes // 32 == h, sums, t_out[here, :])

    back_order = (4, 2, 6, 3, 5, 1, 7)

    def give_back(h):
        for step in back_order:
            target = lax.rem(j + step, J)
            place = pl.ds(pl.multiple_of(target * rows, rows), rows)
            send(o_out.at[h, place], o_in.at[h, j], send_sem.at[9], one_recv.at[4], z * J + target, t)
        o_in[h, j] = o_out[h, pl.ds(pl.multiple_of(j * rows, rows), rows), :]

    def give_totals():
        for i in range(J):
            across = jnp.transpose(t_out[i * rows : (i + 1) * rows, :])
            picks = [across[32 * h : 32 * h + 1, :] for h in range(4)]
            t_row[i] = jnp.concatenate(picks + picks, axis=0)
        for step in back_order:
            target = lax.rem(j + step, J)
            send(t_row.at[target], t_in.at[j], send_sem.at[10], one_recv.at[5], z * J + target, t)
        t_in[j] = t_row[j]

    quarter = rows // TP

    def project():
        drain(o_in.at[:, pl.ds(0, J - 1)], one_recv.at[4])
        drain(t_in.at[pl.ds(0, J - 1)], one_recv.at[5])
        load_o.wait()
        tsum = jnp.zeros(t_in.shape[1:], f32)
        for i in range(J):
            tsum = tsum + t_in[i]
        tsum = jnp.transpose(jnp.concatenate([tsum] * (128 // tsum.shape[0]), axis=0))
        heads = []
        for h in range(4):
            osum = jnp.zeros((rows, VD), f32)
            for i in range(J):
                osum = osum + o_in[h, i].astype(f32)
            heads.append((osum / tsum[:, h : h + 1]).astype(bf16))
        attended = jnp.concatenate(heads, axis=1)
        p_out[...] = jnp.dot(attended, ow[...], preferred_element_type=f32).astype(bf16)
        for step in range(1, TP):
            peer = lax.rem(t + step, TP)
            place = pl.ds(pl.multiple_of(peer * quarter, quarter), quarter)
            send(p_out.at[place], p_in.at[t], send_sem.at[11], one_recv.at[6], e, peer)
        p_in[t] = p_out[pl.ds(pl.multiple_of(t * quarter, quarter), quarter), :]

    def finish_mixed():
        drain(p_in.at[pl.ds(0, TP - 1)], one_recv.at[6])
        projected = jnp.zeros((quarter, p_in.shape[2]), f32)
        for i in range(TP):
            projected = projected + p_in[i].astype(f32)
        mixed_out[...] = rms(projected, out_gain[...]).astype(bf16)

    with jax.named_scope("s00_dispatch_7"):
        dispatch(7)
    with jax.named_scope("s01_dispatch_3"):
        dispatch(3)
    with jax.named_scope("s02_dispatch_4"):
        dispatch(4)
    with jax.named_scope("s03_pass_on_1"):
        pass_on(1)
    with jax.named_scope("s04_take_1"):
        take(1)
    with jax.named_scope("s05_relay_X_1"):
        relay(X, 1, x_recv, 4)
    with jax.named_scope("s06_take_7"):
        take(7)
    with jax.named_scope("s07_dispatch_6"):
        dispatch(6)
    with jax.named_scope("s08_dispatch_5"):
        dispatch(5)
    with jax.named_scope("s09_take_0"):
        take(0)
    with jax.named_scope("s10_take_2"):
        take(2)
    with jax.named_scope("s11_take_3"):
        take(3)
    with jax.named_scope("s12_pass_on_2"):
        pass_on(2)
    with jax.named_scope("s13_load_gu_"):
        load_g.wait()
        load_u.wait()
    with jax.named_scope("s14_hidden_0"):
        hidden(0)
    with jax.named_scope("s15_relay_X_3"):
        relay(X, 3, x_recv, 4)
    with jax.named_scope("s16_relay_X_2"):
        relay(X, 2, x_recv, 4)
    with jax.named_scope("s17_pass_on_3"):
        pass_on(3)
    with jax.named_scope("s18_take_5"):
        take(5)
    with jax.named_scope("s19_hidden_1"):
        hidden(1)
    with jax.named_scope("s20_take_4"):
        take(4)
    with jax.named_scope("s21_share_queries_"):
        share_queries()
    with jax.named_scope("s22_expand_"):
        expand()
    with jax.named_scope("s23_hidden_relay_1"):
        hidden_relay(1)
    with jax.named_scope("s24_hidden_relay_0"):
        hidden_relay(0)
    with jax.named_scope("s25_head_0"):
        head(0)
    with jax.named_scope("s26_give_back_0"):
        give_back(0)
    with jax.named_scope("s27_relay_X_4"):
        relay(X, 4, x_recv, 4)
    with jax.named_scope("s28_relay_X_5"):
        relay(X, 5, x_recv, 4)
    with jax.named_scope("s29_take_6"):
        take(6)
    with jax.named_scope("s30_load_dd_"):
        load_d.wait()
        drain(wd.at[pl.ds(0, TP - 1)], one_recv.at[0])
    with jax.named_scope("s31_down_1"):
        down(1)
    with jax.named_scope("s32_head_1"):
        head(1)
    with jax.named_scope("s33_give_back_1"):
        give_back(1)
    with jax.named_scope("s34_down_0"):
        down(0)
    with jax.named_scope("s35_hidden_2"):
        hidden(2)
    with jax.named_scope("s36_head_2"):
        head(2)
    with jax.named_scope("s37_give_back_2"):
        give_back(2)
    with jax.named_scope("s38_relay_X_6"):
        relay(X, 6, x_recv, 4)
    with jax.named_scope("s39_relay_X_7"):
        relay(X, 7, x_recv, 4)
    with jax.named_scope("s40_hidden_relay_2"):
        hidden_relay(2)
    with jax.named_scope("s41_head_3"):
        head(3)
    with jax.named_scope("s42_give_back_3"):
        give_back(3)
    with jax.named_scope("s43_give_totals_"):
        give_totals()
    with jax.named_scope("s44_hidden_3"):
        hidden(3)
    with jax.named_scope("s45_down_2"):
        down(2)
    with jax.named_scope("s46_hidden_relay_3"):
        hidden_relay(3)
    with jax.named_scope("s47_project_"):
        project()
    with jax.named_scope("s48_down_3"):
        down(3)
    with jax.named_scope("s49_finish_mixed_"):
        finish_mixed()

    with jax.named_scope("returns"):
        drain(R.at[pl.ds(0, slots - cell)], one_recv.at[3])
    total = jnp.dot(w_hi[...], R[...], preferred_element_type=f32)
    total = total + jnp.dot(w_lo[...], R[...], preferred_element_type=f32)
    m_send[...] = total.astype(bf16)
    for step in range(1, TP):
        peer = lax.rem(t + step, TP)
        place = pl.ds(pl.multiple_of(peer * quarter, quarter), quarter)
        send(m_send.at[place], m_recv.at[t], send_sem.at[12], one_recv.at[7], e, peer)
    m_recv[t] = m_send[pl.ds(pl.multiple_of(t * quarter, quarter), quarter), :]
    with jax.named_scope("last"):
        drain(m_recv.at[pl.ds(0, TP - 1)], one_recv.at[7])
    for i in range(TP):
        moe_out[:, i * width : (i + 1) * width] = m_recv[i]

    most = slots - unit
    drain(X.at[:, pl.ds(0, unit - cell)], send_sem.at[0])
    drain(outg.at[pl.ds(0, most)], send_sem.at[13])
    drain(wd.at[pl.ds(0, TP - 1)], send_sem.at[1])
    drain(Q.at[pl.ds(0, J // 2 - 1)], send_sem.at[2])
    drain(Q.at[pl.ds(0, J // 2)], send_sem.at[14])
    drain(KV.at[pl.ds(0, NZ - 1)], send_sem.at[3])
    drain(X.at[pl.ds(0, 2), pl.ds(0, most)], send_sem.at[4])
    drain(X.at[0, pl.ds(0, most)], send_sem.at[5])
    drain(H.at[pl.ds(0, 2)], send_sem.at[6])
    drain(H.at[0], send_sem.at[7])
    drain(Dn.at[pl.ds(0, slots - cell)], send_sem.at[8])
    drain(o_in.at[:, pl.ds(0, J - 1)], send_sem.at[9])
    drain(t_in.at[pl.ds(0, J - 1)], send_sem.at[10])
    drain(p_in.at[pl.ds(0, TP - 1)], send_sem.at[11])
    drain(m_recv.at[pl.ds(0, TP - 1)], send_sem.at[12])


def turn_tables(devices, rows):
    inverse = rope_base ** (-np.arange(0, ROPE, 2) / ROPE)
    inverse = np.tile(inverse, 4)[None, :]
    base = np.arange(devices)[:, None] * rows * inverse
    row = np.arange(rows)[:, None] * inverse
    return (
        np.concatenate([np.cos(base), np.sin(base)], axis=1).astype(np.float32),
        np.concatenate([np.cos(row), np.sin(row)], axis=1).astype(np.float32),
    )


def solution(mesh):
    EP, TP = mesh.shape["ep"], mesh.shape["tp"]
    J = 8
    NZ = EP // J
    placed = (
        P("ep", None),
        P(),
        P(None, "tp"),
        P(),
        P(),
        P(),
        P(None, "tp"),
        P(None, "tp"),
        P("tp", None),
        P(),
        P("ep", None),
        P(),
        P("ep", None, "tp"),
        P("ep", None, "tp"),
        P("ep", "tp", None),
        P("ep", None),
        P("ep", None),
    )

    def local(
        mix_in,
        mix_gain,
        query_weight,
        latent_weight,
        rotary_weight,
        latent_gain,
        key_weight,
        value_weight,
        output_weight,
        out_gain,
        ffn_in,
        ffn_gain,
        gate_weight,
        up_weight,
        down_weight,
        routes,
        route_scores,
    ):
        rows, D = mix_in.shape
        width = D // TP
        cell = MOST * (rows // QB)
        slots = EP * cell
        unit = gate_weight.shape[2]
        quarter = rows // TP
        base_turn, row_turn = turn_tables(EP, rows)
        hbm = pl.BlockSpec(memory_space=pl.ANY)
        vmem = pl.BlockSpec(memory_space=pltpu.VMEM)
        V = lambda *shape: pltpu.VMEM(shape, bf16)
        F = lambda *shape: pltpu.VMEM(shape, f32)
        S = pltpu.SemaphoreType.DMA

        def body(*refs):
            kernel(NZ, J, TP, *refs)

        out = jax.ShapeDtypeStruct((quarter, D), bf16)
        return pl.pallas_call(
            body,
            name="layer",
            out_shape=(out, out),
            in_specs=[
                hbm, vmem, hbm, hbm, hbm, vmem, hbm, hbm, hbm, vmem,
                hbm, vmem, hbm, hbm, hbm, vmem, vmem, vmem, vmem,
            ],
            out_specs=(vmem, vmem),
            scratch_shapes=[
                V(rows, D),
                V(rows, D),
                V(D, query_weight.shape[1]),
                V(D, latent_weight.shape[1]),
                V(ROPE, D),
                V(*key_weight.shape),
                V(*value_weight.shape),
                V(*output_weight.shape),
                V(D, unit),
                V(D, unit),
                V(TP, unit, width),
                V(slots, width),
                V(TP, J * cell, width),
                V(TP, slots, width),
                V(TP, slots, unit),
                V(slots, width),
                V(slots, width),
                V(slots, rows),
                V(rows, slots),
                V(rows, slots),
                V(rows, width),
                V(TP, quarter, width),
                V(J, rows, 768),
                V(NZ, rows, 640),
                V(rows, 768),
                V(4, NZ * rows, 256),
                V(4, NZ * rows, 256),
                V(4, J * rows, VD),
                F(J * rows, 128),
                F(J, 8, rows),
                V(4, J, rows, VD),
                F(J, 8, rows),
                V(rows, D),
                V(TP, quarter, D),
                S((11,)),
                S((8,)),
                S((3, 8)),
                S((3, 8)),
                S((2, NZ // 2)),
                S((9,)),
                S((15,)),
            ],
            compiler_params=pltpu.CompilerParams(
                collective_id=0, has_side_effects=True, vmem_limit_bytes=62 * 1024 * 1024
            ),
        )(
            mix_in,
            mix_gain[None, :],
            query_weight,
            latent_weight,
            rotary_weight.T,
            latent_gain[None, :],
            key_weight,
            value_weight,
            output_weight,
            out_gain[None, :],
            ffn_in,
            ffn_gain[None, :],
            gate_weight,
            up_weight,
            down_weight,
            routes.T,
            route_scores.T,
            base_turn,
            row_turn,
        )

    return jax.shard_map(
        local,
        mesh=mesh,
        in_specs=placed,
        out_specs=(P(("ep", "tp"), None), P(("ep", "tp"), None)),
        check_vma=False,
    )
```

```python
import jax
import jax.numpy as jnp
import numpy as np
from jax import lax
from jax.experimental import pallas as pl
from jax.experimental.pallas import tpu as pltpu
from jax.sharding import PartitionSpec as P

NOPE = 128
ROPE = 64
VD = 128
QB = 32
MOST = 4

norm_eps = 1e-06
clamp_limit = 7.0
gate_slope = 1.702
rope_base = 10000.0

MESH = pl.DeviceIdType.MESH
bf16 = jnp.bfloat16
f32 = jnp.float32

ORDER = (0, 4, 3, 5, 2, 6, 1, 7)

BATCHES = ((0, 1), (2, 3), (4, 5), (6,), (7,))
DIRECT = (7,)


def iota(shape, dim):
    return lax.broadcasted_iota(jnp.int32, shape, dim)


def rms(rows, gain):
    mean_square = jnp.mean(rows * rows, axis=-1, keepdims=True)
    return rows * lax.rsqrt(mean_square + norm_eps) * gain


def drain(view, sem):
    with jax.named_scope("wait"):
        pltpu.make_async_copy(view, view, sem).wait()


def kernel(
    NZ,
    J,
    TP,
    mix_in,
    mix_gain,
    query_weight,
    latent_weight,
    rotary_weight,
    latent_gain,
    key_weight,
    value_weight,
    output_weight,
    out_gain,
    ffn_in,
    ffn_gain,
    gate_weight,
    up_weight,
    down_weight,
    routes,
    route_scores,
    base_turn,
    row_turn,
    mixed_out,
    moe_out,
    mix_v,
    ffn_v,
    qw,
    lw,
    rw,
    kw,
    vw,
    ow,
    gw,
    uw,
    wd,
    outg,
    near,
    X,
    H,
    Dn,
    R,
    sel,
    w_hi,
    w_lo,
    m_send,
    m_recv,
    Q,
    KV,
    q_out,
    Kc,
    Vc,
    o_out,
    t_out,
    t_row,
    o_in,
    t_in,
    p_out,
    p_in,
    load_sem,
    disp_recv,
    x_recv,
    h_recv,
    kv_recv,
    one_recv,
    send_sem,
):
    E = NZ * J
    e = lax.axis_index("ep")
    t = lax.axis_index("tp")
    z = e // J
    j = e % J
    rows = ffn_v.shape[0]
    width = outg.shape[1]
    cell = outg.shape[0] // E
    right = lax.rem(t + 1, TP)
    left = lax.rem(t + TP - 1, TP)
    unit = J * cell

    def load(src, dst, number):
        copy = pltpu.make_async_copy(src, dst, load_sem.at[number])
        copy.start()
        return copy

    def send(src, dst, s_sem, r_sem, ep, tp):
        pltpu.make_async_remote_copy(
            src_ref=src,
            dst_ref=dst,
            send_sem=s_sem,
            recv_sem=r_sem,
            device_id=(ep, tp),
            device_id_type=MESH,
        ).start()

    load_ffn = load(ffn_in, ffn_v, 0)
    load_mix = load(mix_in, mix_v, 1)
    load_q = load(query_weight, qw, 2)
    load_l = load(latent_weight, lw, 3)
    load_r = load(rotary_weight, rw, 4)
    load_k = load(key_weight, kw, 5)
    load_v = load(value_weight, vw, 6)
    load_g = load(gate_weight.at[0], gw, 7)
    load_u = load(up_weight.at[0], uw, 8)
    load_d = load(
        down_weight.at[0, :, pl.ds(pl.multiple_of(t * width, 128), width)], wd.at[t], 9
    )
    load_o = load(output_weight, ow, 10)

    barrier = pltpu.get_barrier_semaphore()

    for dz in (4, 3, 5, 2, 6, 1, 7, 0):

        @pl.loop(1 if dz == 0 else 0, J)
        def _(step, dz=dz):
            peer = lax.rem(z + dz, NZ) * J + lax.rem(j + step, J)
            pl.semaphore_signal(barrier, inc=1, device_id=(peer, t), device_id_type=MESH)

    for step in range(1, TP):
        pl.semaphore_signal(
            barrier, inc=1, device_id=(e, lax.rem(t + step, TP)), device_id_type=MESH
        )

    slots = outg.shape[0]
    blocks = rows // QB
    slot = iota((slots, 1), 0)
    slot_expert = slot // cell
    slot_block = (slot // MOST) % blocks
    slot_rank = (slot % MOST).astype(f32)
    row_block = iota((1, rows), 1) // QB
    route = routes[...]
    choose = route.shape[0]
    named = jnp.zeros((slots, rows), f32)
    for k in range(choose):
        named = named + jnp.where(route[k : k + 1, :] == slot_expert, 1.0, 0.0)
    up_r = iota((rows, rows), 0)
    up_c = iota((rows, rows), 1)
    upper = jnp.where((up_r < up_c) & (up_c // QB == up_r // QB), 1.0, 0.0).astype(bf16)
    rank = jnp.dot(named.astype(bf16), upper, preferred_element_type=f32)
    picked = jnp.where((rank == slot_rank) & (row_block == slot_block), named, 0.0)
    sel[...] = picked.astype(bf16)

    load_ffn.wait()
    ffn_v[...] = rms(ffn_v[...].astype(f32), ffn_gain[...]).astype(bf16)
    columns = pl.ds(pl.multiple_of(t * width, 128), width)
    outg[...] = jnp.dot(sel[...], ffn_v[:, columns], preferred_element_type=f32).astype(bf16)
    own_z = pl.ds(pl.multiple_of(z * unit, unit), unit)
    for part in range(TP):
        near[part] = jnp.dot(
            sel[own_z, :], ffn_v[:, part * width : (part + 1) * width], preferred_element_type=f32
        ).astype(bf16)

    base = base_turn[pl.ds(e, 1), :]
    base_cos, base_sin = base[:, :128], base[:, 128:]
    row_cos, row_sin = row_turn[:, :128], row_turn[:, 128:]
    cosine = base_cos * row_cos - base_sin * row_sin
    sine = base_sin * row_cos + base_cos * row_sin
    lane = iota((rows, 128), 1)
    first_half = lane % ROPE < ROPE // 2
    sine = jnp.where(first_half, -sine, sine)

    def turned(v):
        partner = jnp.where(first_half, pltpu.roll(v, 96, 1), pltpu.roll(v, 32, 1))
        return v * cosine + partner * sine

    with jax.named_scope("barrier"):
        pl.semaphore_wait(barrier, E - 1 + TP - 1)

    def share_down(step):
        peer = lax.rem(t + step, TP)
        send(
            down_weight.at[0, :, pl.ds(pl.multiple_of(peer * width, 128), width)],
            wd.at[t],
            send_sem.at[1],
            one_recv.at[0],
            e,
            peer,
        )

    share_down(1)
    share_down(TP - 1)

    my_rows = pl.ds(pl.multiple_of(e * cell, cell), cell)

    @pl.loop(1, J)
    def _(step):
        to = lax.rem(j + step, J)
        send(
            near.at[:, pl.ds(pl.multiple_of(to * cell, cell), cell)],
            X.at[:, my_rows],
            send_sem.at[0],
            disp_recv.at[0],
            z * J + to,
            t,
        )

    for part in range(TP):
        X[part, my_rows] = near[part, pl.ds(pl.multiple_of(j * cell, cell), cell)]

    def dispatch(number):
        target_z = lax.rem(z + NZ - ORDER[number], NZ)

        @pl.loop(0, J)
        def _(step):
            target = target_z * J + lax.rem(j + step, J)
            send(
                outg.at[pl.ds(pl.multiple_of(target * cell, cell), cell)],
                X.at[t, my_rows],
                send_sem.at[13],
                disp_recv.at[number],
                target,
                t,
            )

    up_z, down_z = lax.rem(z + 1, NZ), lax.rem(z + NZ - 1, NZ)
    half = rows // 2

    def pass_on(hop):
        if hop > 0:
            at_up, at_down = lax.rem(z + NZ - hop, NZ), lax.rem(z + hop, NZ)
            drain(KV.at[at_up], kv_recv.at[0, hop - 1])
            drain(KV.at[at_down], kv_recv.at[1, hop - 1])
        else:
            at_up = at_down = z
        upward, downward = KV.at[at_up], KV.at[at_down]
        if 2 * (hop + 1) == NZ:
            upward, downward = KV.at[at_up, pl.ds(0, half)], KV.at[at_down, pl.ds(half, half)]
        send(upward, upward, send_sem.at[3], kv_recv.at[0, hop], up_z * J + j, t)
        send(downward, downward, send_sem.at[3], kv_recv.at[1, hop], down_z * J + j, t)

    def latents_here():
        across = lax.rem(z + NZ // 2, NZ)
        drain(KV.at[across, pl.ds(0, half)], kv_recv.at[0, NZ // 2 - 1])
        drain(KV.at[across, pl.ds(half, half)], kv_recv.at[1, NZ // 2 - 1])

    def own_norm():
        load_mix.wait()
        mix_v[...] = rms(mix_v[...].astype(f32), mix_gain[...]).astype(bf16)

    def own_latents():
        load_l.wait()
        latent = jnp.dot(mix_v[...], lw[...], preferred_element_type=f32)
        KV[z, :, 0:512] = rms(latent, latent_gain[...]).astype(bf16)
        load_r.wait()
        rotary = lax.dot_general(
            mix_v[...], rw[...], (((1,), (1,)), ((), ())), preferred_element_type=f32
        )
        KV[z, :, 512:640] = turned(jnp.concatenate([rotary, rotary], axis=1)).astype(bf16)

        pass_on(0)

    mate = j + 1 - 2 * lax.rem(j, 2)

    def own_queries():
        load_q.wait()
        queries = jnp.dot(mix_v[...], qw[...], preferred_element_type=f32)
        low_lanes = lane < 64
        A = [queries[:, 128 * i : 128 * (i + 1)] for i in range(6)]
        q_out[:, 0:128] = A[0].astype(bf16)
        q_out[:, 128:256] = pltpu.roll(jnp.where(low_lanes, A[2], A[1]), 64, 1).astype(bf16)
        q_out[:, 256:384] = A[3].astype(bf16)
        q_out[:, 384:512] = pltpu.roll(jnp.where(low_lanes, A[5], A[4]), 64, 1).astype(bf16)
        q_out[:, 512:640] = turned(jnp.where(low_lanes, A[1], A[2])).astype(bf16)
        q_out[:, 640:768] = turned(jnp.where(low_lanes, A[4], A[5])).astype(bf16)
        Q[j] = q_out[...]
        for step in range(2, J, 2):
            send(Q.at[j], Q.at[j], send_sem.at[2], one_recv.at[1], z * J + lax.rem(j + step, J), t)
        send(Q.at[j], Q.at[j], send_sem.at[14], one_recv.at[8], z * J + mate, t)

    def share_queries():
        drain(Q.at[pl.ds(0, J // 2 - 1)], one_recv.at[1])
        for step in range(2, J, 2):
            from_j = lax.rem(j + step, J)
            send(Q.at[from_j], Q.at[from_j], send_sem.at[14], one_recv.at[8], z * J + mate, t)

    def weigh():
        score = route_scores[...]
        grown = jnp.exp(score - jnp.max(score, axis=0, keepdims=True))
        share = grown / jnp.sum(grown, axis=0, keepdims=True)
        gates = jnp.zeros((slots, rows), f32)
        for k in range(choose):
            gates = gates + jnp.where(route[k : k + 1, :] == slot_expert, share[k : k + 1, :], 0.0)
        gates = jnp.transpose(gates * sel[...].astype(f32))
        gates_hi = gates.astype(bf16)
        w_hi[...] = gates_hi
        w_lo[...] = (gates - gates_hi.astype(f32)).astype(bf16)

    def unit_rows(number):
        source_z = lax.rem(z + ORDER[number], NZ)
        return pl.ds(pl.multiple_of(source_z * unit, unit), unit)

    def spread(buf, number, sems, base_send):
        place = unit_rows(number)
        send(buf.at[t, place], buf.at[t, place], send_sem.at[base_send], sems.at[0, number], e, right)
        send(buf.at[t, place], buf.at[t, place], send_sem.at[base_send], sems.at[1, number], e, left)
        if buf is H and number in DIRECT:
            send(
                buf.at[t, place],
                buf.at[t, place],
                send_sem.at[base_send + 1],
                sems.at[2, number],
                e,
                lax.rem(t + 2, TP),
            )

    def relay(buf, number, sems, base_send):
        place = unit_rows(number)
        drain(buf.at[left, place], sems.at[0, number])
        drain(buf.at[right, place], sems.at[1, number])
        if buf is H and number in DIRECT:
            return
        if number % 2 == 0 or (buf is H and number == 7):
            send(
                buf.at[left, place],
                buf.at[left, place],
                send_sem.at[base_send + 1],
                sems.at[2, number],
                e,
                right,
            )
        else:
            send(
                buf.at[right, place],
                buf.at[right, place],
                send_sem.at[base_send + 1],
                sems.at[2, number],
                e,
                left,
            )

    def relayed(buf, number, sems):
        across = lax.rem(t + 2, TP)
        drain(buf.at[across, unit_rows(number)], sems.at[2, number])

    def take(number):
        if number == 0:
            drain(X.at[:, pl.ds(0, unit - cell)], disp_recv.at[0])
        else:
            drain(X.at[t, pl.ds(0, unit)], disp_recv.at[number])
            spread(X, number, x_recv, 4)

    def hidden(batch):
        pair = BATCHES[batch]
        for number in pair:
            if number > 0:
                relayed(X, number, x_recv)
        tall = len(pair) * unit
        gate_part = jnp.zeros((tall, gw.shape[1]), f32)
        up_part = jnp.zeros((tall, gw.shape[1]), f32)
        for part in range(TP):
            block = jnp.concatenate([X[part, unit_rows(number)] for number in pair], axis=0)
            depth = pl.ds(part * width, width)
            gate_part = gate_part + jnp.dot(block, gw[depth, :], preferred_element_type=f32)
            up_part = up_part + jnp.dot(block, uw[depth, :], preferred_element_type=f32)
        gate_part = jnp.minimum(gate_part, clamp_limit)
        up_part = jnp.clip(up_part, -clamp_limit, clamp_limit)
        result = (gate_part * jax.nn.sigmoid(gate_slope * gate_part) * (up_part + 1.0)).astype(bf16)
        for i, number in enumerate(pair):
            H[t, unit_rows(number)] = result[i * unit : (i + 1) * unit]
        for number in pair:
            spread(H, number, h_recv, 6)

    def hidden_relay(batch):
        for number in BATCHES[batch]:
            relay(H, number, h_recv, 6)

    def down(batch):
        pair = BATCHES[batch]
        for number in pair:
            relayed(H, number, h_recv)
        total = jnp.zeros((len(pair) * unit, width), f32)
        for part in range(TP):
            block = jnp.concatenate([H[part, unit_rows(number)] for number in pair], axis=0)
            total = total + jnp.dot(block, wd[part], preferred_element_type=f32)
        total = total.astype(bf16)
        for i, number in enumerate(pair):
            Dn[unit_rows(number), :] = total[i * unit : (i + 1) * unit]
        for number in pair:
            source_z = lax.rem(z + ORDER[number], NZ)

            @pl.loop(1 if ORDER[number] == 0 else 0, J)
            def _(step, source_z=source_z):
                source = source_z * J + lax.rem(j + step, J)
                send(
                    Dn.at[pl.ds(pl.multiple_of(source * cell, cell), cell)],
                    R.at[my_rows],
                    send_sem.at[8],
                    one_recv.at[3],
                    source,
                    t,
                )

            if ORDER[number] == 0:
                R[my_rows, :] = Dn[my_rows, :]

    def expand():
        drain(Q.at[pl.ds(0, J // 2)], one_recv.at[8])
        latents_here()
        load_k.wait()
        load_v.wait()
        lat = jnp.concatenate([KV[lax.rem(z + p, NZ)] for p in range(NZ)], axis=0)
        turn = lat[:, 512:640]
        keys = jnp.dot(lat[:, :512], kw[...], preferred_element_type=f32).astype(bf16)
        values = jnp.dot(lat[:, :512], vw[...], preferred_element_type=f32).astype(bf16)
        low = iota((rows, 128), 1) < 64
        zero = jnp.zeros((rows, 128), bf16)
        for p in range(NZ):
            here = slice(p * rows, (p + 1) * rows)
            earlier = z + p >= NZ
            keep = (lambda v: v) if p == 0 else (lambda v, earlier=earlier: jnp.where(earlier, v, zero))
            piece = keep(turn[here])
            even, odd = jnp.where(low, piece, zero), jnp.where(low, zero, piece)
            ones = keep(jnp.ones((rows, 128), bf16))
            for h in range(4):
                Kc[h, here, 0:128] = keep(keys[here, 128 * h : 128 * (h + 1)])
                Kc[h, here, 128:256] = even if h % 2 == 0 else odd
                Vc[h, here, 0:128] = keep(values[here, 128 * h : 128 * (h + 1)])
                Vc[h, here, 128:256] = ones

    scale = (NOPE + ROPE) ** (-0.5) * float(np.log2(np.e))

    def head(part):
        h, first = part // 2, (part % 2) * (J // 4)
        span = 2 * rows

        @pl.loop(first, first + J // 4)
        def _(chunk):
            plain = Q[pl.ds(2 * chunk, 2), :, 128 * h : 128 * (h + 1)].reshape(span, 128)
            pair = 512 + 128 * (h // 2)
            turn = Q[pl.ds(2 * chunk, 2), :, pair : pair + 128].reshape(span, 128)
            both = jnp.concatenate([plain, turn], axis=1)
            scores = lax.dot_general(
                both, Kc[h], (((1,), (1,)), ((), ())), preferred_element_type=f32
            )
            grown = jnp.exp2(scores * scale)
            key_place = j * rows + iota((1, rows), 1)
            query_place = chunk * span + iota((span, 1), 0)
            near_z = jnp.where(key_place <= query_place, grown[:, :rows], 0.0)
            weights = jnp.concatenate([near_z.astype(bf16), grown[:, rows:].astype(bf16)], axis=1)
            both_out = jnp.dot(weights, Vc[h], preferred_element_type=f32)
            here = pl.ds(pl.multiple_of(chunk * span, span), span)
            o_out[h, here, :] = both_out[:, :128].astype(bf16)
            sums = both_out[:, 128:]
            if h == 0:
                t_out[here, :] = sums
            else:
                lanes = iota((span, 128), 1)
                t_out[here, :] = jnp.where(lanes // 32 == h, sums, t_out[here, :])

    back_order = (4, 2, 6, 3, 5, 1, 7)

    def give_back(h):
        for step in back_order:
            target = lax.rem(j + step, J)
            place = pl.ds(pl.multiple_of(target * rows, rows), rows)
            send(o_out.at[h, place], o_in.at[h, j], send_sem.at[9], one_recv.at[4], z * J + target, t)
        o_in[h, j] = o_out[h, pl.ds(pl.multiple_of(j * rows, rows), rows), :]

    def give_totals():
        for i in range(J):
            across = jnp.transpose(t_out[i * rows : (i + 1) * rows, :])
            picks = [across[32 * h : 32 * h + 1, :] for h in range(4)]
            t_row[i] = jnp.concatenate(picks + picks, axis=0)
        for step in back_order:
            target = lax.rem(j + step, J)
            send(t_row.at[target], t_in.at[j], send_sem.at[10], one_recv.at[5], z * J + target, t)
        t_in[j] = t_row[j]

    quarter = rows // TP

    def project():
        drain(o_in.at[:, pl.ds(0, J - 1)], one_recv.at[4])
        drain(t_in.at[pl.ds(0, J - 1)], one_recv.at[5])
        load_o.wait()
        tsum = jnp.zeros(t_in.shape[1:], f32)
        for i in range(J):
            tsum = tsum + t_in[i]
        tsum = jnp.transpose(jnp.concatenate([tsum] * (128 // tsum.shape[0]), axis=0))
        heads = []
        for h in range(4):
            osum = jnp.zeros((rows, VD), f32)
            for i in range(J):
                osum = osum + o_in[h, i].astype(f32)
            heads.append((osum / tsum[:, h : h + 1]).astype(bf16))
        attended = jnp.concatenate(heads, axis=1)
        p_out[...] = jnp.dot(attended, ow[...], preferred_element_type=f32).astype(bf16)
        for step in range(1, TP):
            peer = lax.rem(t + step, TP)
            place = pl.ds(pl.multiple_of(peer * quarter, quarter), quarter)
            send(p_out.at[place], p_in.at[t], send_sem.at[11], one_recv.at[6], e, peer)
        p_in[t] = p_out[pl.ds(pl.multiple_of(t * quarter, quarter), quarter), :]

    def finish_mixed():
        drain(p_in.at[pl.ds(0, TP - 1)], one_recv.at[6])
        projected = jnp.zeros((quarter, p_in.shape[2]), f32)
        for i in range(TP):
            projected = projected + p_in[i].astype(f32)
        mixed_out[...] = rms(projected, out_gain[...]).astype(bf16)

    with jax.named_scope("s00_share_down_0"):
        share_down(2)
    with jax.named_scope("s01_dispatch_2"):
        dispatch(2)
    with jax.named_scope("s02_dispatch_3"):
        dispatch(3)
    with jax.named_scope("s03_dispatch_1"):
        dispatch(1)
    with jax.named_scope("s04_own_norm_"):
        own_norm()
    with jax.named_scope("s05_own_queries_0"):
        own_queries()
    with jax.named_scope("s06_own_latents_0"):
        own_latents()
    with jax.named_scope("s07_weigh_0"):
        weigh()
    with jax.named_scope("s08_take_3"):
        take(3)
    with jax.named_scope("s09_take_2"):
        take(2)
    with jax.named_scope("s10_dispatch_5"):
        dispatch(5)
    with jax.named_scope("s11_dispatch_6"):
        dispatch(6)
    with jax.named_scope("s12_relay_3"):
        relay(X, 3, x_recv, 4)
    with jax.named_scope("s13_take_1"):
        take(1)
    with jax.named_scope("s14_pass_on_1"):
        pass_on(1)
    with jax.named_scope("s15_dispatch_4"):
        dispatch(4)
    with jax.named_scope("s16_relay_2"):
        relay(X, 2, x_recv, 4)
    with jax.named_scope("s17_take_6"):
        take(6)
    with jax.named_scope("s18_take_5"):
        take(5)
    with jax.named_scope("s19_load_gu_"):
        load_g.wait()
        load_u.wait()
    with jax.named_scope("s20_hidden_1"):
        hidden(1)
    with jax.named_scope("s21_relay_1"):
        relay(X, 1, x_recv, 4)
    with jax.named_scope("s22_pass_on_2"):
        pass_on(2)
    with jax.named_scope("s23_relay_6"):
        relay(X, 6, x_recv, 4)
    with jax.named_scope("s24_dispatch_7"):
        dispatch(7)
    with jax.named_scope("s25_take_4"):
        take(4)
    with jax.named_scope("s26_hidden_relay_1"):
        hidden_relay(1)
    with jax.named_scope("s27_take_0"):
        take(0)
    with jax.named_scope("s28_pass_on_3"):
        pass_on(3)
    with jax.named_scope("s29_share_queries_0"):
        share_queries()
    with jax.named_scope("s30_hidden_0"):
        hidden(0)
    with jax.named_scope("s31_expand_0"):
        expand()
    with jax.named_scope("s32_relay_5"):
        relay(X, 5, x_recv, 4)
    with jax.named_scope("s33_relay_4"):
        relay(X, 4, x_recv, 4)
    with jax.named_scope("s34_head_0"):
        head(0)
    with jax.named_scope("s35_head_1"):
        head(1)
        give_back(0)
    with jax.named_scope("s36_take_7"):
        take(7)
    with jax.named_scope("s37_load_dd_"):
        load_d.wait()
        drain(wd.at[pl.ds(0, TP - 1)], one_recv.at[0])
    with jax.named_scope("s38_down_1"):
        down(1)
    with jax.named_scope("s39_head_2"):
        head(2)
    with jax.named_scope("s40_hidden_relay_0"):
        hidden_relay(0)
    with jax.named_scope("s41_head_3"):
        head(3)
        give_back(1)
    with jax.named_scope("s42_head_4"):
        head(4)
    with jax.named_scope("s43_head_5"):
        head(5)
        give_back(2)
    with jax.named_scope("s44_hidden_2"):
        hidden(2)
    with jax.named_scope("s45_relay_7"):
        relay(X, 7, x_recv, 4)
    with jax.named_scope("s46_head_6"):
        head(6)
    with jax.named_scope("s47_head_7"):
        head(7)
        give_back(3)
        give_totals()
    with jax.named_scope("s48_down_0"):
        down(0)
    with jax.named_scope("s49_hidden_relay_2"):
        hidden_relay(2)
    with jax.named_scope("s50_hidden_3"):
        hidden(3)
    with jax.named_scope("s51_hidden_4"):
        hidden(4)
    with jax.named_scope("s52_down_2"):
        down(2)
    with jax.named_scope("s53_hidden_relay_3"):
        hidden_relay(3)
    with jax.named_scope("s54_project_0"):
        project()
    with jax.named_scope("s55_hidden_relay_4"):
        hidden_relay(4)
    with jax.named_scope("s56_down_4"):
        down(4)
    with jax.named_scope("s57_down_3"):
        down(3)
    with jax.named_scope("s58_finish_mixed_0"):
        finish_mixed()

    with jax.named_scope("returns"):
        drain(R.at[pl.ds(0, slots - cell)], one_recv.at[3])
    total = jnp.dot(w_hi[...], R[...], preferred_element_type=f32)
    total = total + jnp.dot(w_lo[...], R[...], preferred_element_type=f32)
    m_send[...] = total.astype(bf16)
    for step in range(1, TP):
        peer = lax.rem(t + step, TP)
        place = pl.ds(pl.multiple_of(peer * quarter, quarter), quarter)
        send(m_send.at[place], m_recv.at[t], send_sem.at[12], one_recv.at[7], e, peer)
    m_recv[t] = m_send[pl.ds(pl.multiple_of(t * quarter, quarter), quarter), :]
    with jax.named_scope("last"):
        drain(m_recv.at[pl.ds(0, TP - 1)], one_recv.at[7])
    for i in range(TP):
        moe_out[:, i * width : (i + 1) * width] = m_recv[i]

    most = slots - unit
    drain(X.at[:, pl.ds(0, unit - cell)], send_sem.at[0])
    drain(outg.at[pl.ds(0, most)], send_sem.at[13])
    drain(wd.at[pl.ds(0, TP - 1)], send_sem.at[1])
    drain(Q.at[pl.ds(0, J // 2 - 1)], send_sem.at[2])
    drain(Q.at[pl.ds(0, J // 2)], send_sem.at[14])
    drain(KV.at[pl.ds(0, NZ - 1)], send_sem.at[3])
    drain(X.at[pl.ds(0, 2), pl.ds(0, most)], send_sem.at[4])
    drain(X.at[0, pl.ds(0, most)], send_sem.at[5])
    drain(H.at[pl.ds(0, 2)], send_sem.at[6])
    drain(H.at[0], send_sem.at[7])
    drain(Dn.at[pl.ds(0, slots - cell)], send_sem.at[8])
    drain(o_in.at[:, pl.ds(0, J - 1)], send_sem.at[9])
    drain(t_in.at[pl.ds(0, J - 1)], send_sem.at[10])
    drain(p_in.at[pl.ds(0, TP - 1)], send_sem.at[11])
    drain(m_recv.at[pl.ds(0, TP - 1)], send_sem.at[12])


def turn_tables(devices, rows):
    inverse = rope_base ** (-np.arange(0, ROPE, 2) / ROPE)
    inverse = np.tile(inverse, 4)[None, :]
    base = np.arange(devices)[:, None] * rows * inverse
    row = np.arange(rows)[:, None] * inverse
    return (
        np.concatenate([np.cos(base), np.sin(base)], axis=1).astype(np.float32),
        np.concatenate([np.cos(row), np.sin(row)], axis=1).astype(np.float32),
    )


def solution(mesh):
    EP, TP = mesh.shape["ep"], mesh.shape["tp"]
    J = 8
    NZ = EP // J
    placed = (
        P("ep", None),
        P(),
        P(None, "tp"),
        P(),
        P(),
        P(),
        P(None, "tp"),
        P(None, "tp"),
        P("tp", None),
        P(),
        P("ep", None),
        P(),
        P("ep", None, "tp"),
        P("ep", None, "tp"),
        P("ep", "tp", None),
        P("ep", None),
        P("ep", None),
    )

    def local(
        mix_in,
        mix_gain,
        query_weight,
        latent_weight,
        rotary_weight,
        latent_gain,
        key_weight,
        value_weight,
        output_weight,
        out_gain,
        ffn_in,
        ffn_gain,
        gate_weight,
        up_weight,
        down_weight,
        routes,
        route_scores,
    ):
        rows, D = mix_in.shape
        width = D // TP
        cell = MOST * (rows // QB)
        slots = EP * cell
        unit = gate_weight.shape[2]
        quarter = rows // TP
        base_turn, row_turn = turn_tables(EP, rows)
        hbm = pl.BlockSpec(memory_space=pl.ANY)
        vmem = pl.BlockSpec(memory_space=pltpu.VMEM)
        V = lambda *shape: pltpu.VMEM(shape, bf16)
        F = lambda *shape: pltpu.VMEM(shape, f32)
        S = pltpu.SemaphoreType.DMA

        def body(*refs):
            kernel(NZ, J, TP, *refs)

        out = pltpu.VMEM((quarter, D), bf16)
        return pl.pallas_call(
            body,
            name="layer",
            out_shape=(out, out),
            in_specs=[
                hbm, vmem, hbm, hbm, hbm, vmem, hbm, hbm, hbm, vmem,
                hbm, vmem, hbm, hbm, hbm, vmem, vmem, vmem, vmem,
            ],
            out_specs=(vmem, vmem),
            scratch_shapes=[
                V(rows, D),
                V(rows, D),
                V(D, query_weight.shape[1]),
                V(D, latent_weight.shape[1]),
                V(ROPE, D),
                V(*key_weight.shape),
                V(*value_weight.shape),
                V(*output_weight.shape),
                V(D, unit),
                V(D, unit),
                V(TP, unit, width),
                V(slots, width),
                V(TP, J * cell, width),
                V(TP, slots, width),
                V(TP, slots, unit),
                V(slots, width),
                V(slots, width),
                V(slots, rows),
                V(rows, slots),
                V(rows, slots),
                V(rows, width),
                V(TP, quarter, width),
                V(J, rows, 768),
                V(NZ, rows, 640),
                V(rows, 768),
                V(4, NZ * rows, 256),
                V(4, NZ * rows, 256),
                V(4, J * rows, VD),
                F(J * rows, 128),
                F(J, 8, rows),
                V(4, J, rows, VD),
                F(J, 8, rows),
                V(rows, D),
                V(TP, quarter, D),
                S((11,)),
                S((8,)),
                S((3, 8)),
                S((3, 8)),
                S((2, NZ // 2)),
                S((9,)),
                S((15,)),
            ],
            compiler_params=pltpu.CompilerParams(
                collective_id=0, has_side_effects=True, vmem_limit_bytes=62 * 1024 * 1024
            ),
        )(
            mix_in,
            mix_gain[None, :],
            query_weight,
            latent_weight,
            rotary_weight.T,
            latent_gain[None, :],
            key_weight,
            value_weight,
            output_weight,
            out_gain[None, :],
            ffn_in,
            ffn_gain[None, :],
            gate_weight,
            up_weight,
            down_weight,
            routes.T,
            route_scores.T,
            base_turn,
            row_turn,
        )

    return jax.shard_map(
        local,
        mesh=mesh,
        in_specs=placed,
        out_specs=(P(("ep", "tp"), None), P(("ep", "tp"), None)),
        check_vma=False,
    )
```

```python
import jax
import jax.numpy as jnp
import numpy as np
from jax import lax
from jax.experimental import pallas as pl
from jax.experimental.pallas import tpu as pltpu
from jax.sharding import PartitionSpec as P

NOPE = 128
ROPE = 64
VD = 128
QB = 32
MOST = 4

norm_eps = 1e-06
clamp_limit = 7.0
gate_slope = 1.702
rope_base = 10000.0

MESH = pl.DeviceIdType.MESH
bf16 = jnp.bfloat16
f32 = jnp.float32

ORDER = (0, 4, 3, 5, 2, 6, 1, 7)

BATCHES = ((0, 1), (2, 3), (4, 5), (6,), (7,))
LATE = (6, 7)
DIRECT = (6, 7)


def iota(shape, dim):
    return lax.broadcasted_iota(jnp.int32, shape, dim)


def rms(rows, gain):
    mean_square = jnp.mean(rows * rows, axis=-1, keepdims=True)
    return rows * lax.rsqrt(mean_square + norm_eps) * gain


def drain(view, sem):
    with jax.named_scope("wait"):
        pltpu.make_async_copy(view, view, sem).wait()


def kernel(
    NZ,
    J,
    TP,
    mix_in,
    mix_gain,
    query_weight,
    latent_weight,
    rotary_weight,
    latent_gain,
    key_weight,
    value_weight,
    output_weight,
    out_gain,
    ffn_in,
    ffn_gain,
    gate_weight,
    up_weight,
    down_weight,
    routes,
    route_scores,
    base_turn,
    row_turn,
    mixed_out,
    moe_out,
    mix_v,
    ffn_v,
    qw,
    lw,
    rw,
    kw,
    vw,
    ow,
    gw,
    uw,
    wd,
    dw,
    outg,
    near,
    X,
    H,
    Dn,
    R,
    sel,
    w_hi,
    w_lo,
    m_send,
    m_recv,
    Q,
    KV,
    q_out,
    Kc,
    Vc,
    o_out,
    t_out,
    t_row,
    o_in,
    t_in,
    p_out,
    p_in,
    load_sem,
    disp_recv,
    x_recv,
    h_recv,
    kv_recv,
    one_recv,
    send_sem,
):
    E = NZ * J
    e = lax.axis_index("ep")
    t = lax.axis_index("tp")
    z = e // J
    j = e % J
    rows = ffn_v.shape[0]
    width = outg.shape[1]
    cell = outg.shape[0] // E
    right = lax.rem(t + 1, TP)
    left = lax.rem(t + TP - 1, TP)
    unit = J * cell

    def load(src, dst, number):
        copy = pltpu.make_async_copy(src, dst, load_sem.at[number])
        copy.start()
        return copy

    def send(src, dst, s_sem, r_sem, ep, tp):
        pltpu.make_async_remote_copy(
            src_ref=src,
            dst_ref=dst,
            send_sem=s_sem,
            recv_sem=r_sem,
            device_id=(ep, tp),
            device_id_type=MESH,
        ).start()

    barrier = pltpu.get_barrier_semaphore()

    for dz in (4, 3, 5, 2, 6, 1, 7, 0):

        @pl.loop(1 if dz == 0 else 0, J, unroll=True)
        def _(step, dz=dz):
            peer = lax.rem(z + dz, NZ) * J + lax.rem(j + step, J)
            pl.semaphore_signal(barrier, inc=1, device_id=(peer, t), device_id_type=MESH)

    for step in range(1, TP):
        pl.semaphore_signal(
            barrier, inc=1, device_id=(e, lax.rem(t + step, TP)), device_id_type=MESH
        )

    load_ffn = load(ffn_in, ffn_v, 0)
    load_mix = load(mix_in, mix_v, 1)
    load_q = load(query_weight, qw, 2)
    load_l = load(latent_weight, lw, 3)
    load_r = load(rotary_weight, rw, 4)
    load_k = load(key_weight, kw, 5)
    load_v = load(value_weight, vw, 6)
    load_g = load(gate_weight.at[0], gw, 7)
    load_u = load(up_weight.at[0], uw, 8)
    load_d = load(
        down_weight.at[0, :, pl.ds(pl.multiple_of(t * width, 128), width)], wd.at[t], 9
    )
    load_w = load(down_weight.at[0], dw, 11)
    load_o = load(output_weight, ow, 10)

    slots = outg.shape[0]
    blocks = rows // QB
    slot = iota((slots, 1), 0)
    slot_expert = slot // cell
    slot_block = (slot // MOST) % blocks
    slot_rank = (slot % MOST).astype(f32)
    row_block = iota((1, rows), 1) // QB
    route = routes[...]
    choose = route.shape[0]
    named = jnp.zeros((slots, rows), f32)
    for k in range(choose):
        named = named + jnp.where(route[k : k + 1, :] == slot_expert, 1.0, 0.0)
    up_r = iota((rows, rows), 0)
    up_c = iota((rows, rows), 1)
    upper = jnp.where((up_r < up_c) & (up_c // QB == up_r // QB), 1.0, 0.0).astype(bf16)
    rank = jnp.dot(named.astype(bf16), upper, preferred_element_type=f32)
    picked = jnp.where((rank == slot_rank) & (row_block == slot_block), named, 0.0)
    sel[...] = picked.astype(bf16)

    load_ffn.wait()
    ffn_v[...] = rms(ffn_v[...].astype(f32), ffn_gain[...]).astype(bf16)
    columns = pl.ds(pl.multiple_of(t * width, 128), width)
    outg[...] = jnp.dot(sel[...], ffn_v[:, columns], preferred_element_type=f32).astype(bf16)
    own_z = pl.ds(pl.multiple_of(z * unit, unit), unit)
    for part in range(TP):
        near[part] = jnp.dot(
            sel[own_z, :], ffn_v[:, part * width : (part + 1) * width], preferred_element_type=f32
        ).astype(bf16)

    base = base_turn[pl.ds(e, 1), :]
    base_cos, base_sin = base[:, :128], base[:, 128:]
    row_cos, row_sin = row_turn[:, :128], row_turn[:, 128:]
    cosine = base_cos * row_cos - base_sin * row_sin
    sine = base_sin * row_cos + base_cos * row_sin
    lane = iota((rows, 128), 1)
    first_half = lane % ROPE < ROPE // 2
    sine = jnp.where(first_half, -sine, sine)

    def turned(v):
        partner = jnp.where(first_half, pltpu.roll(v, 96, 1), pltpu.roll(v, 32, 1))
        return v * cosine + partner * sine

    load_w.wait()
    with jax.named_scope("barrier"):
        pl.semaphore_wait(barrier, E - 1 + TP - 1)

    def share_down(step):
        peer = lax.rem(t + step, TP)
        send(
            dw.at[:, pl.ds(pl.multiple_of(peer * width, 128), width)],
            wd.at[t],
            send_sem.at[1],
            one_recv.at[0],
            e,
            peer,
        )

    share_down(1)
    share_down(TP - 1)

    my_rows = pl.ds(pl.multiple_of(e * cell, cell), cell)

    @pl.loop(1, J)
    def _(step):
        to = lax.rem(j + step, J)
        send(
            near.at[:, pl.ds(pl.multiple_of(to * cell, cell), cell)],
            X.at[:, my_rows],
            send_sem.at[0],
            disp_recv.at[0],
            z * J + to,
            t,
        )

    for part in range(TP):
        X[part, my_rows] = near[part, pl.ds(pl.multiple_of(j * cell, cell), cell)]

    def dispatch(number):
        target_z = lax.rem(z + NZ - ORDER[number], NZ)

        @pl.loop(0, J)
        def _(step):
            target = target_z * J + lax.rem(j + step, J)
            send(
                outg.at[pl.ds(pl.multiple_of(target * cell, cell), cell)],
                X.at[t, my_rows],
                send_sem.at[13],
                disp_recv.at[number],
                target,
                t,
            )

    up_z, down_z = lax.rem(z + 1, NZ), lax.rem(z + NZ - 1, NZ)
    half = rows // 2

    def pass_on(hop):
        if hop > 0:
            at_up, at_down = lax.rem(z + NZ - hop, NZ), lax.rem(z + hop, NZ)
            drain(KV.at[at_up], kv_recv.at[0, hop - 1])
            drain(KV.at[at_down], kv_recv.at[1, hop - 1])
        else:
            at_up = at_down = z
        upward, downward = KV.at[at_up], KV.at[at_down]
        if 2 * (hop + 1) == NZ:
            upward, downward = KV.at[at_up, pl.ds(0, half)], KV.at[at_down, pl.ds(half, half)]
        send(upward, upward, send_sem.at[3], kv_recv.at[0, hop], up_z * J + j, t)
        send(downward, downward, send_sem.at[3], kv_recv.at[1, hop], down_z * J + j, t)

    def latents_here():
        across = lax.rem(z + NZ // 2, NZ)
        drain(KV.at[across, pl.ds(0, half)], kv_recv.at[0, NZ // 2 - 1])
        drain(KV.at[across, pl.ds(half, half)], kv_recv.at[1, NZ // 2 - 1])

    def own_norm():
        load_mix.wait()
        mix_v[...] = rms(mix_v[...].astype(f32), mix_gain[...]).astype(bf16)

    def own_latents():
        load_l.wait()
        latent = jnp.dot(mix_v[...], lw[...], preferred_element_type=f32)
        KV[z, :, 0:512] = rms(latent, latent_gain[...]).astype(bf16)
        load_r.wait()
        rotary = lax.dot_general(
            mix_v[...], rw[...], (((1,), (1,)), ((), ())), preferred_element_type=f32
        )
        KV[z, :, 512:640] = turned(jnp.concatenate([rotary, rotary], axis=1)).astype(bf16)

        pass_on(0)

    mate = j + 1 - 2 * lax.rem(j, 2)

    def own_queries():
        load_q.wait()
        queries = jnp.dot(mix_v[...], qw[...], preferred_element_type=f32)
        low_lanes = lane < 64
        A = [queries[:, 128 * i : 128 * (i + 1)] for i in range(6)]
        q_out[:, 0:128] = A[0].astype(bf16)
        q_out[:, 128:256] = pltpu.roll(jnp.where(low_lanes, A[2], A[1]), 64, 1).astype(bf16)
        q_out[:, 256:384] = A[3].astype(bf16)
        q_out[:, 384:512] = pltpu.roll(jnp.where(low_lanes, A[5], A[4]), 64, 1).astype(bf16)
        q_out[:, 512:640] = turned(jnp.where(low_lanes, A[1], A[2])).astype(bf16)
        q_out[:, 640:768] = turned(jnp.where(low_lanes, A[4], A[5])).astype(bf16)
        Q[j] = q_out[...]
        for step in range(2, J, 2):
            send(Q.at[j], Q.at[j], send_sem.at[2], one_recv.at[1], z * J + lax.rem(j + step, J), t)
        send(Q.at[j], Q.at[j], send_sem.at[14], one_recv.at[8], z * J + mate, t)

    def share_queries():
        drain(Q.at[pl.ds(0, J // 2 - 1)], one_recv.at[1])
        for step in range(2, J, 2):
            from_j = lax.rem(j + step, J)
            send(Q.at[from_j], Q.at[from_j], send_sem.at[14], one_recv.at[8], z * J + mate, t)

    def weigh():
        score = route_scores[...]
        grown = jnp.exp(score - jnp.max(score, axis=0, keepdims=True))
        share = grown / jnp.sum(grown, axis=0, keepdims=True)
        gates = jnp.zeros((slots, rows), f32)
        for k in range(choose):
            gates = gates + jnp.where(route[k : k + 1, :] == slot_expert, share[k : k + 1, :], 0.0)
        gates = jnp.transpose(gates * sel[...].astype(f32))
        gates_hi = gates.astype(bf16)
        w_hi[...] = gates_hi
        w_lo[...] = (gates - gates_hi.astype(f32)).astype(bf16)

    def unit_rows(number):
        source_z = lax.rem(z + ORDER[number], NZ)
        return pl.ds(pl.multiple_of(source_z * unit, unit), unit)

    def spread(buf, number, sems, base_send):
        place = unit_rows(number)
        send(buf.at[t, place], buf.at[t, place], send_sem.at[base_send], sems.at[0, number], e, right)
        send(buf.at[t, place], buf.at[t, place], send_sem.at[base_send], sems.at[1, number], e, left)
        if buf is H and number in DIRECT:
            send(
                buf.at[t, place],
                buf.at[t, place],
                send_sem.at[base_send + 1],
                sems.at[2, number],
                e,
                lax.rem(t + 2, TP),
            )

    def relay(buf, number, sems, base_send):
        place = unit_rows(number)
        drain(buf.at[left, place], sems.at[0, number])
        drain(buf.at[right, place], sems.at[1, number])
        if buf is H and number in DIRECT:
            return
        if number % 2 == 0 or (buf is H and number == 7):
            send(
                buf.at[left, place],
                buf.at[left, place],
                send_sem.at[base_send + 1],
                sems.at[2, number],
                e,
                right,
            )
        else:
            send(
                buf.at[right, place],
                buf.at[right, place],
                send_sem.at[base_send + 1],
                sems.at[2, number],
                e,
                left,
            )

    def relayed(buf, number, sems):
        across = lax.rem(t + 2, TP)
        drain(buf.at[across, unit_rows(number)], sems.at[2, number])

    def take(number):
        if number == 0:
            drain(X.at[:, pl.ds(0, unit - cell)], disp_recv.at[0])
        else:
            drain(X.at[t, pl.ds(0, unit)], disp_recv.at[number])
            spread(X, number, x_recv, 4)

    def hidden(batch):
        pair = BATCHES[batch]
        for number in pair:
            if number > 0:
                relayed(X, number, x_recv)
        tall = len(pair) * unit
        gate_part = jnp.zeros((tall, gw.shape[1]), f32)
        up_part = jnp.zeros((tall, gw.shape[1]), f32)
        for part in range(TP):
            block = jnp.concatenate([X[part, unit_rows(number)] for number in pair], axis=0)
            depth = pl.ds(part * width, width)
            gate_part = gate_part + jnp.dot(block, gw[depth, :], preferred_element_type=f32)
            up_part = up_part + jnp.dot(block, uw[depth, :], preferred_element_type=f32)
        gate_part = jnp.minimum(gate_part, clamp_limit)
        up_part = jnp.clip(up_part, -clamp_limit, clamp_limit)
        result = (gate_part * jax.nn.sigmoid(gate_slope * gate_part) * (up_part + 1.0)).astype(bf16)
        for i, number in enumerate(pair):
            H[t, unit_rows(number)] = result[i * unit : (i + 1) * unit]
        for number in pair:
            spread(H, number, h_recv, 6)

    def hidden_relay(batch):
        for number in BATCHES[batch]:
            relay(H, number, h_recv, 6)

    def down(batch):
        pair = BATCHES[batch]
        for number in pair:
            relayed(H, number, h_recv)
        total = jnp.zeros((len(pair) * unit, width), f32)
        for part in range(TP):
            block = jnp.concatenate([H[part, unit_rows(number)] for number in pair], axis=0)
            total = total + jnp.dot(block, wd[part], preferred_element_type=f32)
        total = total.astype(bf16)
        for i, number in enumerate(pair):
            Dn[unit_rows(number), :] = total[i * unit : (i + 1) * unit]
        for number in pair:
            source_z = lax.rem(z + ORDER[number], NZ)

            @pl.loop(1 if ORDER[number] == 0 else 0, J)
            def _(step, source_z=source_z, back=9 if number in LATE else 3):
                source = source_z * J + lax.rem(j + step, J)
                send(
                    Dn.at[pl.ds(pl.multiple_of(source * cell, cell), cell)],
                    R.at[my_rows],
                    send_sem.at[8],
                    one_recv.at[back],
                    source,
                    t,
                )

            if ORDER[number] == 0:
                R[my_rows, :] = Dn[my_rows, :]

    def expand():
        drain(Q.at[pl.ds(0, J // 2)], one_recv.at[8])
        latents_here()
        load_k.wait()
        load_v.wait()
        lat = jnp.concatenate([KV[lax.rem(z + p, NZ)] for p in range(NZ)], axis=0)
        turn = lat[:, 512:640]
        keys = jnp.dot(lat[:, :512], kw[...], preferred_element_type=f32).astype(bf16)
        values = jnp.dot(lat[:, :512], vw[...], preferred_element_type=f32).astype(bf16)
        low = iota((rows, 128), 1) < 64
        zero = jnp.zeros((rows, 128), bf16)
        for p in range(NZ):
            here = slice(p * rows, (p + 1) * rows)
            earlier = z + p >= NZ
            keep = (lambda v: v) if p == 0 else (lambda v, earlier=earlier: jnp.where(earlier, v, zero))
            piece = keep(turn[here])
            even, odd = jnp.where(low, piece, zero), jnp.where(low, zero, piece)
            ones = keep(jnp.ones((rows, 128), bf16))
            for h in range(4):
                Kc[h, here, 0:128] = keep(keys[here, 128 * h : 128 * (h + 1)])
                Kc[h, here, 128:256] = even if h % 2 == 0 else odd
                Vc[h, here, 0:128] = keep(values[here, 128 * h : 128 * (h + 1)])
                Vc[h, here, 128:256] = ones

    scale = (NOPE + ROPE) ** (-0.5) * float(np.log2(np.e))

    def head(part):
        h, chunk = part // 2, part % 2
        span = (J // 2) * rows
        plain = Q[chunk * (J // 2) : (chunk + 1) * (J // 2), :, 128 * h : 128 * (h + 1)].reshape(span, 128)
        pair = 512 + 128 * (h // 2)
        turn = Q[chunk * (J // 2) : (chunk + 1) * (J // 2), :, pair : pair + 128].reshape(span, 128)
        both = jnp.concatenate([plain, turn], axis=1)
        scores = lax.dot_general(
            both, Kc[h], (((1,), (1,)), ((), ())), preferred_element_type=f32
        )
        grown = jnp.exp2(scores * scale)
        key_place = j * rows + iota((1, rows), 1)
        query_place = chunk * span + iota((span, 1), 0)
        near_z = jnp.where(key_place <= query_place, grown[:, :rows], 0.0)
        weights = jnp.concatenate([near_z.astype(bf16), grown[:, rows:].astype(bf16)], axis=1)
        both_out = jnp.dot(weights, Vc[h], preferred_element_type=f32)
        here = slice(chunk * span, (chunk + 1) * span)
        o_out[h, here, :] = both_out[:, :128].astype(bf16)
        sums = both_out[:, 128:]
        if h == 0:
            t_out[here, :] = sums
        else:
            lanes = iota((span, 128), 1)
            t_out[here, :] = jnp.where(lanes // 32 == h, sums, t_out[here, :])

    back_order = (4, 2, 6, 3, 5, 1, 7)

    def give_back(h):
        for step in back_order:
            target = lax.rem(j + step, J)
            place = pl.ds(pl.multiple_of(target * rows, rows), rows)
            send(o_out.at[h, place], o_in.at[h, j], send_sem.at[9], one_recv.at[4], z * J + target, t)
        o_in[h, j] = o_out[h, pl.ds(pl.multiple_of(j * rows, rows), rows), :]

    def give_totals():
        for i in range(J):
            across = jnp.transpose(t_out[i * rows : (i + 1) * rows, :])
            picks = [across[32 * h : 32 * h + 1, :] for h in range(4)]
            t_row[i] = jnp.concatenate(picks + picks, axis=0)
        for step in back_order:
            target = lax.rem(j + step, J)
            send(t_row.at[target], t_in.at[j], send_sem.at[10], one_recv.at[5], z * J + target, t)
        t_in[j] = t_row[j]

    quarter = rows // TP

    def project():
        drain(o_in.at[:, pl.ds(0, J - 1)], one_recv.at[4])
        drain(t_in.at[pl.ds(0, J - 1)], one_recv.at[5])
        load_o.wait()
        tsum = jnp.zeros(t_in.shape[1:], f32)
        for i in range(J):
            tsum = tsum + t_in[i]
        tsum = jnp.transpose(jnp.concatenate([tsum] * (128 // tsum.shape[0]), axis=0))
        heads = []
        for h in range(4):
            osum = jnp.zeros((rows, VD), f32)
            for i in range(J):
                osum = osum + o_in[h, i].astype(f32)
            heads.append((osum / tsum[:, h : h + 1]).astype(bf16))
        attended = jnp.concatenate(heads, axis=1)
        p_out[...] = jnp.dot(attended, ow[...], preferred_element_type=f32).astype(bf16)
        for step in range(1, TP):
            peer = lax.rem(t + step, TP)
            place = pl.ds(pl.multiple_of(peer * quarter, quarter), quarter)
            send(p_out.at[place], p_in.at[t], send_sem.at[11], one_recv.at[6], e, peer)
        p_in[t] = p_out[pl.ds(pl.multiple_of(t * quarter, quarter), quarter), :]

    def finish_mixed():
        drain(p_in.at[pl.ds(0, TP - 1)], one_recv.at[6])
        projected = jnp.zeros((quarter, p_in.shape[2]), f32)
        for i in range(TP):
            projected = projected + p_in[i].astype(f32)
        mixed_out[...] = rms(projected, out_gain[...]).astype(bf16)

    def add_up(total, numbers, back):
        count = len(numbers) * unit - (cell if 0 in numbers else 0)
        with jax.named_scope("returns"):
            drain(R.at[pl.ds(0, count)], one_recv.at[back])
        for number in numbers:
            from_z = lax.rem(z + NZ - ORDER[number], NZ)
            place = pl.ds(pl.multiple_of(from_z * unit, unit), unit)
            total = total + jnp.dot(w_hi[:, place], R[place, :], preferred_element_type=f32)
            total = total + jnp.dot(w_lo[:, place], R[place, :], preferred_element_type=f32)
        return total

    with jax.named_scope("s00_share_down_0"):
        share_down(2)
    with jax.named_scope("s01_dispatch_6"):
        dispatch(6)
    with jax.named_scope("s02_dispatch_3"):
        dispatch(3)
    with jax.named_scope("s03_dispatch_5"):
        dispatch(5)
    with jax.named_scope("s04_dispatch_2"):
        dispatch(2)
    with jax.named_scope("s05_own_norm_"):
        own_norm()
    with jax.named_scope("s06_own_latents_0"):
        own_latents()
    with jax.named_scope("s07_take_6"):
        take(6)
    with jax.named_scope("s08_dispatch_4"):
        dispatch(4)
    with jax.named_scope("s09_own_queries_0"):
        own_queries()
    with jax.named_scope("s10_take_3"):
        take(3)
    with jax.named_scope("s11_take_2"):
        take(2)
    with jax.named_scope("s12_take_5"):
        take(5)
    with jax.named_scope("s13_pass_on_1"):
        pass_on(1)
    with jax.named_scope("s14_relay_3"):
        relay(X, 3, x_recv, 4)
    with jax.named_scope("s15_relay_2"):
        relay(X, 2, x_recv, 4)
    with jax.named_scope("s16_dispatch_1"):
        dispatch(1)
    with jax.named_scope("s17_take_4"):
        take(4)
    with jax.named_scope("s18_share_queries_0"):
        share_queries()
    with jax.named_scope("s19_pass_on_2"):
        pass_on(2)
    with jax.named_scope("s20_load_gu_"):
        load_g.wait()
        load_u.wait()
    with jax.named_scope("s21_hidden_1"):
        hidden(1)
    with jax.named_scope("s22_relay_4"):
        relay(X, 4, x_recv, 4)
    with jax.named_scope("s23_relay_5"):
        relay(X, 5, x_recv, 4)
    with jax.named_scope("s24_dispatch_7"):
        dispatch(7)
    with jax.named_scope("s25_weigh_0"):
        weigh()
    with jax.named_scope("s26_hidden_relay_1"):
        hidden_relay(1)
    with jax.named_scope("s27_pass_on_3"):
        pass_on(3)
    with jax.named_scope("s28_take_1"):
        take(1)
    with jax.named_scope("s29_hidden_2"):
        hidden(2)
    with jax.named_scope("s30_load_dd_"):
        load_d.wait()
        drain(wd.at[pl.ds(0, TP - 1)], one_recv.at[0])
    with jax.named_scope("s31_down_1"):
        down(1)
    with jax.named_scope("s32_expand_0"):
        expand()
    with jax.named_scope("s33_relay_6"):
        relay(X, 6, x_recv, 4)
    with jax.named_scope("s34_relay_1"):
        relay(X, 1, x_recv, 4)
    with jax.named_scope("s35_head_0"):
        head(0)
    with jax.named_scope("s36_head_1"):
        head(1)
        give_back(0)
    with jax.named_scope("s37_head_2"):
        head(2)
    with jax.named_scope("s38_hidden_relay_2"):
        hidden_relay(2)
    with jax.named_scope("s39_take_0"):
        take(0)
    with jax.named_scope("s40_take_7"):
        take(7)
    with jax.named_scope("s41_head_3"):
        head(3)
        give_back(1)
    with jax.named_scope("s42_head_4"):
        head(4)
    with jax.named_scope("s43_head_5"):
        head(5)
        give_back(2)
    with jax.named_scope("s44_hidden_0"):
        hidden(0)
    with jax.named_scope("s45_head_6"):
        head(6)
    with jax.named_scope("s46_relay_7"):
        relay(X, 7, x_recv, 4)
    with jax.named_scope("s47_head_7"):
        head(7)
        give_back(3)
        give_totals()
    with jax.named_scope("s48_down_2"):
        down(2)
    with jax.named_scope("s49_hidden_relay_0"):
        hidden_relay(0)
    with jax.named_scope("s50_hidden_3"):
        hidden(3)
    with jax.named_scope("s51_hidden_4"):
        hidden(4)
    with jax.named_scope("s52_down_0"):
        down(0)
    with jax.named_scope("s53_project_0"):
        project()
    with jax.named_scope("s54_hidden_relay_3"):
        hidden_relay(3)
    with jax.named_scope("s55_down_3"):
        down(3)
    with jax.named_scope("s56_hidden_relay_4"):
        hidden_relay(4)
    with jax.named_scope("s57_down_4"):
        down(4)
    total = jnp.zeros((rows, width), f32)
    total = add_up(total, tuple(n for n in range(NZ) if n not in LATE), 3)
    with jax.named_scope("s58_finish_mixed_0"):
        finish_mixed()

    total = add_up(total, LATE, 9)
    m_send[...] = total.astype(bf16)
    for step in range(1, TP):
        peer = lax.rem(t + step, TP)
        place = pl.ds(pl.multiple_of(peer * quarter, quarter), quarter)
        send(m_send.at[place], m_recv.at[t], send_sem.at[12], one_recv.at[7], e, peer)
    m_recv[t] = m_send[pl.ds(pl.multiple_of(t * quarter, quarter), quarter), :]
    with jax.named_scope("last"):
        drain(m_recv.at[pl.ds(0, TP - 1)], one_recv.at[7])
    for i in range(TP):
        moe_out[:, i * width : (i + 1) * width] = m_recv[i]

    most = slots - unit
    drain(X.at[:, pl.ds(0, unit - cell)], send_sem.at[0])
    drain(outg.at[pl.ds(0, most)], send_sem.at[13])
    drain(wd.at[pl.ds(0, TP - 1)], send_sem.at[1])
    drain(Q.at[pl.ds(0, J // 2 - 1)], send_sem.at[2])
    drain(Q.at[pl.ds(0, J // 2)], send_sem.at[14])
    drain(KV.at[pl.ds(0, NZ - 1)], send_sem.at[3])
    drain(X.at[pl.ds(0, 2), pl.ds(0, most)], send_sem.at[4])
    drain(X.at[0, pl.ds(0, most)], send_sem.at[5])
    drain(H.at[pl.ds(0, 2)], send_sem.at[6])
    drain(H.at[0], send_sem.at[7])
    drain(Dn.at[pl.ds(0, slots - cell)], send_sem.at[8])
    drain(o_in.at[:, pl.ds(0, J - 1)], send_sem.at[9])
    drain(t_in.at[pl.ds(0, J - 1)], send_sem.at[10])
    drain(p_in.at[pl.ds(0, TP - 1)], send_sem.at[11])
    drain(m_recv.at[pl.ds(0, TP - 1)], send_sem.at[12])


def turn_tables(devices, rows):
    inverse = rope_base ** (-np.arange(0, ROPE, 2) / ROPE)
    inverse = np.tile(inverse, 4)[None, :]
    base = np.arange(devices)[:, None] * rows * inverse
    row = np.arange(rows)[:, None] * inverse
    return (
        np.concatenate([np.cos(base), np.sin(base)], axis=1).astype(np.float32),
        np.concatenate([np.cos(row), np.sin(row)], axis=1).astype(np.float32),
    )


def solution(mesh):
    EP, TP = mesh.shape["ep"], mesh.shape["tp"]
    J = 8
    NZ = EP // J
    placed = (
        P("ep", None),
        P(),
        P(None, "tp"),
        P(),
        P(),
        P(),
        P(None, "tp"),
        P(None, "tp"),
        P("tp", None),
        P(),
        P("ep", None),
        P(),
        P("ep", None, "tp"),
        P("ep", None, "tp"),
        P("ep", "tp", None),
        P("ep", None),
        P("ep", None),
    )

    def local(
        mix_in,
        mix_gain,
        query_weight,
        latent_weight,
        rotary_weight,
        latent_gain,
        key_weight,
        value_weight,
        output_weight,
        out_gain,
        ffn_in,
        ffn_gain,
        gate_weight,
        up_weight,
        down_weight,
        routes,
        route_scores,
    ):
        rows, D = mix_in.shape
        width = D // TP
        cell = MOST * (rows // QB)
        slots = EP * cell
        unit = gate_weight.shape[2]
        quarter = rows // TP
        base_turn, row_turn = turn_tables(EP, rows)
        hbm = pl.BlockSpec(memory_space=pl.ANY)
        vmem = pl.BlockSpec(memory_space=pltpu.VMEM)
        V = lambda *shape: pltpu.VMEM(shape, bf16)
        F = lambda *shape: pltpu.VMEM(shape, f32)
        S = pltpu.SemaphoreType.DMA

        def body(*refs):
            kernel(NZ, J, TP, *refs)

        out = pltpu.VMEM((quarter, D), bf16)
        return pl.pallas_call(
            body,
            name="layer",
            out_shape=(out, out),
            in_specs=[
                hbm, vmem, hbm, hbm, hbm, vmem, hbm, hbm, hbm, vmem,
                hbm, vmem, hbm, hbm, hbm, vmem, vmem, vmem, vmem,
            ],
            out_specs=(vmem, vmem),
            scratch_shapes=[
                V(rows, D),
                V(rows, D),
                V(D, query_weight.shape[1]),
                V(D, latent_weight.shape[1]),
                V(ROPE, D),
                V(*key_weight.shape),
                V(*value_weight.shape),
                V(*output_weight.shape),
                V(D, unit),
                V(D, unit),
                V(TP, unit, width),
                V(unit, D),
                V(slots, width),
                V(TP, J * cell, width),
                V(TP, slots, width),
                V(TP, slots, unit),
                V(slots, width),
                V(slots, width),
                V(slots, rows),
                V(rows, slots),
                V(rows, slots),
                V(rows, width),
                V(TP, quarter, width),
                V(J, rows, 768),
                V(NZ, rows, 640),
                V(rows, 768),
                V(4, NZ * rows, 256),
                V(4, NZ * rows, 256),
                V(4, J * rows, VD),
                F(J * rows, 128),
                F(J, 8, rows),
                V(4, J, rows, VD),
                F(J, 8, rows),
                V(rows, D),
                V(TP, quarter, D),
                S((12,)),
                S((8,)),
                S((3, 8)),
                S((3, 8)),
                S((2, NZ // 2)),
                S((10,)),
                S((15,)),
            ],
            compiler_params=pltpu.CompilerParams(
                collective_id=0, has_side_effects=True, vmem_limit_bytes=62 * 1024 * 1024
            ),
        )(
            mix_in,
            mix_gain[None, :],
            query_weight,
            latent_weight,
            rotary_weight.T,
            latent_gain[None, :],
            key_weight,
            value_weight,
            output_weight,
            out_gain[None, :],
            ffn_in,
            ffn_gain[None, :],
            gate_weight,
            up_weight,
            down_weight,
            routes.T,
            route_scores.T,
            base_turn,
            row_turn,
        )

    return jax.shard_map(
        local,
        mesh=mesh,
        in_specs=placed,
        out_specs=(P(("ep", "tp"), None), P(("ep", "tp"), None)),
        check_vma=False,
    )
```

```python
import jax
import jax.numpy as jnp
import numpy as np
from jax import lax
from jax.experimental import pallas as pl
from jax.experimental.pallas import tpu as pltpu
from jax.sharding import PartitionSpec as P

NOPE = 128
ROPE = 64
VD = 128
QB = 32
MOST = 4

norm_eps = 1e-06
clamp_limit = 7.0
gate_slope = 1.702
rope_base = 10000.0

MESH = pl.DeviceIdType.MESH
bf16 = jnp.bfloat16
f32 = jnp.float32

ORDER = (0, 4, 3, 5, 2, 6, 1, 7)

BATCHES = ((0, 1), (2, 3), (4, 5), (6,), (7,))
LATE = (6, 7)
DIRECT = (6, 7)


def iota(shape, dim):
    return lax.broadcasted_iota(jnp.int32, shape, dim)


def rms(rows, gain):
    mean_square = jnp.mean(rows * rows, axis=-1, keepdims=True)
    return rows * lax.rsqrt(mean_square + norm_eps) * gain


def drain(view, sem):
    with jax.named_scope("wait"):
        pltpu.make_async_copy(view, view, sem).wait()


def kernel(
    NZ,
    J,
    TP,
    mix_in,
    mix_gain,
    query_weight,
    latent_weight,
    rotary_weight,
    latent_gain,
    key_weight,
    value_weight,
    output_weight,
    out_gain,
    ffn_in,
    ffn_gain,
    gate_weight,
    up_weight,
    down_weight,
    routes,
    route_scores,
    base_turn,
    row_turn,
    mixed_out,
    moe_out,
    mix_v,
    ffn_v,
    qw,
    lw,
    rw,
    kw,
    vw,
    ow,
    gw,
    uw,
    wd,
    dw,
    outg,
    near,
    X,
    H,
    Dn,
    R,
    sel,
    w_hi,
    w_lo,
    m_send,
    m_recv,
    Q,
    KV,
    q_out,
    Kc,
    Vc,
    o_out,
    t_out,
    t_row,
    o_in,
    t_in,
    p_out,
    p_in,
    load_sem,
    disp_recv,
    x_recv,
    h_recv,
    kv_recv,
    one_recv,
    send_sem,
):
    E = NZ * J
    e = lax.axis_index("ep")
    t = lax.axis_index("tp")
    z = e // J
    j = e % J
    rows = ffn_v.shape[0]
    width = outg.shape[1]
    cell = outg.shape[0] // E
    right = lax.rem(t + 1, TP)
    left = lax.rem(t + TP - 1, TP)
    unit = J * cell

    def load(src, dst, number):
        copy = pltpu.make_async_copy(src, dst, load_sem.at[number])
        copy.start()
        return copy

    def send(src, dst, s_sem, r_sem, ep, tp):
        pltpu.make_async_remote_copy(
            src_ref=src,
            dst_ref=dst,
            send_sem=s_sem,
            recv_sem=r_sem,
            device_id=(ep, tp),
            device_id_type=MESH,
        ).start()

    load_ffn = load(ffn_in, ffn_v, 0)
    load_w = load(down_weight.at[0], dw, 11)

    barrier = pltpu.get_barrier_semaphore()

    for dz in (4, 3, 5, 2, 6, 1, 7, 0):

        @pl.loop(1 if dz == 0 else 0, J, unroll=True)
        def _(step, dz=dz):
            peer = lax.rem(z + dz, NZ) * J + lax.rem(j + step, J)
            pl.semaphore_signal(barrier, inc=1, device_id=(peer, t), device_id_type=MESH)

    for step in range(1, TP):
        pl.semaphore_signal(
            barrier, inc=1, device_id=(e, lax.rem(t + step, TP)), device_id_type=MESH
        )


    slots = outg.shape[0]
    blocks = rows // QB
    slot = iota((slots, 1), 0)
    slot_expert = slot // cell
    slot_block = (slot // MOST) % blocks
    slot_rank = (slot % MOST).astype(f32)
    row_block = iota((1, rows), 1) // QB
    route = routes[...]
    choose = route.shape[0]
    named = jnp.zeros((slots, rows), f32)
    for k in range(choose):
        named = named + jnp.where(route[k : k + 1, :] == slot_expert, 1.0, 0.0)
    up_r = iota((rows, rows), 0)
    up_c = iota((rows, rows), 1)
    upper = jnp.where((up_r < up_c) & (up_c // QB == up_r // QB), 1.0, 0.0).astype(bf16)
    rank = jnp.dot(named.astype(bf16), upper, preferred_element_type=f32)
    picked = jnp.where((rank == slot_rank) & (row_block == slot_block), named, 0.0)
    sel[...] = picked.astype(bf16)

    load_ffn.wait()
    load_mix = load(mix_in, mix_v, 1)
    load_q = load(query_weight, qw, 2)
    load_l = load(latent_weight, lw, 3)
    load_r = load(rotary_weight, rw, 4)
    load_k = load(key_weight, kw, 5)
    load_v = load(value_weight, vw, 6)
    load_g = load(gate_weight.at[0], gw, 7)
    load_u = load(up_weight.at[0], uw, 8)
    load_d = load(
        down_weight.at[0, :, pl.ds(pl.multiple_of(t * width, 128), width)], wd.at[t], 9
    )
    load_o = load(output_weight, ow, 10)
    ffn_v[...] = rms(ffn_v[...].astype(f32), ffn_gain[...]).astype(bf16)
    columns = pl.ds(pl.multiple_of(t * width, 128), width)
    outg[...] = jnp.dot(sel[...], ffn_v[:, columns], preferred_element_type=f32).astype(bf16)
    own_z = pl.ds(pl.multiple_of(z * unit, unit), unit)
    for part in range(TP):
        near[part] = jnp.dot(
            sel[own_z, :], ffn_v[:, part * width : (part + 1) * width], preferred_element_type=f32
        ).astype(bf16)

    base = base_turn[pl.ds(e, 1), :]
    base_cos, base_sin = base[:, :128], base[:, 128:]
    row_cos, row_sin = row_turn[:, :128], row_turn[:, 128:]
    cosine = base_cos * row_cos - base_sin * row_sin
    sine = base_sin * row_cos + base_cos * row_sin
    lane = iota((rows, 128), 1)
    first_half = lane % ROPE < ROPE // 2
    sine = jnp.where(first_half, -sine, sine)

    def turned(v):
        partner = jnp.where(first_half, pltpu.roll(v, 96, 1), pltpu.roll(v, 32, 1))
        return v * cosine + partner * sine

    load_w.wait()
    with jax.named_scope("barrier"):
        pl.semaphore_wait(barrier, E - 1 + TP - 1)

    def share_down(step):
        peer = lax.rem(t + step, TP)
        send(
            dw.at[:, pl.ds(pl.multiple_of(peer * width, 128), width)],
            wd.at[t],
            send_sem.at[1],
            one_recv.at[0],
            e,
            peer,
        )

    share_down(1)
    share_down(TP - 1)

    my_rows = pl.ds(pl.multiple_of(e * cell, cell), cell)

    @pl.loop(1, J)
    def _(step):
        to = lax.rem(j + step, J)
        send(
            near.at[:, pl.ds(pl.multiple_of(to * cell, cell), cell)],
            X.at[:, my_rows],
            send_sem.at[0],
            disp_recv.at[0],
            z * J + to,
            t,
        )

    for part in range(TP):
        X[part, my_rows] = near[part, pl.ds(pl.multiple_of(j * cell, cell), cell)]

    def dispatch(number):
        target_z = lax.rem(z + NZ - ORDER[number], NZ)

        @pl.loop(0, J)
        def _(step):
            target = target_z * J + lax.rem(j + step, J)
            send(
                outg.at[pl.ds(pl.multiple_of(target * cell, cell), cell)],
                X.at[t, my_rows],
                send_sem.at[13],
                disp_recv.at[number],
                target,
                t,
            )

    up_z, down_z = lax.rem(z + 1, NZ), lax.rem(z + NZ - 1, NZ)
    half = rows // 2

    def pass_on(hop):
        if hop > 0:
            at_up, at_down = lax.rem(z + NZ - hop, NZ), lax.rem(z + hop, NZ)
            drain(KV.at[at_up], kv_recv.at[0, hop - 1])
            drain(KV.at[at_down], kv_recv.at[1, hop - 1])
        else:
            at_up = at_down = z
        upward, downward = KV.at[at_up], KV.at[at_down]
        if 2 * (hop + 1) == NZ:
            upward, downward = KV.at[at_up, pl.ds(0, half)], KV.at[at_down, pl.ds(half, half)]
        send(upward, upward, send_sem.at[3], kv_recv.at[0, hop], up_z * J + j, t)
        send(downward, downward, send_sem.at[3], kv_recv.at[1, hop], down_z * J + j, t)

    def latents_here():
        across = lax.rem(z + NZ // 2, NZ)
        drain(KV.at[across, pl.ds(0, half)], kv_recv.at[0, NZ // 2 - 1])
        drain(KV.at[across, pl.ds(half, half)], kv_recv.at[1, NZ // 2 - 1])

    def own_norm():
        load_mix.wait()
        mix_v[...] = rms(mix_v[...].astype(f32), mix_gain[...]).astype(bf16)

    def own_latents():
        load_l.wait()
        latent = jnp.dot(mix_v[...], lw[...], preferred_element_type=f32)
        KV[z, :, 0:512] = rms(latent, latent_gain[...]).astype(bf16)
        load_r.wait()
        rotary = lax.dot_general(
            mix_v[...], rw[...], (((1,), (1,)), ((), ())), preferred_element_type=f32
        )
        KV[z, :, 512:640] = turned(jnp.concatenate([rotary, rotary], axis=1)).astype(bf16)

        pass_on(0)

    mate = j + 1 - 2 * lax.rem(j, 2)

    def own_queries():
        load_q.wait()
        queries = jnp.dot(mix_v[...], qw[...], preferred_element_type=f32)
        low_lanes = lane < 64
        A = [queries[:, 128 * i : 128 * (i + 1)] for i in range(6)]
        q_out[:, 0:128] = A[0].astype(bf16)
        q_out[:, 128:256] = pltpu.roll(jnp.where(low_lanes, A[2], A[1]), 64, 1).astype(bf16)
        q_out[:, 256:384] = A[3].astype(bf16)
        q_out[:, 384:512] = pltpu.roll(jnp.where(low_lanes, A[5], A[4]), 64, 1).astype(bf16)
        q_out[:, 512:640] = turned(jnp.where(low_lanes, A[1], A[2])).astype(bf16)
        q_out[:, 640:768] = turned(jnp.where(low_lanes, A[4], A[5])).astype(bf16)
        Q[j] = q_out[...]
        for step in range(2, J, 2):
            send(Q.at[j], Q.at[j], send_sem.at[2], one_recv.at[1], z * J + lax.rem(j + step, J), t)
        send(Q.at[j], Q.at[j], send_sem.at[14], one_recv.at[8], z * J + mate, t)

    def share_queries():
        drain(Q.at[pl.ds(0, J // 2 - 1)], one_recv.at[1])
        for step in range(2, J, 2):
            from_j = lax.rem(j + step, J)
            send(Q.at[from_j], Q.at[from_j], send_sem.at[14], one_recv.at[8], z * J + mate, t)

    def weigh():
        score = route_scores[...]
        grown = jnp.exp(score - jnp.max(score, axis=0, keepdims=True))
        share = grown / jnp.sum(grown, axis=0, keepdims=True)
        gates = jnp.zeros((slots, rows), f32)
        for k in range(choose):
            gates = gates + jnp.where(route[k : k + 1, :] == slot_expert, share[k : k + 1, :], 0.0)
        gates = jnp.transpose(gates * sel[...].astype(f32))
        gates_hi = gates.astype(bf16)
        w_hi[...] = gates_hi
        w_lo[...] = (gates - gates_hi.astype(f32)).astype(bf16)

    def unit_rows(number):
        source_z = lax.rem(z + ORDER[number], NZ)
        return pl.ds(pl.multiple_of(source_z * unit, unit), unit)

    def spread(buf, number, sems, base_send):
        place = unit_rows(number)
        send(buf.at[t, place], buf.at[t, place], send_sem.at[base_send], sems.at[0, number], e, right)
        send(buf.at[t, place], buf.at[t, place], send_sem.at[base_send], sems.at[1, number], e, left)
        if buf is H and number in DIRECT:
            send(
                buf.at[t, place],
                buf.at[t, place],
                send_sem.at[base_send + 1],
                sems.at[2, number],
                e,
                lax.rem(t + 2, TP),
            )

    def relay(buf, number, sems, base_send):
        place = unit_rows(number)
        drain(buf.at[left, place], sems.at[0, number])
        drain(buf.at[right, place], sems.at[1, number])
        if buf is H and number in DIRECT:
            return
        if number % 2 == 0 or (buf is H and number in (1, 7)):
            send(
                buf.at[left, place],
                buf.at[left, place],
                send_sem.at[base_send + 1],
                sems.at[2, number],
                e,
                right,
            )
        else:
            send(
                buf.at[right, place],
                buf.at[right, place],
                send_sem.at[base_send + 1],
                sems.at[2, number],
                e,
                left,
            )

    def relayed(buf, number, sems):
        across = lax.rem(t + 2, TP)
        drain(buf.at[across, unit_rows(number)], sems.at[2, number])

    def take(number):
        if number == 0:
            drain(X.at[:, pl.ds(0, unit - cell)], disp_recv.at[0])
        else:
            drain(X.at[t, pl.ds(0, unit)], disp_recv.at[number])
            spread(X, number, x_recv, 4)

    def hidden(batch):
        pair = BATCHES[batch]
        for number in pair:
            if number > 0:
                relayed(X, number, x_recv)
        tall = len(pair) * unit
        gate_part = jnp.zeros((tall, gw.shape[1]), f32)
        up_part = jnp.zeros((tall, gw.shape[1]), f32)
        for part in range(TP):
            block = jnp.concatenate([X[part, unit_rows(number)] for number in pair], axis=0)
            depth = pl.ds(part * width, width)
            gate_part = gate_part + jnp.dot(block, gw[depth, :], preferred_element_type=f32)
            up_part = up_part + jnp.dot(block, uw[depth, :], preferred_element_type=f32)
        gate_part = jnp.minimum(gate_part, clamp_limit)
        up_part = jnp.clip(up_part, -clamp_limit, clamp_limit)
        result = (gate_part * jax.nn.sigmoid(gate_slope * gate_part) * (up_part + 1.0)).astype(bf16)
        for i, number in enumerate(pair):
            H[t, unit_rows(number)] = result[i * unit : (i + 1) * unit]
        for number in pair:
            spread(H, number, h_recv, 6)

    def hidden_relay(batch):
        for number in BATCHES[batch]:
            relay(H, number, h_recv, 6)

    def down(batch):
        pair = BATCHES[batch]
        for number in pair:
            relayed(H, number, h_recv)
        total = jnp.zeros((len(pair) * unit, width), f32)
        for part in range(TP):
            block = jnp.concatenate([H[part, unit_rows(number)] for number in pair], axis=0)
            total = total + jnp.dot(block, wd[part], preferred_element_type=f32)
        total = total.astype(bf16)
        for i, number in enumerate(pair):
            Dn[unit_rows(number), :] = total[i * unit : (i + 1) * unit]
        for number in pair:
            source_z = lax.rem(z + ORDER[number], NZ)

            @pl.loop(1 if ORDER[number] == 0 else 0, J)
            def _(step, source_z=source_z, back=9 if number in LATE else 3):
                source = source_z * J + lax.rem(j + step, J)
                send(
                    Dn.at[pl.ds(pl.multiple_of(source * cell, cell), cell)],
                    R.at[my_rows],
                    send_sem.at[8],
                    one_recv.at[back],
                    source,
                    t,
                )

            if ORDER[number] == 0:
                R[my_rows, :] = Dn[my_rows, :]

    def expand():
        drain(Q.at[pl.ds(0, J // 2)], one_recv.at[8])
        latents_here()
        load_k.wait()
        load_v.wait()
        lat = jnp.concatenate([KV[lax.rem(z + p, NZ)] for p in range(NZ)], axis=0)
        turn = lat[:, 512:640]
        keys = jnp.dot(lat[:, :512], kw[...], preferred_element_type=f32).astype(bf16)
        values = jnp.dot(lat[:, :512], vw[...], preferred_element_type=f32).astype(bf16)
        low = iota((rows, 128), 1) < 64
        zero = jnp.zeros((rows, 128), bf16)
        for p in range(NZ):
            here = slice(p * rows, (p + 1) * rows)
            earlier = z + p >= NZ
            keep = (lambda v: v) if p == 0 else (lambda v, earlier=earlier: jnp.where(earlier, v, zero))
            piece = keep(turn[here])
            even, odd = jnp.where(low, piece, zero), jnp.where(low, zero, piece)
            ones = keep(jnp.ones((rows, 128), bf16))
            for h in range(4):
                Kc[h, here, 0:128] = keep(keys[here, 128 * h : 128 * (h + 1)])
                Kc[h, here, 128:256] = even if h % 2 == 0 else odd
                Vc[h, here, 0:128] = keep(values[here, 128 * h : 128 * (h + 1)])
                Vc[h, here, 128:256] = ones

    scale = (NOPE + ROPE) ** (-0.5) * float(np.log2(np.e))

    def head(part):
        h, chunk = part // 2, part % 2
        span = (J // 2) * rows
        plain = Q[chunk * (J // 2) : (chunk + 1) * (J // 2), :, 128 * h : 128 * (h + 1)].reshape(span, 128)
        pair = 512 + 128 * (h // 2)
        turn = Q[chunk * (J // 2) : (chunk + 1) * (J // 2), :, pair : pair + 128].reshape(span, 128)
        both = jnp.concatenate([plain, turn], axis=1)
        scores = lax.dot_general(
            both, Kc[h], (((1,), (1,)), ((), ())), preferred_element_type=f32
        )
        grown = jnp.exp2(scores * scale)
        key_place = j * rows + iota((1, rows), 1)
        query_place = chunk * span + iota((span, 1), 0)
        near_z = jnp.where(key_place <= query_place, grown[:, :rows], 0.0)
        weights = jnp.concatenate([near_z.astype(bf16), grown[:, rows:].astype(bf16)], axis=1)
        both_out = jnp.dot(weights, Vc[h], preferred_element_type=f32)
        here = slice(chunk * span, (chunk + 1) * span)
        o_out[h, here, :] = both_out[:, :128].astype(bf16)
        sums = both_out[:, 128:]
        if h == 0:
            t_out[here, :] = sums
        else:
            lanes = iota((span, 128), 1)
            t_out[here, :] = jnp.where(lanes // 32 == h, sums, t_out[here, :])

    back_order = (4, 2, 6, 3, 5, 1, 7)

    def give_back(h):
        for step in back_order:
            target = lax.rem(j + step, J)
            place = pl.ds(pl.multiple_of(target * rows, rows), rows)
            send(o_out.at[h, place], o_in.at[h, j], send_sem.at[9], one_recv.at[4], z * J + target, t)
        o_in[h, j] = o_out[h, pl.ds(pl.multiple_of(j * rows, rows), rows), :]

    def give_totals():
        for i in range(J):
            across = jnp.transpose(t_out[i * rows : (i + 1) * rows, :])
            picks = [across[32 * h : 32 * h + 1, :] for h in range(4)]
            t_row[i] = jnp.concatenate(picks + picks, axis=0)
        for step in back_order:
            target = lax.rem(j + step, J)
            send(t_row.at[target], t_in.at[j], send_sem.at[10], one_recv.at[5], z * J + target, t)
        t_in[j] = t_row[j]

    quarter = rows // TP
    far_first = sorted(range(1, TP), key=lambda step: -min(step, TP - step))

    def project():
        drain(o_in.at[:, pl.ds(0, J - 1)], one_recv.at[4])
        drain(t_in.at[pl.ds(0, J - 1)], one_recv.at[5])
        load_o.wait()
        tsum = jnp.zeros(t_in.shape[1:], f32)
        for i in range(J):
            tsum = tsum + t_in[i]
        tsum = jnp.transpose(jnp.concatenate([tsum] * (128 // tsum.shape[0]), axis=0))
        heads = []
        for h in range(4):
            osum = jnp.zeros((rows, VD), f32)
            for i in range(J):
                osum = osum + o_in[h, i].astype(f32)
            heads.append((osum / tsum[:, h : h + 1]).astype(bf16))
        attended = jnp.concatenate(heads, axis=1)
        p_out[...] = jnp.dot(attended, ow[...], preferred_element_type=f32).astype(bf16)
        for step in far_first:
            peer = lax.rem(t + step, TP)
            place = pl.ds(pl.multiple_of(peer * quarter, quarter), quarter)
            send(p_out.at[place], p_in.at[t], send_sem.at[11], one_recv.at[6], e, peer)
        p_in[t] = p_out[pl.ds(pl.multiple_of(t * quarter, quarter), quarter), :]

    def finish_mixed():
        drain(p_in.at[pl.ds(0, TP - 1)], one_recv.at[6])
        projected = jnp.zeros((quarter, p_in.shape[2]), f32)
        for i in range(TP):
            projected = projected + p_in[i].astype(f32)
        mixed_out[...] = rms(projected, out_gain[...]).astype(bf16)

    def add_up(total, numbers, back):
        count = len(numbers) * unit - (cell if 0 in numbers else 0)
        with jax.named_scope("returns"):
            drain(R.at[pl.ds(0, count)], one_recv.at[back])
        for number in numbers:
            from_z = lax.rem(z + NZ - ORDER[number], NZ)
            place = pl.ds(pl.multiple_of(from_z * unit, unit), unit)
            total = total + jnp.dot(w_hi[:, place], R[place, :], preferred_element_type=f32)
            total = total + jnp.dot(w_lo[:, place], R[place, :], preferred_element_type=f32)
        return total

    with jax.named_scope("s00_share_down_0"):
        share_down(2)
    with jax.named_scope("s01_dispatch_6"):
        dispatch(6)
    with jax.named_scope("s02_dispatch_3"):
        dispatch(3)
    with jax.named_scope("s03_dispatch_5"):
        dispatch(5)
    with jax.named_scope("s04_dispatch_2"):
        dispatch(2)
    with jax.named_scope("s05_own_norm_"):
        own_norm()
    with jax.named_scope("s06_own_latents_0"):
        own_latents()
    with jax.named_scope("s07_take_6"):
        take(6)
    with jax.named_scope("s08_dispatch_4"):
        dispatch(4)
    with jax.named_scope("s09_own_queries_0"):
        own_queries()
    with jax.named_scope("s10_take_3"):
        take(3)
    with jax.named_scope("s11_take_2"):
        take(2)
    with jax.named_scope("s12_take_5"):
        take(5)
    with jax.named_scope("s13_pass_on_1"):
        pass_on(1)
    with jax.named_scope("s14_relay_3"):
        relay(X, 3, x_recv, 4)
    with jax.named_scope("s15_relay_2"):
        relay(X, 2, x_recv, 4)
    with jax.named_scope("s16_dispatch_1"):
        dispatch(1)
    with jax.named_scope("s17_take_4"):
        take(4)
    with jax.named_scope("s18_share_queries_0"):
        share_queries()
    with jax.named_scope("s19_pass_on_2"):
        pass_on(2)
    with jax.named_scope("s20_load_gu_"):
        load_g.wait()
        load_u.wait()
    with jax.named_scope("s21_hidden_1"):
        hidden(1)
    with jax.named_scope("s22_relay_4"):
        relay(X, 4, x_recv, 4)
    with jax.named_scope("s23_relay_5"):
        relay(X, 5, x_recv, 4)
    with jax.named_scope("s24_dispatch_7"):
        dispatch(7)
    with jax.named_scope("s25_weigh_0"):
        weigh()
    with jax.named_scope("s26_hidden_relay_1"):
        hidden_relay(1)
    with jax.named_scope("s27_pass_on_3"):
        pass_on(3)
    with jax.named_scope("s28_take_1"):
        take(1)
    with jax.named_scope("s29_hidden_2"):
        hidden(2)
    with jax.named_scope("s30_load_dd_"):
        load_d.wait()
        drain(wd.at[pl.ds(0, TP - 1)], one_recv.at[0])
    with jax.named_scope("s31_down_1"):
        down(1)
    with jax.named_scope("s32_expand_0"):
        expand()
    with jax.named_scope("s33_relay_6"):
        relay(X, 6, x_recv, 4)
    with jax.named_scope("s34_relay_1"):
        relay(X, 1, x_recv, 4)
    with jax.named_scope("s35_head_0"):
        head(0)
    with jax.named_scope("s36_head_1"):
        head(1)
        give_back(0)
    with jax.named_scope("s37_head_2"):
        head(2)
    with jax.named_scope("s38_hidden_relay_2"):
        hidden_relay(2)
    with jax.named_scope("s39_take_0"):
        take(0)
    with jax.named_scope("s40_take_7"):
        take(7)
    with jax.named_scope("s41_head_3"):
        head(3)
        give_back(1)
    with jax.named_scope("s42_head_4"):
        head(4)
    with jax.named_scope("s43_head_5"):
        head(5)
        give_back(2)
    with jax.named_scope("s44_hidden_0"):
        hidden(0)
    with jax.named_scope("s45_head_6"):
        head(6)
    with jax.named_scope("s47_head_7"):
        head(7)
        give_back(3)
        give_totals()
    with jax.named_scope("s46_relay_7"):
        relay(X, 7, x_recv, 4)
    with jax.named_scope("s48_down_2"):
        down(2)
    with jax.named_scope("s49_hidden_relay_0"):
        hidden_relay(0)
    with jax.named_scope("s50_hidden_3"):
        hidden(3)
    with jax.named_scope("s51_hidden_4"):
        hidden(4)
    with jax.named_scope("s52_down_0"):
        down(0)
    with jax.named_scope("s53_project_0"):
        project()
    with jax.named_scope("s54_hidden_relay_3"):
        hidden_relay(3)
    with jax.named_scope("s55_down_3"):
        down(3)
    with jax.named_scope("s56_hidden_relay_4"):
        hidden_relay(4)
    with jax.named_scope("s57_down_4"):
        down(4)
    total = jnp.zeros((rows, width), f32)
    total = add_up(total, tuple(n for n in range(NZ) if n not in LATE), 3)

    total = add_up(total, LATE, 9)
    m_send[...] = total.astype(bf16)
    for step in far_first:
        peer = lax.rem(t + step, TP)
        place = pl.ds(pl.multiple_of(peer * quarter, quarter), quarter)
        send(m_send.at[place], m_recv.at[t], send_sem.at[12], one_recv.at[7], e, peer)
    m_recv[t] = m_send[pl.ds(pl.multiple_of(t * quarter, quarter), quarter), :]
    with jax.named_scope("s58_finish_mixed_0"):
        finish_mixed()
    with jax.named_scope("last"):
        drain(m_recv.at[pl.ds(0, TP - 1)], one_recv.at[7])
    for i in range(TP):
        moe_out[:, i * width : (i + 1) * width] = m_recv[i]

    most = slots - unit
    drain(X.at[:, pl.ds(0, unit - cell)], send_sem.at[0])
    drain(outg.at[pl.ds(0, most)], send_sem.at[13])
    drain(wd.at[pl.ds(0, TP - 1)], send_sem.at[1])
    drain(Q.at[pl.ds(0, J // 2 - 1)], send_sem.at[2])
    drain(Q.at[pl.ds(0, J // 2)], send_sem.at[14])
    drain(KV.at[pl.ds(0, NZ - 1)], send_sem.at[3])
    drain(X.at[pl.ds(0, 2), pl.ds(0, most)], send_sem.at[4])
    drain(X.at[0, pl.ds(0, most)], send_sem.at[5])
    drain(H.at[pl.ds(0, 2)], send_sem.at[6])
    drain(H.at[0], send_sem.at[7])
    drain(Dn.at[pl.ds(0, slots - cell)], send_sem.at[8])
    drain(o_in.at[:, pl.ds(0, J - 1)], send_sem.at[9])
    drain(t_in.at[pl.ds(0, J - 1)], send_sem.at[10])
    drain(p_in.at[pl.ds(0, TP - 1)], send_sem.at[11])
    drain(m_recv.at[pl.ds(0, TP - 1)], send_sem.at[12])


def turn_tables(devices, rows):
    inverse = rope_base ** (-np.arange(0, ROPE, 2) / ROPE)
    inverse = np.tile(inverse, 4)[None, :]
    base = np.arange(devices)[:, None] * rows * inverse
    row = np.arange(rows)[:, None] * inverse
    return (
        np.concatenate([np.cos(base), np.sin(base)], axis=1).astype(np.float32),
        np.concatenate([np.cos(row), np.sin(row)], axis=1).astype(np.float32),
    )


def solution(mesh):
    EP, TP = mesh.shape["ep"], mesh.shape["tp"]
    J = 8
    NZ = EP // J
    placed = (
        P("ep", None),
        P(),
        P(None, "tp"),
        P(),
        P(),
        P(),
        P(None, "tp"),
        P(None, "tp"),
        P("tp", None),
        P(),
        P("ep", None),
        P(),
        P("ep", None, "tp"),
        P("ep", None, "tp"),
        P("ep", "tp", None),
        P("ep", None),
        P("ep", None),
    )

    def local(
        mix_in,
        mix_gain,
        query_weight,
        latent_weight,
        rotary_weight,
        latent_gain,
        key_weight,
        value_weight,
        output_weight,
        out_gain,
        ffn_in,
        ffn_gain,
        gate_weight,
        up_weight,
        down_weight,
        routes,
        route_scores,
    ):
        rows, D = mix_in.shape
        width = D // TP
        cell = MOST * (rows // QB)
        slots = EP * cell
        unit = gate_weight.shape[2]
        quarter = rows // TP
        base_turn, row_turn = turn_tables(EP, rows)
        hbm = pl.BlockSpec(memory_space=pl.ANY)
        vmem = pl.BlockSpec(memory_space=pltpu.VMEM)
        V = lambda *shape: pltpu.VMEM(shape, bf16)
        F = lambda *shape: pltpu.VMEM(shape, f32)
        S = pltpu.SemaphoreType.DMA

        def body(*refs):
            kernel(NZ, J, TP, *refs)

        out = pltpu.VMEM((quarter, D), bf16)
        return pl.pallas_call(
            body,
            name="layer",
            out_shape=(out, out),
            in_specs=[
                hbm, vmem, hbm, hbm, hbm, vmem, hbm, hbm, hbm, vmem,
                hbm, vmem, hbm, hbm, hbm, vmem, vmem, vmem, vmem,
            ],
            out_specs=(vmem, vmem),
            scratch_shapes=[
                V(rows, D),
                V(rows, D),
                V(D, query_weight.shape[1]),
                V(D, latent_weight.shape[1]),
                V(ROPE, D),
                V(*key_weight.shape),
                V(*value_weight.shape),
                V(*output_weight.shape),
                V(D, unit),
                V(D, unit),
                V(TP, unit, width),
                V(unit, D),
                V(slots, width),
                V(TP, J * cell, width),
                V(TP, slots, width),
                V(TP, slots, unit),
                V(slots, width),
                V(slots, width),
                V(slots, rows),
                V(rows, slots),
                V(rows, slots),
                V(rows, width),
                V(TP, quarter, width),
                V(J, rows, 768),
                V(NZ, rows, 640),
                V(rows, 768),
                V(4, NZ * rows, 256),
                V(4, NZ * rows, 256),
                V(4, J * rows, VD),
                F(J * rows, 128),
                F(J, 8, rows),
                V(4, J, rows, VD),
                F(J, 8, rows),
                V(rows, D),
                V(TP, quarter, D),
                S((12,)),
                S((8,)),
                S((3, 8)),
                S((3, 8)),
                S((2, NZ // 2)),
                S((10,)),
                S((15,)),
            ],
            compiler_params=pltpu.CompilerParams(
                collective_id=0, has_side_effects=True, vmem_limit_bytes=62 * 1024 * 1024
            ),
        )(
            mix_in,
            mix_gain[None, :],
            query_weight,
            latent_weight,
            rotary_weight.T,
            latent_gain[None, :],
            key_weight,
            value_weight,
            output_weight,
            out_gain[None, :],
            ffn_in,
            ffn_gain[None, :],
            gate_weight,
            up_weight,
            down_weight,
            routes.T,
            route_scores.T,
            base_turn,
            row_turn,
        )

    return jax.shard_map(
        local,
        mesh=mesh,
        in_specs=placed,
        out_specs=(P(("ep", "tp"), None), P(("ep", "tp"), None)),
        check_vma=False,
    )
```

```python
import jax
import jax.numpy as jnp
import numpy as np
from jax import lax
from jax.experimental import pallas as pl
from jax.experimental.pallas import tpu as pltpu
from jax.sharding import PartitionSpec as P

NOPE = 128
ROPE = 64
VD = 128
QB = 32
MOST = 4

norm_eps = 1e-06
clamp_limit = 7.0
gate_slope = 1.702
rope_base = 10000.0

MESH = pl.DeviceIdType.MESH
bf16 = jnp.bfloat16
f32 = jnp.float32

ORDER = (0, 4, 3, 5, 2, 6, 1, 7)

BATCHES = ((0, 1), (2, 3), (4, 5), (6,), (7,))
LATE = (6, 7)
DIRECT = (6, 7)


def iota(shape, dim):
    return lax.broadcasted_iota(jnp.int32, shape, dim)


def rms(rows, gain):
    mean_square = jnp.mean(rows * rows, axis=-1, keepdims=True)
    return rows * lax.rsqrt(mean_square + norm_eps) * gain


def drain(view, sem):
    with jax.named_scope("wait"):
        pltpu.make_async_copy(view, view, sem).wait()


def kernel(
    NZ,
    J,
    TP,
    mix_in,
    mix_gain,
    query_weight,
    latent_weight,
    rotary_weight,
    latent_gain,
    key_weight,
    value_weight,
    output_weight,
    out_gain,
    ffn_in,
    ffn_gain,
    gate_weight,
    up_weight,
    down_weight,
    routes,
    route_scores,
    base_turn,
    row_turn,
    mixed_out,
    moe_out,
    mix_v,
    ffn_v,
    qw,
    lw,
    rw,
    kw,
    vw,
    ow,
    gw,
    uw,
    wd,
    dw,
    outg,
    near,
    X,
    H,
    Dn,
    R,
    sel,
    w_hi,
    w_lo,
    m_send,
    m_recv,
    Q,
    KV,
    q_out,
    Kc,
    Vc,
    o_out,
    t_out,
    t_row,
    o_in,
    t_in,
    p_out,
    p_in,
    load_sem,
    disp_recv,
    x_recv,
    h_recv,
    kv_recv,
    one_recv,
    send_sem,
):
    E = NZ * J
    e = lax.axis_index("ep")
    t = lax.axis_index("tp")
    z = e // J
    j = e % J
    rows = ffn_v.shape[0]
    width = outg.shape[1]
    cell = outg.shape[0] // E
    right = lax.rem(t + 1, TP)
    left = lax.rem(t + TP - 1, TP)
    unit = J * cell

    def load(src, dst, number):
        copy = pltpu.make_async_copy(src, dst, load_sem.at[number])
        copy.start()
        return copy

    def send(src, dst, s_sem, r_sem, ep, tp):
        pltpu.make_async_remote_copy(
            src_ref=src,
            dst_ref=dst,
            send_sem=s_sem,
            recv_sem=r_sem,
            device_id=(ep, tp),
            device_id_type=MESH,
        ).start()

    load_ffn = load(ffn_in, ffn_v, 0)
    load_w = load(down_weight.at[0], dw, 11)

    barrier = pltpu.get_barrier_semaphore()

    for dz in (4, 3, 5, 2, 6, 1, 7, 0):

        @pl.loop(1 if dz == 0 else 0, J, unroll=True)
        def _(step, dz=dz):
            peer = lax.rem(z + dz, NZ) * J + lax.rem(j + step, J)
            pl.semaphore_signal(barrier, inc=1, device_id=(peer, t), device_id_type=MESH)

    for step in range(1, TP):
        pl.semaphore_signal(
            barrier, inc=1, device_id=(e, lax.rem(t + step, TP)), device_id_type=MESH
        )


    slots = outg.shape[0]
    blocks = rows // QB
    slot = iota((slots, 1), 0)
    slot_expert = slot // cell
    slot_block = (slot // MOST) % blocks
    slot_rank = (slot % MOST).astype(f32)
    row_block = iota((1, rows), 1) // QB
    route = routes[...]
    choose = route.shape[0]
    named = jnp.zeros((slots, rows), f32)
    for k in range(choose):
        named = named + jnp.where(route[k : k + 1, :] == slot_expert, 1.0, 0.0)
    up_r = iota((rows, rows), 0)
    up_c = iota((rows, rows), 1)
    upper = jnp.where((up_r < up_c) & (up_c // QB == up_r // QB), 1.0, 0.0).astype(bf16)
    rank = jnp.dot(named.astype(bf16), upper, preferred_element_type=f32)
    picked = jnp.where((rank == slot_rank) & (row_block == slot_block), named, 0.0)
    sel[...] = picked.astype(bf16)

    load_ffn.wait()
    load_mix = load(mix_in, mix_v, 1)
    load_q = load(query_weight, qw, 2)
    load_l = load(latent_weight, lw, 3)
    load_r = load(rotary_weight, rw, 4)
    load_k = load(key_weight, kw, 5)
    load_v = load(value_weight, vw, 6)
    load_g = load(gate_weight.at[0], gw, 7)
    load_u = load(up_weight.at[0], uw, 8)
    load_d = load(
        down_weight.at[0, :, pl.ds(pl.multiple_of(t * width, 128), width)], wd.at[t], 9
    )
    load_o = load(output_weight, ow, 10)
    ffn_v[...] = rms(ffn_v[...].astype(f32), ffn_gain[...]).astype(bf16)
    columns = pl.ds(pl.multiple_of(t * width, 128), width)
    outg[...] = jnp.dot(sel[...], ffn_v[:, columns], preferred_element_type=f32).astype(bf16)
    own_z = pl.ds(pl.multiple_of(z * unit, unit), unit)
    for part in range(TP):
        near[part] = jnp.dot(
            sel[own_z, :], ffn_v[:, part * width : (part + 1) * width], preferred_element_type=f32
        ).astype(bf16)

    base = base_turn[pl.ds(e, 1), :]
    base_cos, base_sin = base[:, :128], base[:, 128:]
    row_cos, row_sin = row_turn[:, :128], row_turn[:, 128:]
    cosine = base_cos * row_cos - base_sin * row_sin
    sine = base_sin * row_cos + base_cos * row_sin
    lane = iota((rows, 128), 1)
    first_half = lane % ROPE < ROPE // 2
    sine = jnp.where(first_half, -sine, sine)

    def turned(v):
        partner = jnp.where(first_half, pltpu.roll(v, 96, 1), pltpu.roll(v, 32, 1))
        return v * cosine + partner * sine

    load_w.wait()
    with jax.named_scope("barrier"):
        pl.semaphore_wait(barrier, E - 1 + TP - 1)

    def share_down(step):
        peer = lax.rem(t + step, TP)
        send(
            dw.at[:, pl.ds(pl.multiple_of(peer * width, 128), width)],
            wd.at[t],
            send_sem.at[1],
            one_recv.at[0],
            e,
            peer,
        )

    share_down(1)
    share_down(TP - 1)

    my_rows = pl.ds(pl.multiple_of(e * cell, cell), cell)

    @pl.loop(1, J)
    def _(step):
        to = lax.rem(j + step, J)
        send(
            near.at[:, pl.ds(pl.multiple_of(to * cell, cell), cell)],
            X.at[:, my_rows],
            send_sem.at[0],
            disp_recv.at[0],
            z * J + to,
            t,
        )

    for part in range(TP):
        X[part, my_rows] = near[part, pl.ds(pl.multiple_of(j * cell, cell), cell)]

    def dispatch(number):
        target_z = lax.rem(z + NZ - ORDER[number], NZ)

        @pl.loop(0, J)
        def _(step):
            target = target_z * J + lax.rem(j + step, J)
            send(
                outg.at[pl.ds(pl.multiple_of(target * cell, cell), cell)],
                X.at[t, my_rows],
                send_sem.at[13],
                disp_recv.at[number],
                target,
                t,
            )

    up_z, down_z = lax.rem(z + 1, NZ), lax.rem(z + NZ - 1, NZ)
    half = rows // 2

    def pass_on(hop):
        if hop > 0:
            at_up, at_down = lax.rem(z + NZ - hop, NZ), lax.rem(z + hop, NZ)
            drain(KV.at[at_up], kv_recv.at[0, hop - 1])
            drain(KV.at[at_down], kv_recv.at[1, hop - 1])
        else:
            at_up = at_down = z
        upward, downward = KV.at[at_up], KV.at[at_down]
        if 2 * (hop + 1) == NZ:
            upward, downward = KV.at[at_up, pl.ds(0, half)], KV.at[at_down, pl.ds(half, half)]
        send(upward, upward, send_sem.at[3], kv_recv.at[0, hop], up_z * J + j, t)
        send(downward, downward, send_sem.at[3], kv_recv.at[1, hop], down_z * J + j, t)

    def latents_here():
        across = lax.rem(z + NZ // 2, NZ)
        drain(KV.at[across, pl.ds(0, half)], kv_recv.at[0, NZ // 2 - 1])
        drain(KV.at[across, pl.ds(half, half)], kv_recv.at[1, NZ // 2 - 1])

    def own_norm():
        load_mix.wait()
        mix_v[...] = rms(mix_v[...].astype(f32), mix_gain[...]).astype(bf16)

    def own_latents():
        load_l.wait()
        latent = jnp.dot(mix_v[...], lw[...], preferred_element_type=f32)
        KV[z, :, 0:512] = rms(latent, latent_gain[...]).astype(bf16)
        load_r.wait()
        rotary = lax.dot_general(
            mix_v[...], rw[...], (((1,), (1,)), ((), ())), preferred_element_type=f32
        )
        KV[z, :, 512:640] = turned(jnp.concatenate([rotary, rotary], axis=1)).astype(bf16)

        pass_on(0)

    mate = j + 1 - 2 * lax.rem(j, 2)

    def own_queries():
        load_q.wait()
        queries = jnp.dot(mix_v[...], qw[...], preferred_element_type=f32)
        low_lanes = lane < 64
        A = [queries[:, 128 * i : 128 * (i + 1)] for i in range(6)]
        q_out[:, 0:128] = A[0].astype(bf16)
        q_out[:, 128:256] = pltpu.roll(jnp.where(low_lanes, A[2], A[1]), 64, 1).astype(bf16)
        q_out[:, 256:384] = A[3].astype(bf16)
        q_out[:, 384:512] = pltpu.roll(jnp.where(low_lanes, A[5], A[4]), 64, 1).astype(bf16)
        q_out[:, 512:640] = turned(jnp.where(low_lanes, A[1], A[2])).astype(bf16)
        q_out[:, 640:768] = turned(jnp.where(low_lanes, A[4], A[5])).astype(bf16)
        Q[j] = q_out[...]
        for step in range(2, J, 2):
            send(Q.at[j], Q.at[j], send_sem.at[2], one_recv.at[1], z * J + lax.rem(j + step, J), t)
        send(Q.at[j], Q.at[j], send_sem.at[14], one_recv.at[8], z * J + mate, t)

    def share_queries():
        drain(Q.at[pl.ds(0, J // 2 - 1)], one_recv.at[1])
        for step in range(2, J, 2):
            from_j = lax.rem(j + step, J)
            send(Q.at[from_j], Q.at[from_j], send_sem.at[14], one_recv.at[8], z * J + mate, t)

    def weigh():
        score = route_scores[...]
        grown = jnp.exp(score - jnp.max(score, axis=0, keepdims=True))
        share = grown / jnp.sum(grown, axis=0, keepdims=True)
        gates = jnp.zeros((slots, rows), f32)
        for k in range(choose):
            gates = gates + jnp.where(route[k : k + 1, :] == slot_expert, share[k : k + 1, :], 0.0)
        gates = jnp.transpose(gates * sel[...].astype(f32))
        gates_hi = gates.astype(bf16)
        w_hi[...] = gates_hi
        w_lo[...] = (gates - gates_hi.astype(f32)).astype(bf16)

    def unit_rows(number):
        source_z = lax.rem(z + ORDER[number], NZ)
        return pl.ds(pl.multiple_of(source_z * unit, unit), unit)

    def spread(buf, number, sems, base_send):
        place = unit_rows(number)
        send(buf.at[t, place], buf.at[t, place], send_sem.at[base_send], sems.at[0, number], e, right)
        send(buf.at[t, place], buf.at[t, place], send_sem.at[base_send], sems.at[1, number], e, left)
        if buf is H and number in DIRECT:
            send(
                buf.at[t, place],
                buf.at[t, place],
                send_sem.at[base_send + 1],
                sems.at[2, number],
                e,
                lax.rem(t + 2, TP),
            )

    def relay(buf, number, sems, base_send):
        place = unit_rows(number)
        drain(buf.at[left, place], sems.at[0, number])
        drain(buf.at[right, place], sems.at[1, number])
        if buf is H and number in DIRECT:
            return
        if number % 2 == 0 or (buf is H and number in (1, 7)):
            send(
                buf.at[left, place],
                buf.at[left, place],
                send_sem.at[base_send + 1],
                sems.at[2, number],
                e,
                right,
            )
        else:
            send(
                buf.at[right, place],
                buf.at[right, place],
                send_sem.at[base_send + 1],
                sems.at[2, number],
                e,
                left,
            )

    def relayed(buf, number, sems):
        across = lax.rem(t + 2, TP)
        drain(buf.at[across, unit_rows(number)], sems.at[2, number])

    def take(number):
        if number == 0:
            drain(X.at[:, pl.ds(0, unit - cell)], disp_recv.at[0])
        else:
            drain(X.at[t, pl.ds(0, unit)], disp_recv.at[number])
            spread(X, number, x_recv, 4)

    def hidden(batch):
        pair = BATCHES[batch]
        for number in pair:
            if number > 0:
                relayed(X, number, x_recv)
        tall = len(pair) * unit
        gate_part = jnp.zeros((tall, gw.shape[1]), f32)
        up_part = jnp.zeros((tall, gw.shape[1]), f32)
        for part in range(TP):
            block = jnp.concatenate([X[part, unit_rows(number)] for number in pair], axis=0)
            depth = pl.ds(part * width, width)
            gate_part = gate_part + jnp.dot(block, gw[depth, :], preferred_element_type=f32)
            up_part = up_part + jnp.dot(block, uw[depth, :], preferred_element_type=f32)
        gate_part = jnp.minimum(gate_part, clamp_limit)
        up_part = jnp.clip(up_part, -clamp_limit, clamp_limit)
        result = (gate_part * jax.nn.sigmoid(gate_slope * gate_part) * (up_part + 1.0)).astype(bf16)
        for i, number in enumerate(pair):
            H[t, unit_rows(number)] = result[i * unit : (i + 1) * unit]
        for number in pair:
            spread(H, number, h_recv, 6)

    def hidden_relay(batch):
        for number in BATCHES[batch]:
            relay(H, number, h_recv, 6)

    def down(batch):
        pair = BATCHES[batch]
        for number in pair:
            relayed(H, number, h_recv)
        total = jnp.zeros((len(pair) * unit, width), f32)
        for part in range(TP):
            block = jnp.concatenate([H[part, unit_rows(number)] for number in pair], axis=0)
            total = total + jnp.dot(block, wd[part], preferred_element_type=f32)
        total = total.astype(bf16)
        for i, number in enumerate(pair):
            Dn[unit_rows(number), :] = total[i * unit : (i + 1) * unit]
        for number in pair:
            source_z = lax.rem(z + ORDER[number], NZ)

            @pl.loop(1 if ORDER[number] == 0 else 0, J)
            def _(step, source_z=source_z, back=9 if number in LATE else 3):
                source = source_z * J + lax.rem(j + step, J)
                send(
                    Dn.at[pl.ds(pl.multiple_of(source * cell, cell), cell)],
                    R.at[my_rows],
                    send_sem.at[8],
                    one_recv.at[back],
                    source,
                    t,
                )

            if ORDER[number] == 0:
                R[my_rows, :] = Dn[my_rows, :]

    def expand():
        drain(Q.at[pl.ds(0, J // 2)], one_recv.at[8])
        latents_here()
        load_k.wait()
        load_v.wait()
        lat = jnp.concatenate([KV[lax.rem(z + p, NZ)] for p in range(NZ)], axis=0)
        turn = lat[:, 512:640]
        keys = jnp.dot(lat[:, :512], kw[...], preferred_element_type=f32).astype(bf16)
        values = jnp.dot(lat[:, :512], vw[...], preferred_element_type=f32).astype(bf16)
        low = iota((rows, 128), 1) < 64
        zero = jnp.zeros((rows, 128), bf16)
        for p in range(NZ):
            here = slice(p * rows, (p + 1) * rows)
            earlier = z + p >= NZ
            keep = (lambda v: v) if p == 0 else (lambda v, earlier=earlier: jnp.where(earlier, v, zero))
            piece = keep(turn[here])
            even, odd = jnp.where(low, piece, zero), jnp.where(low, zero, piece)
            ones = keep(jnp.ones((rows, 128), bf16))
            for h in range(4):
                Kc[h, here, 0:128] = keep(keys[here, 128 * h : 128 * (h + 1)])
                Kc[h, here, 128:256] = even if h % 2 == 0 else odd
                Vc[h, here, 0:128] = keep(values[here, 128 * h : 128 * (h + 1)])
                Vc[h, here, 128:256] = ones

    scale = (NOPE + ROPE) ** (-0.5) * float(np.log2(np.e))

    def head(part):
        h, chunk = part // 2, part % 2
        span = (J // 2) * rows
        plain = Q[chunk * (J // 2) : (chunk + 1) * (J // 2), :, 128 * h : 128 * (h + 1)].reshape(span, 128)
        pair = 512 + 128 * (h // 2)
        turn = Q[chunk * (J // 2) : (chunk + 1) * (J // 2), :, pair : pair + 128].reshape(span, 128)
        both = jnp.concatenate([plain, turn], axis=1)
        scores = lax.dot_general(
            both, Kc[h], (((1,), (1,)), ((), ())), preferred_element_type=f32
        )
        grown = jnp.exp2(scores * scale)
        key_place = j * rows + iota((1, rows), 1)
        query_place = chunk * span + iota((span, 1), 0)
        near_z = jnp.where(key_place <= query_place, grown[:, :rows], 0.0)
        weights = jnp.concatenate([near_z.astype(bf16), grown[:, rows:].astype(bf16)], axis=1)
        both_out = jnp.dot(weights, Vc[h], preferred_element_type=f32)
        here = slice(chunk * span, (chunk + 1) * span)
        o_out[h, here, :] = both_out[:, :128].astype(bf16)
        sums = both_out[:, 128:]
        if h == 0:
            t_out[here, :] = sums
        else:
            lanes = iota((span, 128), 1)
            t_out[here, :] = jnp.where(lanes // 32 == h, sums, t_out[here, :])

    back_order = (4, 2, 6, 3, 5, 1, 7)

    def give_back(h):
        for step in back_order:
            target = lax.rem(j + step, J)
            place = pl.ds(pl.multiple_of(target * rows, rows), rows)
            send(o_out.at[h, place], o_in.at[h, j], send_sem.at[9], one_recv.at[4], z * J + target, t)
        o_in[h, j] = o_out[h, pl.ds(pl.multiple_of(j * rows, rows), rows), :]

    def give_totals():
        for i in range(J):
            across = jnp.transpose(t_out[i * rows : (i + 1) * rows, :])
            picks = [across[32 * h : 32 * h + 1, :] for h in range(4)]
            t_row[i] = jnp.concatenate(picks + picks, axis=0)
        for step in back_order:
            target = lax.rem(j + step, J)
            send(t_row.at[target], t_in.at[j], send_sem.at[10], one_recv.at[5], z * J + target, t)
        t_in[j] = t_row[j]

    quarter = rows // TP
    far_first = sorted(range(1, TP), key=lambda step: -min(step, TP - step))

    def project():
        drain(o_in.at[:, pl.ds(0, J - 1)], one_recv.at[4])
        drain(t_in.at[pl.ds(0, J - 1)], one_recv.at[5])
        load_o.wait()
        tsum = jnp.zeros(t_in.shape[1:], f32)
        for i in range(J):
            tsum = tsum + t_in[i]
        tsum = jnp.transpose(jnp.concatenate([tsum] * (128 // tsum.shape[0]), axis=0))
        heads = []
        for h in range(4):
            osum = jnp.zeros((rows, VD), f32)
            for i in range(J):
                osum = osum + o_in[h, i].astype(f32)
            heads.append((osum / tsum[:, h : h + 1]).astype(bf16))
        attended = jnp.concatenate(heads, axis=1)
        p_out[...] = jnp.dot(attended, ow[...], preferred_element_type=f32).astype(bf16)
        for step in far_first:
            peer = lax.rem(t + step, TP)
            place = pl.ds(pl.multiple_of(peer * quarter, quarter), quarter)
            send(p_out.at[place], p_in.at[t], send_sem.at[11], one_recv.at[6], e, peer)
        p_in[t] = p_out[pl.ds(pl.multiple_of(t * quarter, quarter), quarter), :]

    def finish_mixed():
        drain(p_in.at[pl.ds(0, TP - 1)], one_recv.at[6])
        projected = jnp.zeros((quarter, p_in.shape[2]), f32)
        for i in range(TP):
            projected = projected + p_in[i].astype(f32)
        mixed_out[...] = rms(projected, out_gain[...]).astype(bf16)

    def add_up(total, numbers, back):
        count = len(numbers) * unit - (cell if 0 in numbers else 0)
        with jax.named_scope("returns"):
            drain(R.at[pl.ds(0, count)], one_recv.at[back])
        for number in numbers:
            from_z = lax.rem(z + NZ - ORDER[number], NZ)
            place = pl.ds(pl.multiple_of(from_z * unit, unit), unit)
            total = total + jnp.dot(w_hi[:, place], R[place, :], preferred_element_type=f32)
            total = total + jnp.dot(w_lo[:, place], R[place, :], preferred_element_type=f32)
        return total

    with jax.named_scope("s00_share_down_0"):
        share_down(2)
    with jax.named_scope("s01_dispatch_6"):
        dispatch(6)
    with jax.named_scope("s02_dispatch_3"):
        dispatch(3)
    with jax.named_scope("s03_dispatch_5"):
        dispatch(5)
    with jax.named_scope("s04_dispatch_2"):
        dispatch(2)
    with jax.named_scope("s05_own_norm_"):
        own_norm()
    with jax.named_scope("s06_own_latents_0"):
        own_latents()
    with jax.named_scope("s09_own_queries_0"):
        own_queries()
    with jax.named_scope("s07_take_6"):
        take(6)
    with jax.named_scope("s08_dispatch_4"):
        dispatch(4)
    with jax.named_scope("s10_take_3"):
        take(3)
    with jax.named_scope("s11_take_2"):
        take(2)
    with jax.named_scope("s12_take_5"):
        take(5)
    with jax.named_scope("s13_pass_on_1"):
        pass_on(1)
    with jax.named_scope("s14_relay_3"):
        relay(X, 3, x_recv, 4)
    with jax.named_scope("s15_relay_2"):
        relay(X, 2, x_recv, 4)
    with jax.named_scope("s16_dispatch_1"):
        dispatch(1)
    with jax.named_scope("s17_take_4"):
        take(4)
    with jax.named_scope("s18_share_queries_0"):
        share_queries()
    with jax.named_scope("s19_pass_on_2"):
        pass_on(2)
    with jax.named_scope("s20_load_gu_"):
        load_g.wait()
        load_u.wait()
    with jax.named_scope("s21_hidden_1"):
        hidden(1)
    with jax.named_scope("s22_relay_4"):
        relay(X, 4, x_recv, 4)
    with jax.named_scope("s23_relay_5"):
        relay(X, 5, x_recv, 4)
    with jax.named_scope("s24_dispatch_7"):
        dispatch(7)
    with jax.named_scope("s25_weigh_0"):
        weigh()
    with jax.named_scope("s26_hidden_relay_1"):
        hidden_relay(1)
    with jax.named_scope("s27_pass_on_3"):
        pass_on(3)
    with jax.named_scope("s28_take_1"):
        take(1)
    with jax.named_scope("s29_hidden_2"):
        hidden(2)
    with jax.named_scope("s30_load_dd_"):
        load_d.wait()
        drain(wd.at[pl.ds(0, TP - 1)], one_recv.at[0])
    with jax.named_scope("s31_down_1"):
        down(1)
    with jax.named_scope("s32_expand_0"):
        expand()
    with jax.named_scope("s33_relay_6"):
        relay(X, 6, x_recv, 4)
    with jax.named_scope("s34_relay_1"):
        relay(X, 1, x_recv, 4)
    with jax.named_scope("s35_head_0"):
        head(0)
    with jax.named_scope("s36_head_1"):
        head(1)
        give_back(0)
    with jax.named_scope("s37_head_2"):
        head(2)
    with jax.named_scope("s38_hidden_relay_2"):
        hidden_relay(2)
    with jax.named_scope("s39_take_0"):
        take(0)
    with jax.named_scope("s40_take_7"):
        take(7)
    with jax.named_scope("s41_head_3"):
        head(3)
        give_back(1)
    with jax.named_scope("s42_head_4"):
        head(4)
    with jax.named_scope("s43_head_5"):
        head(5)
        give_back(2)
    with jax.named_scope("s44_hidden_0"):
        hidden(0)
    with jax.named_scope("s45_head_6"):
        head(6)
    with jax.named_scope("s47_head_7"):
        head(7)
        give_back(3)
        give_totals()
    with jax.named_scope("s46_relay_7"):
        relay(X, 7, x_recv, 4)
    with jax.named_scope("s48_down_2"):
        down(2)
    with jax.named_scope("s49_hidden_relay_0"):
        hidden_relay(0)
    with jax.named_scope("s50_hidden_3"):
        hidden(3)
    with jax.named_scope("s51_hidden_4"):
        hidden(4)
    with jax.named_scope("s52_down_0"):
        down(0)
    with jax.named_scope("s53_project_0"):
        project()
    with jax.named_scope("s54_hidden_relay_3"):
        hidden_relay(3)
    with jax.named_scope("s55_down_3"):
        down(3)
    with jax.named_scope("s56_hidden_relay_4"):
        hidden_relay(4)
    with jax.named_scope("s57_down_4"):
        down(4)
    total = jnp.zeros((rows, width), f32)
    total = add_up(total, tuple(n for n in range(NZ) if n not in LATE), 3)

    total = add_up(total, LATE, 9)
    m_send[...] = total.astype(bf16)
    for step in far_first:
        peer = lax.rem(t + step, TP)
        place = pl.ds(pl.multiple_of(peer * quarter, quarter), quarter)
        send(m_send.at[place], m_recv.at[t], send_sem.at[12], one_recv.at[7], e, peer)
    m_recv[t] = m_send[pl.ds(pl.multiple_of(t * quarter, quarter), quarter), :]
    with jax.named_scope("s58_finish_mixed_0"):
        finish_mixed()
    with jax.named_scope("last"):
        drain(m_recv.at[pl.ds(0, TP - 1)], one_recv.at[7])
    for i in range(TP):
        moe_out[:, i * width : (i + 1) * width] = m_recv[i]

    most = slots - unit
    drain(X.at[:, pl.ds(0, unit - cell)], send_sem.at[0])
    drain(outg.at[pl.ds(0, most)], send_sem.at[13])
    drain(wd.at[pl.ds(0, TP - 1)], send_sem.at[1])
    drain(Q.at[pl.ds(0, J // 2 - 1)], send_sem.at[2])
    drain(Q.at[pl.ds(0, J // 2)], send_sem.at[14])
    drain(KV.at[pl.ds(0, NZ - 1)], send_sem.at[3])
    drain(X.at[pl.ds(0, 2), pl.ds(0, most)], send_sem.at[4])
    drain(X.at[0, pl.ds(0, most)], send_sem.at[5])
    drain(H.at[pl.ds(0, 2)], send_sem.at[6])
    drain(H.at[0], send_sem.at[7])
    drain(Dn.at[pl.ds(0, slots - cell)], send_sem.at[8])
    drain(o_in.at[:, pl.ds(0, J - 1)], send_sem.at[9])
    drain(t_in.at[pl.ds(0, J - 1)], send_sem.at[10])
    drain(p_in.at[pl.ds(0, TP - 1)], send_sem.at[11])
    drain(m_recv.at[pl.ds(0, TP - 1)], send_sem.at[12])


def turn_tables(devices, rows):
    inverse = rope_base ** (-np.arange(0, ROPE, 2) / ROPE)
    inverse = np.tile(inverse, 4)[None, :]
    base = np.arange(devices)[:, None] * rows * inverse
    row = np.arange(rows)[:, None] * inverse
    return (
        np.concatenate([np.cos(base), np.sin(base)], axis=1).astype(np.float32),
        np.concatenate([np.cos(row), np.sin(row)], axis=1).astype(np.float32),
    )


def solution(mesh):
    EP, TP = mesh.shape["ep"], mesh.shape["tp"]
    J = 8
    NZ = EP // J
    placed = (
        P("ep", None),
        P(),
        P(None, "tp"),
        P(),
        P(),
        P(),
        P(None, "tp"),
        P(None, "tp"),
        P("tp", None),
        P(),
        P("ep", None),
        P(),
        P("ep", None, "tp"),
        P("ep", None, "tp"),
        P("ep", "tp", None),
        P("ep", None),
        P("ep", None),
    )

    def local(
        mix_in,
        mix_gain,
        query_weight,
        latent_weight,
        rotary_weight,
        latent_gain,
        key_weight,
        value_weight,
        output_weight,
        out_gain,
        ffn_in,
        ffn_gain,
        gate_weight,
        up_weight,
        down_weight,
        routes,
        route_scores,
    ):
        rows, D = mix_in.shape
        width = D // TP
        cell = MOST * (rows // QB)
        slots = EP * cell
        unit = gate_weight.shape[2]
        quarter = rows // TP
        base_turn, row_turn = turn_tables(EP, rows)
        hbm = pl.BlockSpec(memory_space=pl.ANY)
        vmem = pl.BlockSpec(memory_space=pltpu.VMEM)
        V = lambda *shape: pltpu.VMEM(shape, bf16)
        F = lambda *shape: pltpu.VMEM(shape, f32)
        S = pltpu.SemaphoreType.DMA

        def body(*refs):
            kernel(NZ, J, TP, *refs)

        out = pltpu.VMEM((quarter, D), bf16)
        return pl.pallas_call(
            body,
            name="layer",
            out_shape=(out, out),
            in_specs=[
                hbm, vmem, hbm, hbm, hbm, vmem, hbm, hbm, hbm, vmem,
                hbm, vmem, hbm, hbm, hbm, vmem, vmem, vmem, vmem,
            ],
            out_specs=(vmem, vmem),
            scratch_shapes=[
                V(rows, D),
                V(rows, D),
                V(D, query_weight.shape[1]),
                V(D, latent_weight.shape[1]),
                V(ROPE, D),
                V(*key_weight.shape),
                V(*value_weight.shape),
                V(*output_weight.shape),
                V(D, unit),
                V(D, unit),
                V(TP, unit, width),
                V(unit, D),
                V(slots, width),
                V(TP, J * cell, width),
                V(TP, slots, width),
                V(TP, slots, unit),
                V(slots, width),
                V(slots, width),
                V(slots, rows),
                V(rows, slots),
                V(rows, slots),
                V(rows, width),
                V(TP, quarter, width),
                V(J, rows, 768),
                V(NZ, rows, 640),
                V(rows, 768),
                V(4, NZ * rows, 256),
                V(4, NZ * rows, 256),
                V(4, J * rows, VD),
                F(J * rows, 128),
                F(J, 8, rows),
                V(4, J, rows, VD),
                F(J, 8, rows),
                V(rows, D),
                V(TP, quarter, D),
                S((12,)),
                S((8,)),
                S((3, 8)),
                S((3, 8)),
                S((2, NZ // 2)),
                S((10,)),
                S((15,)),
            ],
            compiler_params=pltpu.CompilerParams(
                collective_id=0, has_side_effects=True, vmem_limit_bytes=62 * 1024 * 1024
            ),
        )(
            mix_in,
            mix_gain[None, :],
            query_weight,
            latent_weight,
            rotary_weight.T,
            latent_gain[None, :],
            key_weight,
            value_weight,
            output_weight,
            out_gain[None, :],
            ffn_in,
            ffn_gain[None, :],
            gate_weight,
            up_weight,
            down_weight,
            routes.T,
            route_scores.T,
            base_turn,
            row_turn,
        )

    return jax.shard_map(
        local,
        mesh=mesh,
        in_specs=placed,
        out_specs=(P(("ep", "tp"), None), P(("ep", "tp"), None)),
        check_vma=False,
    )
```
